32 devices in a mesh: ep: 8 (over z, x), tp: 4 (over y, core).
Axes of the slice: x: 2, y: 2, z: 4, core: 2. Of those that a mesh axis runs over, the one named last changes fastest.
Arguments:
- head_inputs_unfiltered: bfloat16 [1024, 4096], P('ep', 'tp'), may hold values from -6 to 6
- group_write_vectors: bfloat16 [1024, 512], P('ep', 'tp'), may hold values from -6 to 6
- group_read_vectors: bfloat16 [1024, 512], P('ep', 'tp'), may hold values from -6 to 6
- output_gate_inputs: bfloat16 [1024, 4096], P('ep', 'tp'), may hold values from -6 to 6
- step_preactivation: float32 [64, 1024], P('tp', 'ep'), may hold values from -3.2 to 3.6
- extra_decay_logs: float32 [64, 1024], P('tp', 'ep'), may hold values from -0.7 to 0
- head_decay_logs: float32 [64], P('tp'), may hold values from -16 to -2.7
- head_filter_taps: bfloat16 [4, 4096], P(None, 'tp'), may hold values from -3 to 3
- write_filter_taps: bfloat16 [4, 512], P(None, 'tp'), may hold values from -3 to 3
- read_filter_taps: bfloat16 [4, 512], P(None, 'tp'), may hold values from -3 to 3
- grouped_norm_gain: float32 [4096], P('tp'), may hold values from 0.1 to 1.9
- mixer_output_weight: bfloat16 [4096, 2048], P('tp'), may hold values from -0.09375 to 0.09375
- expert_input_rows: bfloat16 [4096, 2048], P(('ep', 'tp')), may hold values from -6 to 6
- expert_norm_gain: float32 [2048], replicated, may hold values from 0.1 to 1.9
- routes: int32 [4096, 2], P(('ep', 'tp')), may hold values from 0 to 7, all different within a row; in each aligned block of 128 rows (0 to 127, 128 to 255, ...) at most 48 rows name the same one
- router_chosen_scores: bfloat16 [4096, 2], P(('ep', 'tp')), may hold values from 0.049804688 to 1
- routed_gate_weight: bfloat16 [8, 2048, 1024], P('ep', None, 'tp'), may hold values from -0.125 to 0.125
- routed_up_weight: bfloat16 [8, 2048, 1024], P('ep', None, 'tp'), may hold values from -0.125 to 0.125
- routed_down_weight: bfloat16 [8, 1024, 2048], P('ep', 'tp'), may hold values from -0.1875 to 0.1875
- shared_gate_weight: bfloat16 [2048, 512], P(None, 'tp'), may hold values from -0.125 to 0.125
- shared_up_weight: bfloat16 [2048, 512], P(None, 'tp'), may hold values from -0.125 to 0.125
- shared_down_weight: bfloat16 [512, 2048], P('tp'), may hold values from -0.25 to 0.25
Outputs:
- mixer_result: bfloat16 [1024, 2048], P(('ep', 'tp'))
- moe_result: bfloat16 [4096, 2048], P(('ep', 'tp'))
The draws below stay inside these ranges and needn't reach their ends.
Inputs may be any that keep to these rules, and one draw needn't show every extreme that they name: `routes`: within the 128 rows of one device no expert is named more than 48 times; a row names 2 different experts.
All inputs are finite; a program needn't handle non-finite values.
Results may differ from the reference program's by a relative error of at most 0.0095.
Values may be sent and summed in bfloat16 or wider, within the bound.
A program may use at most 128 MiB of HBM per device.

```python
import math
import jax
import jax.numpy as jnp
import numpy as np
from jax import lax

D = 2048
HEADS = 64
HEAD_DIM = 64
GROUPS = 4
STATE = 128
CONV = 4
BLOCK = 64
INNER = 4096
MIX_ROWS = 128
MIX_TOKENS = 1024
EXPERT_FF = 1024
SHARED_FF = 512
EXPERTS = 8
TOP_K = 2
MOE_ROWS = 128
MOE_TOKENS = 4096
CAPACITY = 48
N_TP = 4


def draw_step_preactivation(key, part):
    key_noise, key_shift = jax.random.split(key)
    block_total = MIX_TOKENS // MIX_ROWS
    noise = jnp.clip(0.7 * jax.random.normal(key_noise, (HEADS, MIX_TOKENS), jnp.float32), -1.6, 1.6)
    shifts = jax.random.uniform(key_shift, (block_total,), jnp.float32, -1.0, 1.5)
    return noise + jnp.repeat(shifts, MIX_ROWS)[None, :]


def draw_extra_decay_logs(key, part):
    key_place, key_depth = jax.random.split(key)
    stride = MIX_TOKENS // 3
    places = jnp.arange(3, dtype=jnp.int32) * stride + jax.random.randint(key_place, (3,), 0, stride)
    kept = jax.random.uniform(key_depth, (3, HEADS), jnp.float32, 0.5, 0.8)
    positions = jnp.arange(MIX_TOKENS, dtype=jnp.int32)
    hits = (positions[None, :] == places[:, None]).astype(jnp.float32)
    return jnp.einsum('bh,bt->ht', jnp.log(kept), hits)


def draw_head_decay_logs(key, part):
    key_kind, key_fast, key_slow = jax.random.split(key, 3)
    fast_share = 0.5
    is_fast = jax.random.uniform(key_kind, (HEADS,), jnp.float32) < fast_share
    fast_log = jax.random.uniform(key_fast, (HEADS,), jnp.float32, math.log(1.0 / 40.0), math.log(1.0 / 15.0))
    slow_log = jax.random.uniform(key_slow, (HEADS,), jnp.float32, math.log(0.02), math.log(0.25)) - math.log(float(MIX_TOKENS))
    return jnp.where(is_fast, fast_log, slow_log)


def shard_levels(key, shape, cuts, smallest, high):
    loudness, own = 1.0, jax.random.fold_in(key, 6)
    for position, blocks in cuts:
        draws = jnp.exp(jax.random.uniform(jax.random.fold_in(own, position), (blocks,), jnp.float32, smallest / len(cuts), high / len(cuts)))
        loudness = loudness * jnp.repeat(draws, shape[position] // blocks).reshape([-1 if axis == position else 1 for axis in range(len(shape))])
    return loudness


def deal_out(key, own, number, rows, amount, top, limit, skew):
    sequence = jax.random.permutation(key, amount)
    packed, ordinary = load_shares(amount, rows * top, limit, skew, True), load_shares(amount, rows * top, limit, skew, False)
    places = jnp.arange(amount)

    def named(tallies, rotation):
        used = int((tallies > 0).sum())
        fixed = max(1, used // 4)
        passed = fixed + (places - fixed + rotation * (used - fixed)) % max(1, amount - fixed)
        return jnp.zeros((amount,), jnp.int32).at[sequence[jnp.where(places < fixed, places, passed)]].set(jnp.asarray(tallies, jnp.int32))

    tallies = jnp.where(number % 4 == 0, named(packed, number // 4), named(ordinary, number - number // 4 - 1))
    mixed = jax.random.permutation(jax.random.fold_in(own, 3), amount)
    giver, taker = mixed[0:amount // 2 * 2:2], mixed[1:amount // 2 * 2:2]
    margin = jnp.minimum(tallies[giver] - 1, limit - tallies[taker]) // 2
    margin = jnp.where((giver == sequence[0]) | (taker == sequence[0]) | (tallies[taker] == 0), 0, jnp.maximum(margin, 0))
    passed = jax.random.randint(jax.random.fold_in(own, 4), (amount // 2,), 0, 1 << 20) % (margin + 1)
    tallies = tallies.at[giver].add(-passed).at[taker].add(passed)
    items = jnp.searchsorted(jnp.cumsum(tallies), jnp.arange(rows * top), side="right").astype(jnp.int32)
    grid = items.reshape(top, rows).T
    grid = grid[jax.random.permutation(jax.random.fold_in(own, 1), rows)]
    rotation = jax.random.randint(jax.random.fold_in(own, 2), (rows, 1), 0, top)
    return jnp.take_along_axis(grid, (jnp.arange(top)[None, :] + rotation) % top, axis=1)


def load_shares(number_of, total, most, lean, full):
    weights = [(1 << 20) // math.isqrt(grade ** lean) + 1 for grade in range(1, number_of + 1)]
    largest = most if full else min(most, max(-(-total // number_of), total * weights[0] // sum(weights)))
    least = 1 if total - largest >= number_of - 1 else 0
    counts, surplus = [largest] + [least] * (number_of - 1), total - largest - least * (number_of - 1)
    while surplus > 0:
        candidates = [i for i in range(1, number_of) if counts[i] < largest] or [i for i in range(1, number_of) if counts[i] < most]
        whole, remaining = sum([weights[i] for i in candidates]), surplus
        for i in candidates:
            more = min(most - counts[i], max(1, remaining * weights[i] // whole), surplus)
            counts[i] = counts[i] + more
            surplus = surplus - more
    return np.array(counts)


def scatter_about(key, dims, deviation, bound, pieces=(), kind=jnp.bfloat16):
    level = shard_levels(key, dims, pieces, -0.22, 0.18) if pieces else 1.0
    result = jax.random.normal(key, dims, jnp.float32) * deviation * level
    return jnp.minimum(jnp.maximum(result, -bound), bound).astype(kind)


def setup_inputs(seed: int = 0) -> dict:
    streams_of = jax.random.split(jax.random.key(seed), 23)
    head_inputs_unfiltered = scatter_about(streams_of[0], (MIX_TOKENS, INNER), 1.0, 6.0, ((0, 8), (1, 4)))
    group_write_vectors = scatter_about(streams_of[1], (MIX_TOKENS, GROUPS * STATE), 1.0, 6.0, ((0, 8), (1, 4)))
    group_read_vectors = scatter_about(streams_of[2], (MIX_TOKENS, GROUPS * STATE), 1.0, 6.0, ((0, 8), (1, 4)))
    output_gate_inputs = scatter_about(streams_of[3], (MIX_TOKENS, INNER), 1.0, 6.0, ((0, 8), (1, 4)))
    step_preactivation = draw_step_preactivation(jax.random.fold_in(streams_of[22], 71), 0)
    extra_decay_logs = draw_extra_decay_logs(jax.random.fold_in(streams_of[22], 71), 0)
    head_decay_logs = draw_head_decay_logs(jax.random.fold_in(streams_of[22], 71), 0)
    head_filter_taps = scatter_about(streams_of[7], (CONV, INNER), 0.5, 3.0, ((1, 4),))
    write_filter_taps = scatter_about(streams_of[8], (CONV, GROUPS * STATE), 0.5, 3.0, ((1, 4),))
    read_filter_taps = scatter_about(streams_of[9], (CONV, GROUPS * STATE), 0.5, 3.0, ((1, 4),))
    grouped_norm_gain = jnp.clip(1.0 + 0.18 * jax.random.normal(streams_of[10], (INNER,), jnp.float32), 0.1, 1.9)
    mixer_output_weight = scatter_about(streams_of[11], (INNER, D), INNER ** -0.5, 0.09375, ((0, 4),))
    expert_input_rows = scatter_about(streams_of[12], (MOE_TOKENS, D), 1.0, 6.0, ((0, 32),))
    expert_norm_gain = jnp.clip(1.0 + 0.18 * jax.random.normal(streams_of[13], (D,), jnp.float32), 0.1, 1.9)
    routes_keys = jax.random.split(jax.random.fold_in(streams_of[14], 1), MOE_TOKENS // MOE_ROWS)
    routes_turns = jax.random.permutation(jax.random.fold_in(streams_of[14], 3), MOE_TOKENS // MOE_ROWS)
    routes = jax.vmap(lambda own, number: deal_out(jax.random.fold_in(streams_of[14], 2), own, number, MOE_ROWS, EXPERTS, TOP_K, CAPACITY, 2))(routes_keys, routes_turns).reshape((MOE_TOKENS, TOP_K))
    router_chosen_scores = jnp.clip(jnp.exp(math.log(1.0) - 2.9996462 * jax.random.uniform(streams_of[15], (MOE_TOKENS, TOP_K), jnp.float32) ** shard_levels(streams_of[15], (MOE_TOKENS, TOP_K), ((0, 32),), -0.2, 0.2)), 0.049804688, 1.0).astype(jnp.bfloat16)
    routed_gate_weight = scatter_about(streams_of[16], (EXPERTS, D, EXPERT_FF), D ** -0.5, 0.125, ((0, 8), (2, 4)))
    routed_up_weight = scatter_about(streams_of[17], (EXPERTS, D, EXPERT_FF), D ** -0.5, 0.125, ((0, 8), (2, 4)))
    routed_down_weight = scatter_about(streams_of[18], (EXPERTS, EXPERT_FF, D), EXPERT_FF ** -0.5, 0.1875, ((0, 8), (1, 4)))
    shared_gate_weight = scatter_about(streams_of[19], (D, SHARED_FF), D ** -0.5, 0.125, ((1, 4),))
    shared_up_weight = scatter_about(streams_of[20], (D, SHARED_FF), D ** -0.5, 0.125, ((1, 4),))
    shared_down_weight = scatter_about(streams_of[21], (SHARED_FF, D), SHARED_FF ** -0.5, 0.25, ((0, 4),))
    return dict(head_inputs_unfiltered=head_inputs_unfiltered, group_write_vectors=group_write_vectors, group_read_vectors=group_read_vectors, output_gate_inputs=output_gate_inputs, step_preactivation=step_preactivation, extra_decay_logs=extra_decay_logs, head_decay_logs=head_decay_logs, head_filter_taps=head_filter_taps, write_filter_taps=write_filter_taps, read_filter_taps=read_filter_taps, grouped_norm_gain=grouped_norm_gain, mixer_output_weight=mixer_output_weight, expert_input_rows=expert_input_rows, expert_norm_gain=expert_norm_gain, routes=routes, router_chosen_scores=router_chosen_scores, routed_gate_weight=routed_gate_weight, routed_up_weight=routed_up_weight, routed_down_weight=routed_down_weight, shared_gate_weight=shared_gate_weight, shared_up_weight=shared_up_weight, shared_down_weight=shared_down_weight)


eps_norm = 1e-06
route_scale = 2.5
highest = lax.Precision.HIGHEST

def causal_conv(values, weights):
    taps = weights.shape[0]
    length = values.shape[0]
    padded = jnp.concatenate([jnp.zeros((taps - 1, values.shape[1]), jnp.float32), values.astype(jnp.float32)], axis=0)
    running_sum = jnp.zeros((length, values.shape[1]), jnp.float32)
    for offset in range(taps):
        running_sum = running_sum + weights[offset].astype(jnp.float32) * padded[offset:offset + length]
    return jax.nn.silu(running_sum)

def state_space(head_values, write_values, read_values, step_length_value, decay_rate_logs):
    length = head_values.shape[0]
    block_count = length // BLOCK
    per_group = HEADS // GROUPS
    head_blocks = head_values.reshape(block_count, BLOCK, GROUPS, per_group, HEAD_DIM)
    write_blocks = write_values.reshape(block_count, BLOCK, GROUPS, STATE)
    read_blocks = read_values.reshape(block_count, BLOCK, GROUPS, STATE)
    step_blocks = step_length_value.T.reshape(block_count, BLOCK, GROUPS, per_group)
    rate_blocks = decay_rate_logs.T.reshape(block_count, BLOCK, GROUPS, per_group)
    lower_mask = jnp.tril(jnp.ones((BLOCK, BLOCK), bool))

    def advance(carried, block_data):
        head_blk, write_blk, read_blk, step_blk, rate_blk = block_data
        cumulative = jnp.cumsum(rate_blk, axis=0)
        weighted = head_blk * step_blk[..., None]
        gap_logs = cumulative[:, None] - cumulative[None, :]
        within = jnp.exp(jnp.where(lower_mask[:, :, None, None], gap_logs, -jnp.inf))
        affinity = jnp.einsum('lgn,sgn->lsg', read_blk, write_blk, precision=highest)
        local_part = jnp.einsum('lsge,sgep->lgep', affinity[..., None] * within, weighted, precision=highest)
        carried_part = jnp.einsum('lgn,gepn->lgep', read_blk, carried, precision=highest) * jnp.exp(cumulative)[..., None]
        to_end = jnp.exp(cumulative[-1:] - cumulative)
        new_state = carried * jnp.exp(cumulative[-1])[..., None, None] + jnp.einsum('sgn,sgep->gepn', write_blk, weighted * to_end[..., None], precision=highest)
        return (new_state, local_part + carried_part)
    initial = jnp.zeros((GROUPS, per_group, HEAD_DIM, STATE), jnp.float32)
    _, outputs = lax.scan(advance, initial, (head_blocks, write_blocks, read_blocks, step_blocks, rate_blocks))
    return outputs.reshape(length, HEADS * HEAD_DIM)

def reference(head_inputs_unfiltered, group_write_vectors, group_read_vectors, output_gate_inputs, step_preactivation, extra_decay_logs, head_decay_logs, head_filter_taps, write_filter_taps, read_filter_taps, grouped_norm_gain, mixer_output_weight, expert_input_rows, expert_norm_gain, routes, router_chosen_scores, routed_gate_weight, routed_up_weight, routed_down_weight, shared_gate_weight, shared_up_weight, shared_down_weight):
    length = head_inputs_unfiltered.shape[0]
    head_values = causal_conv(head_inputs_unfiltered, head_filter_taps)
    write_values = causal_conv(group_write_vectors, write_filter_taps)
    read_values = causal_conv(group_read_vectors, read_filter_taps)
    step_length_value = jax.nn.softplus(step_preactivation)
    decay_rate_logs = -jnp.exp(head_decay_logs)[:, None] * step_length_value + extra_decay_logs
    scan_out = state_space(head_values, write_values, read_values, step_length_value, decay_rate_logs)
    gated = scan_out * jax.nn.silu(output_gate_inputs.astype(jnp.float32))
    grouped = gated.reshape(length, GROUPS, HEADS * HEAD_DIM // GROUPS)
    grouped = grouped * lax.rsqrt(lax.optimization_barrier(jnp.mean(grouped * grouped, axis=-1, keepdims=True)) + eps_norm)
    mixer_normed = (grouped.reshape(length, HEADS * HEAD_DIM) * grouped_norm_gain).astype(jnp.bfloat16)
    mixer_result = jnp.dot(mixer_normed, mixer_output_weight, preferred_element_type=jnp.float32).astype(jnp.bfloat16)
    rows_float = expert_input_rows.astype(jnp.float32)
    moe_normed = (rows_float * lax.rsqrt(lax.optimization_barrier(jnp.mean(rows_float * rows_float, axis=-1, keepdims=True)) + eps_norm) * expert_norm_gain).astype(jnp.bfloat16)
    score_float = router_chosen_scores.astype(jnp.float32)
    route_weight = score_float / lax.optimization_barrier(jnp.sum(score_float, axis=-1, keepdims=True)) * route_scale
    token_total = expert_input_rows.shape[0]
    device_total = token_total // MOE_ROWS
    flat_expert = routes.reshape(device_total, MOE_ROWS * TOP_K)
    onehot = (flat_expert[:, :, None] == jnp.arange(EXPERTS, dtype=jnp.int32)[None, None, :]).astype(jnp.int32)
    before = jnp.cumsum(onehot, axis=1) - onehot
    slot_rank = lax.optimization_barrier(jnp.sum(before * onehot, axis=2))
    slot_index = jnp.arange(device_total, dtype=jnp.int32)[:, None] * CAPACITY + slot_rank
    token_index = jnp.arange(token_total * TOP_K, dtype=jnp.int32) // TOP_K
    table_token = jnp.full((EXPERTS, device_total * CAPACITY), token_total, jnp.int32).at[flat_expert.reshape(-1), slot_index.reshape(-1)].set(token_index)
    table_weight = jnp.zeros((EXPERTS, device_total * CAPACITY), jnp.float32).at[flat_expert.reshape(-1), slot_index.reshape(-1)].set(route_weight.reshape(-1))
    padded_rows = jnp.concatenate([moe_normed, jnp.zeros((1, D), jnp.bfloat16)], axis=0)
    slice_width = EXPERT_FF // N_TP

    def one_expert(running_sum, expert_data):
        tokens_here, weights_here, gate_weight, up_weight, down_weight = expert_data
        picked = padded_rows[tokens_here]
        gate_value = jnp.dot(picked, gate_weight, preferred_element_type=jnp.float32)
        up_value = jnp.dot(picked, up_weight, preferred_element_type=jnp.float32)
        hidden = (jax.nn.silu(gate_value) * up_value).astype(jnp.bfloat16)
        summed = jnp.zeros((picked.shape[0], D), jnp.float32)
        for slice_index in range(N_TP):
            lower_edge = slice_index * slice_width
            part = jnp.dot(hidden[:, lower_edge:lower_edge + slice_width], down_weight[lower_edge:lower_edge + slice_width], preferred_element_type=jnp.float32).astype(jnp.bfloat16)
            summed = summed + part.astype(jnp.float32)
        return (running_sum.at[tokens_here].add(summed * weights_here[:, None]), None)
    routed, _ = lax.scan(one_expert, jnp.zeros((token_total + 1, D), jnp.float32), (table_token, table_weight, routed_gate_weight, routed_up_weight, routed_down_weight))
    shared_hidden = (jax.nn.silu(jnp.dot(moe_normed, shared_gate_weight, preferred_element_type=jnp.float32)) * jnp.dot(moe_normed, shared_up_weight, preferred_element_type=jnp.float32)).astype(jnp.bfloat16)
    shared_total = jnp.dot(shared_hidden, shared_down_weight, preferred_element_type=jnp.float32)
    moe_result = (shared_total + routed[:token_total]).astype(jnp.bfloat16)
    return (mixer_result, moe_result)
```

```python
import functools

import jax
import jax.numpy as jnp
from jax import lax
from jax.experimental import pallas as pl
from jax.experimental.pallas import tpu as pltpu
from jax.sharding import PartitionSpec as P

MESH = pl.DeviceIdType.MESH
HEAD_DIM = 64
STATE = 128
BLOCK = 64


eps_norm = 1e-06
route_scale = 2.5
highest = lax.Precision.HIGHEST


def from_behind(value, axis, by):
    devices = lax.axis_size(axis)
    pairs = [(i, i + by) for i in range(devices) if 0 <= i + by < devices]
    return lax.ppermute(value, axis, pairs)


def sent_state(decay, state, axis, by):
    heads, width = decay.shape[0], state.shape[-1]
    parts, rest = [], decay
    for _ in range(3):
        part = lax.reduce_precision(rest, exponent_bits=8, mantissa_bits=7)
        parts.append(part)
        rest = rest - part
    decay_rows = jnp.pad(jnp.stack(parts, axis=1), ((0, 0), (0, width - 3)))
    packed = jnp.concatenate([state.reshape(-1, width), decay_rows], axis=0).astype(jnp.bfloat16)
    packed = from_behind(packed, axis, by).astype(jnp.float32)
    return jnp.sum(packed[-heads:, :3], axis=-1), packed[:-heads].reshape(state.shape)


def carried_in(decay, state, axis):
    shape = state.shape
    own = (decay.reshape(-1), state.reshape((-1,) + shape[-2:]))
    before, by = None, 1
    while by < lax.axis_size(axis):
        span = own if before is None else combine_states(before, own)
        received = sent_state(*span, axis, by)
        before = received if before is None else combine_states(received, before)
        by *= 2
    if before is None:
        return jnp.zeros_like(state)
    return before[1].reshape(shape)


def combine_states(earlier_part, later_part):
    return (
        earlier_part[0] + later_part[0],
        later_part[1] + jnp.exp(later_part[0])[..., None, None] * earlier_part[1],
    )


def conv_silu(values, weights):
    taps = weights.shape[0]
    length = values.shape[0] - taps + 1
    running_sum = jnp.zeros((length, values.shape[1]), jnp.float32)
    for offset in range(taps):
        running_sum = running_sum + weights[offset].astype(jnp.float32) * values[
            offset : offset + length
        ].astype(jnp.float32)
    return jax.nn.silu(running_sum)


def tail_rows_from_behind(head_inputs, write_vectors, read_vectors, taps):
    start = head_inputs.shape[0] - taps + 1
    tail_rows = jnp.concatenate([head_inputs[start:], write_vectors[start:], read_vectors[start:]], axis=1)
    return from_behind(tail_rows, "ep", 1)


def mixer_rows(
    earlier,
    head_inputs_unfiltered,
    group_write_vectors,
    group_read_vectors,
    output_gate_inputs,
    step_preactivation,
    extra_decay_logs,
    head_decay_logs,
    head_filter_taps,
    write_filter_taps,
    read_filter_taps,
    grouped_norm_gain,
):
    row_total = head_inputs_unfiltered.shape[0]
    head_chans = head_inputs_unfiltered.shape[1]
    write_chans = group_write_vectors.shape[1]
    padded_heads = jnp.concatenate([earlier[:, :head_chans], head_inputs_unfiltered], axis=0)
    padded_write = jnp.concatenate(
        [earlier[:, head_chans : head_chans + write_chans], group_write_vectors], axis=0
    )
    padded_read = jnp.concatenate(
        [earlier[:, head_chans + write_chans :], group_read_vectors], axis=0
    )
    heads_local = step_preactivation.shape[0]
    groups_local = write_chans // STATE
    per_group = heads_local // groups_local
    block_count = row_total // BLOCK
    head_values = conv_silu(padded_heads, head_filter_taps).reshape(
        block_count, BLOCK, groups_local, per_group, HEAD_DIM
    )
    write_values = conv_silu(padded_write, write_filter_taps).reshape(
        block_count, BLOCK, groups_local, STATE
    )
    read_values = conv_silu(padded_read, read_filter_taps).reshape(
        block_count, BLOCK, groups_local, STATE
    )
    step_length_value = jax.nn.softplus(step_preactivation)
    decay_rate_logs = -jnp.exp(head_decay_logs)[:, None] * step_length_value + extra_decay_logs
    step_blocks = step_length_value.reshape(groups_local, per_group, block_count, BLOCK)
    cumulative = jnp.cumsum(
        decay_rate_logs.reshape(groups_local, per_group, block_count, BLOCK), axis=3
    )
    weighted = head_values * jnp.transpose(step_blocks, (2, 3, 0, 1))[..., None]
    lower_mask = jnp.tril(jnp.ones((BLOCK, BLOCK), bool))
    gap_logs = cumulative[..., :, None] - cumulative[..., None, :]
    within = jnp.exp(jnp.where(lower_mask, gap_logs, -jnp.inf))
    affinity = jnp.einsum("blgn,bsgn->gbls", read_values, write_values, precision=highest)
    local_part = jnp.einsum(
        "gebls,bsgep->blgep", affinity[:, None] * within, weighted, precision=highest
    )
    to_end = jnp.exp(cumulative[..., -1:] - cumulative)
    block_states = jnp.einsum(
        "bsgn,bsgep,gebs->bgepn", write_values, weighted, to_end, precision=highest
    )
    block_decay = cumulative[..., -1]
    running = jnp.cumsum(block_decay, axis=2)
    entering = running - block_decay
    earlier_blocks = jnp.tril(jnp.ones((block_count, block_count), bool), -1)
    block_ratio = entering[..., :, None] - running[..., None, :]
    carry_weights = jnp.exp(jnp.where(earlier_blocks, block_ratio, -jnp.inf))
    inside = jnp.einsum("gebc,cgepn->bgepn", carry_weights, block_states, precision=highest)
    device_decay = running[..., -1]
    device_state = jnp.einsum(
        "gec,cgepn->gepn",
        jnp.exp(device_decay[..., None] - running),
        block_states,
        precision=highest,
    )
    incoming = carried_in(device_decay, device_state, "ep")
    states_in = (
        inside + jnp.exp(jnp.transpose(entering, (2, 0, 1)))[..., None, None] * incoming[None]
    )
    carried_part = (
        jnp.einsum("blgn,bgepn->blgep", read_values, states_in, precision=highest)
        * jnp.transpose(jnp.exp(cumulative), (2, 3, 0, 1))[..., None]
    )
    scan_out = (local_part + carried_part).reshape(row_total, groups_local, per_group * HEAD_DIM)
    gate_values = jax.nn.silu(output_gate_inputs.astype(jnp.float32)).reshape(
        row_total, groups_local, per_group * HEAD_DIM
    )
    gated_rows = scan_out * gate_values
    gated_rows = gated_rows * lax.rsqrt(
        jnp.mean(gated_rows * gated_rows, axis=-1, keepdims=True) + eps_norm
    )
    return (gated_rows.reshape(row_total, head_chans) * grouped_norm_gain).astype(jnp.bfloat16)


def local(
    head_inputs_unfiltered,
    group_write_vectors,
    group_read_vectors,
    output_gate_inputs,
    step_preactivation,
    extra_decay_logs,
    head_decay_logs,
    head_filter_taps,
    write_filter_taps,
    read_filter_taps,
    grouped_norm_gain,
    mixer_output_weight,
    expert_input_rows,
    expert_norm_gain,
    routes,
    router_chosen_scores,
    routed_gate_weight,
    routed_up_weight,
    routed_down_weight,
    shared_gate_weight,
    shared_up_weight,
    shared_down_weight,
):
    earlier = tail_rows_from_behind(
        head_inputs_unfiltered, group_write_vectors, group_read_vectors, head_filter_taps.shape[0]
    )
    tp_count = lax.axis_size("tp")
    ep_count = lax.axis_size("ep")
    tok_local = expert_input_rows.shape[0]
    model_width = expert_input_rows.shape[1]
    top_count = routes.shape[1]
    local_experts = routed_gate_weight.shape[0]
    experts = local_experts * ep_count
    capacity = 3 * tok_local * top_count // (2 * experts)
    rows_float = expert_input_rows.astype(jnp.float32)
    normed = (
        rows_float
        * lax.rsqrt(jnp.mean(rows_float * rows_float, axis=-1, keepdims=True) + eps_norm)
        * expert_norm_gain
    ).astype(jnp.bfloat16)
    score_float = router_chosen_scores.astype(jnp.float32)
    weights = score_float / jnp.sum(score_float, axis=1, keepdims=True) * route_scale
    choice = routes[None, :, :] == jnp.arange(experts, dtype=jnp.int32)[:, None, None]
    named = jnp.any(choice, axis=2)
    weight_of = jnp.sum(jnp.where(choice, weights[None], 0.0), axis=2)
    row_order = jnp.arange(tok_local, dtype=jnp.int32)
    earlier_rows = (row_order[:, None] < row_order[None, :]).astype(jnp.bfloat16)
    rank = jnp.dot(
        named.astype(jnp.bfloat16), earlier_rows, preferred_element_type=jnp.float32
    ).astype(jnp.int32)

    cuts = [0, capacity // 2, capacity] if capacity > 1 else [0, capacity]
    picks, outgoing = [], []
    for low, high in zip(cuts[:-1], cuts[1:]):
        places = jnp.arange(low, high, dtype=jnp.int32)
        picked = named[:, None, :] & (rank[:, None, :] == places[None, :, None])
        picks.append(picked)
        outgoing.append(
            jnp.dot(
                picked.reshape(-1, tok_local).astype(jnp.bfloat16),
                normed,
                preferred_element_type=jnp.float32,
            ).astype(jnp.bfloat16)
        )
    group_rows = lax.all_gather(normed, "tp", axis=0, tiled=True)
    earlier, group_rows, outgoing[0] = lax.optimization_barrier((earlier, group_rows, outgoing[0]))

    arrived = []
    for block in outgoing:
        arrived.append(lax.all_to_all(block, "ep", split_axis=0, concat_axis=0, tiled=True))
    gathered = [lax.all_gather(block, "tp", axis=0) for block in arrived]

    shared_hidden = (
        jax.nn.silu(jnp.dot(group_rows, shared_gate_weight, preferred_element_type=jnp.float32))
        * jnp.dot(group_rows, shared_up_weight, preferred_element_type=jnp.float32)
    ).astype(jnp.bfloat16)
    shared_part = jnp.dot(shared_hidden, shared_down_weight, preferred_element_type=jnp.float32)

    mixer_normed = mixer_rows(
        earlier,
        head_inputs_unfiltered,
        group_write_vectors,
        group_read_vectors,
        output_gate_inputs,
        step_preactivation,
        extra_decay_logs,
        head_decay_logs,
        head_filter_taps,
        write_filter_taps,
        read_filter_taps,
        grouped_norm_gain,
    )

    def expert_rows(block):
        sources = block.reshape(tp_count, ep_count, local_experts, -1, model_width)
        gate_value = jnp.einsum(
            "osecd,edf->osecf", sources, routed_gate_weight, preferred_element_type=jnp.float32
        )
        up_value = jnp.einsum(
            "osecd,edf->osecf", sources, routed_up_weight, preferred_element_type=jnp.float32
        )
        hidden = (jax.nn.silu(gate_value) * up_value).astype(jnp.bfloat16)
        partial_value = jnp.einsum(
            "osecf,efd->osecd", hidden, routed_down_weight, preferred_element_type=jnp.float32
        ).astype(jnp.bfloat16)
        return lax.psum_scatter(
            partial_value.reshape(-1, model_width), "tp", scatter_dimension=0, tiled=True
        )

    own_term = jnp.zeros((tok_local, model_width), jnp.float32)
    for block, picked in zip(gathered, picks):
        returned = lax.all_to_all(
            expert_rows(block), "ep", split_axis=0, concat_axis=0, tiled=True
        )
        mixing = jnp.where(picked, weight_of[:, None, :], 0.0).reshape(-1, tok_local)
        own_term = own_term + jnp.einsum(
            "sr,sd->rd", mixing, returned.astype(jnp.float32), precision=highest
        )
    mix_block = mixer_normed.shape[0] // tp_count
    block_rows = mix_block + tok_local
    mix_term = jnp.dot(
        mixer_normed, mixer_output_weight, preferred_element_type=jnp.float32
    ).astype(jnp.bfloat16).reshape(tp_count, mix_block, model_width)
    moe_term = shared_part.astype(jnp.bfloat16).reshape(tp_count, tok_local, model_width)
    row_sums = lax.psum_scatter(
        jnp.concatenate([mix_term, moe_term], axis=1).reshape(tp_count * block_rows, model_width),
        "tp",
        scatter_dimension=0,
        tiled=True,
    )
    mixer_result = row_sums[:mix_block]
    moe_total = row_sums[mix_block:].astype(jnp.float32) + own_term
    return (mixer_result.astype(jnp.bfloat16), moe_total.astype(jnp.bfloat16))


def message_names(half):
    names = ["meta_core", "meta_y", "meta_far", "rows_core", "rows_y", "rows_fwd", "shared", "dense", "mix_core", "mix_far", "mix_y"]
    for d in range(half):
        names += [f"{kind}{d}" for kind in ("a", "ay", "ac", "ra", "ry", "fa", "b", "bc", "rb", "fb")]
    return {name: i for i, name in enumerate(names)}


def exchange_kernel(
    ep_count,
    capacity,
    rows_hbm,
    meta_ref,
    gain_ref,
    mix_hbm,
    gate_hbm,
    up_hbm,
    down_hbm,
    sgate_hbm,
    sup_hbm,
    sdown_hbm,
    mix_out,
    moe_out,
    rows_v,
    mix_v,
    gate_v,
    up_v,
    down_v,
    sgate_v,
    sup_v,
    sdown_v,
    meta_v,
    grp,
    pack_a,
    pack_b,
    xa,
    xb,
    ya,
    yb,
    ra,
    rb,
    sa,
    sb,
    ry,
    fa,
    ret_a,
    ret_b,
    sp,
    rsp,
    dense,
    dense_s,
    dense_r,
    mix_r,
    mix_s,
    mix_ry,
    load_sem,
    send_sem,
    recv_sem,
):
    half = ep_count // 2
    cap = capacity
    tok, width = rows_v.shape
    col = 512
    ids = message_names(half)
    e = lax.axis_index("ep")
    t = lax.axis_index("tp")
    base = (e // half) * half
    q = e - base
    other = half - base
    t_core = t + 1 - 2 * (t % 2)
    t_y = (t + 2) % 4
    t_far = (t_core + 2) % 4
    core, ydev, far = (e, t_core), (e, t_y), (e, t_far)

    def to_a(d):
        return (other + (q + d) % half, t)

    def from_a(d):
        return (other + (q + half - d) % half, t)

    def to_b(d):
        return (base + (q + d) % half, t)

    def from_b(d):
        return (base + (q + half - d) % half, t)

    loads = {}
    for i, (name, src, dst) in enumerate(
        (
            ("rows", rows_hbm, rows_v),
            ("sgate", sgate_hbm, sgate_v),
            ("sup", sup_hbm, sup_v),
            ("sdown", sdown_hbm, sdown_v),
            ("gate", gate_hbm, gate_v),
            ("up", up_hbm, up_v),
            ("down", down_hbm, down_v),
            ("mix", mix_hbm, mix_v),
        )
    ):
        loads[name] = pltpu.make_async_copy(src, dst, load_sem.at[i])
        loads[name].start()

    copies = {}

    def send(name, src, dst, device):
        i = ids[name]
        copies[name] = pltpu.make_async_remote_copy(
            src_ref=src,
            dst_ref=dst,
            send_sem=send_sem.at[i],
            recv_sem=recv_sem.at[i],
            device_id=device,
            device_id_type=MESH,
        )
        copies[name].start()

    def arrived(name):
        copies[name].wait_recv()

    barrier = pltpu.get_barrier_semaphore()
    peers = [core, ydev, far] + [to_a(d) for d in range(half)] + [to_b(d) for d in range(1, half)]
    for peer in peers:
        pl.semaphore_signal(barrier, inc=1, device_id=peer, device_id_type=MESH)

    meta_v[0] = meta_ref[...]
    loads["rows"].wait()

    def norm_rows(i, carry):
        at = pl.ds(pl.multiple_of(i * 16, 16), 16)
        x = rows_v[at, :].astype(jnp.float32)
        scale = lax.rsqrt(jnp.mean(x * x, axis=-1, keepdims=True) + eps_norm)
        grp[0, at, :] = (x * scale * gain_ref[...]).astype(jnp.bfloat16)
        return carry

    lax.fori_loop(0, tok // 16, norm_rows, 0)
    pl.semaphore_wait(barrier, len(peers))

    send("meta_y", meta_v.at[0], meta_v.at[1], ydev)
    send("meta_core", meta_v.at[0], meta_v.at[2], core)
    send("meta_far", meta_v.at[0], meta_v.at[3], far)
    send("rows_y", grp.at[0], grp.at[1], ydev)
    send("rows_core", grp.at[0], grp.at[2], core)

    def pack(pos, expert, put):
        places = lax.broadcasted_iota(jnp.int32, (cap, tok), 0) + expert * cap
        places = places.astype(jnp.float32)
        chosen = (places == meta_v[pos, 0:1, :]) | (places == meta_v[pos, 1:2, :])
        chosen = jnp.where(chosen, 1.0, 0.0).astype(jnp.bfloat16)
        for n in range(0, width, col):
            put(
                n,
                jnp.dot(chosen, grp[pos, :, n : n + col], preferred_element_type=jnp.float32).astype(
                    jnp.bfloat16
                ),
            )

    def put_in(ref, *lead):
        def put(n, value):
            ref[(*lead, slice(n, n + col))] = value

        return put

    for d in range(half):
        pack(0, other + (q + d) % half, put_in(pack_a, d, slice(None)))
        send(f"a{d}", pack_a.at[d], xa.at[d, pl.ds(0, cap)], to_a(d))

    def shared_rows(pos):
        x = grp[pos]
        g = jnp.dot(x, sgate_v[...], preferred_element_type=jnp.float32)
        u = jnp.dot(x, sup_v[...], preferred_element_type=jnp.float32)
        h = (jax.nn.silu(g) * u).astype(jnp.bfloat16)
        for n in range(0, width, col):
            sp[pos, :, n : n + col] = jnp.dot(
                h, sdown_v[:, n : n + col], preferred_element_type=jnp.float32
            ).astype(jnp.bfloat16)

    def expert(x_ref, y_ref):
        x = x_ref[...]
        g = jnp.dot(x, gate_v[...], preferred_element_type=jnp.float32)
        u = jnp.dot(x, up_v[...], preferred_element_type=jnp.float32)
        h = (jax.nn.silu(g) * u).astype(jnp.bfloat16)
        for n in range(0, width, col):
            y_ref[:, n : n + col] = jnp.dot(
                h, down_v[:, n : n + col], preferred_element_type=jnp.float32
            ).astype(jnp.bfloat16)

    f32 = jnp.float32

    def a1(d):
        arrived(f"a{d}")
        send(f"ay{d}", xa.at[d, pl.ds(0, cap)], xa.at[d, pl.ds(cap, cap)], ydev)

    def a2(d):
        arrived(f"ay{d}")
        send(f"ac{d}", xa.at[d, pl.ds(0, 2 * cap)], xa.at[d, pl.ds(2 * cap, 2 * cap)], core)

    def a3(d):
        arrived(f"ac{d}")
        expert(xa.at[d], ya.at[d])
        send(f"ra{d}", ya.at[d, pl.ds(2 * cap, 2 * cap)], ra.at[d], core)

    def a4(d):
        arrived(f"ra{d}")
        sa[d] = (ya[d, 0 : 2 * cap].astype(f32) + ra[d].astype(f32)).astype(jnp.bfloat16)
        send(f"ry{d}", sa.at[d, pl.ds(cap, cap)], ry.at[d], ydev)

    def a5(d):
        arrived(f"ry{d}")
        fa[d] = (sa[d, 0:cap].astype(f32) + ry[d].astype(f32)).astype(jnp.bfloat16)
        send(f"fa{d}", fa.at[d], ret_a.at[pl.ds(d * cap, cap)], from_a(d))

    def b1(d):
        for p in range(2):
            pack(p, base + (q + d) % half, put_in(pack_b, d - 1, slice(p * cap, (p + 1) * cap)))
        send(f"b{d}", pack_b.at[d - 1], xb.at[d, pl.ds(0, 2 * cap)], to_b(d))

    def b2(d):
        arrived(f"b{d}")
        send(f"bc{d}", xb.at[d, pl.ds(0, 2 * cap)], xb.at[d, pl.ds(2 * cap, 2 * cap)], core)

    def b3(d):
        if d:
            arrived(f"bc{d}")
        expert(xb.at[d], yb.at[d])
        send(f"rb{d}", yb.at[d, pl.ds(2 * cap, 2 * cap)], rb.at[d], core)

    def b4(d):
        arrived(f"rb{d}")
        for p in range(2):
            at = slice(p * cap, (p + 1) * cap)
            total = (yb[d, at].astype(f32) + rb[d, at].astype(f32)).astype(jnp.bfloat16)
            if d:
                sb[d - 1, p] = total
            else:
                ret_b[p, 0:cap] = total
        if d:
            send(f"fb{d}", sb.at[d - 1], ret_b.at[:, pl.ds(d * cap, cap)], from_b(d))

    def chosen_slots(columns, first):
        lanes = lax.broadcasted_iota(jnp.int32, (1, half * cap), 1)
        code = lanes + (first + q) * cap
        for d in range(1, half):
            moved = (first + (q + d) % half - d) * cap
            code = jnp.where(lanes >= d * cap, lanes + moved, code)
        code = code.astype(f32)
        return [jnp.where(columns[:, k : k + 1] == code, 1.0, 0.0).astype(jnp.bfloat16) for k in range(2)]

    def mixed(columns, picks, returned):
        total = None
        for k in range(2):
            part = columns[:, 2 + k : 3 + k] * jnp.dot(picks[k], returned, preferred_element_type=f32)
            total = part if total is None else total + part
        return total

    def dense_rows(p):
        columns = jnp.transpose(meta_v[p])
        picks = chosen_slots(columns, base)
        for n in range(0, width, col):
            at = slice(n, n + col)
            value = (
                mixed(columns, picks, ret_b[p, :, at])
                + sp[p, :, at].astype(f32)
                + rsp[p, :, at].astype(f32)
            )
            if p:
                dense_s[:, at] = value.astype(jnp.bfloat16)
            else:
                dense[:, at] = value

    loads["sgate"].wait()
    loads["sup"].wait()
    loads["sdown"].wait()
    shared_rows(0)
    loads["mix"].wait()
    send("mix_core", mix_v.at[t_core], mix_r.at[0], core)
    send("mix_far", mix_v.at[t_far], mix_r.at[1], core)
    arrived("meta_y")
    arrived("rows_y")
    send("rows_fwd", grp.at[1], grp.at[3], core)
    for d in range(1, half):
        b1(d)
    arrived("meta_core")
    arrived("meta_far")
    arrived("rows_core")
    shared_rows(1)
    shared_rows(2)
    for p in (0, 1, 2):
        pack(p, e, put_in(xb, 0, slice(p * cap, (p + 1) * cap)))
    a1(0)
    arrived("rows_fwd")
    shared_rows(3)
    send("shared", sp.at[pl.ds(2, 2)], rsp, core)
    pack(3, e, put_in(xb, 0, slice(3 * cap, 4 * cap)))
    loads["gate"].wait()
    loads["up"].wait()
    loads["down"].wait()
    b3(0)
    a2(0)
    b2(1)
    a3(0)
    a1(1)
    b4(0)
    a4(0)
    b3(1)
    a2(1)
    b4(1)
    b2(2)
    a3(1)
    a5(0)
    a1(2)
    a4(1)
    b3(2)
    a2(2)
    b4(2)
    b2(3)
    a3(2)
    a5(1)
    a1(3)
    a4(2)
    b3(3)
    a2(3)
    b4(3)
    a3(3)
    a5(2)
    a4(3)
    a5(3)
    arrived("mix_core")
    arrived("mix_far")
    mix_s[...] = (mix_v[t_y].astype(f32) + mix_r[1].astype(f32)).astype(jnp.bfloat16)
    send("mix_y", mix_s, mix_ry, ydev)
    for d in range(1, half):
        arrived(f"fb{d}")
    arrived("shared")
    dense_rows(1)
    send("dense", dense_s, dense_r, ydev)
    dense_rows(0)
    arrived("mix_y")
    mix_out[...] = (
        mix_v[t].astype(f32) + mix_r[0].astype(f32) + mix_ry[...].astype(f32)
    ).astype(jnp.bfloat16)
    for d in range(half):
        arrived(f"fa{d}")
    arrived("dense")
    columns = jnp.transpose(meta_v[0])
    picks = chosen_slots(columns, other)
    for n in range(0, width, col):
        at = slice(n, n + col)
        value = mixed(columns, picks, ret_a[:, at]) + dense[:, at] + dense_r[:, at].astype(f32)
        moe_out[:, at] = value.astype(jnp.bfloat16)
    for name in copies:
        copies[name].wait_send()


def exchange(ep_count, capacity, rows, meta, gain, mix_term, gate, up, down, sgate, sup, sdown):
    half = ep_count // 2
    tok, width = rows.shape
    bf16, f32 = jnp.bfloat16, jnp.float32
    cap = capacity
    mix_block = mix_term.shape[1]
    count = len(message_names(half))
    shapes = [
        ((tok, width), bf16),
        (mix_term.shape, bf16),
        (gate.shape, bf16),
        (up.shape, bf16),
        (down.shape, bf16),
        (sgate.shape, bf16),
        (sup.shape, bf16),
        (sdown.shape, bf16),
        ((4, 8, tok), f32),
        ((4, tok, width), bf16),
        ((half, cap, width), bf16),
        ((half - 1, 2 * cap, width), bf16),
        ((half, 4 * cap, width), bf16),
        ((half, 4 * cap, width), bf16),
        ((half, 4 * cap, width), bf16),
        ((half, 4 * cap, width), bf16),
        ((half, 2 * cap, width), bf16),
        ((half, 2 * cap, width), bf16),
        ((half, 2 * cap, width), bf16),
        ((half - 1, 2, cap, width), bf16),
        ((half, cap, width), bf16),
        ((half, cap, width), bf16),
        ((half * cap, width), bf16),
        ((2, half * cap, width), bf16),
        ((4, tok, width), bf16),
        ((2, tok, width), bf16),
        ((tok, width), f32),
        ((tok, width), bf16),
        ((tok, width), bf16),
        ((2, mix_block, width), bf16),
        ((mix_block, width), bf16),
        ((mix_block, width), bf16),
    ]
    any_spec = pl.BlockSpec(memory_space=pl.ANY)
    vmem_spec = pl.BlockSpec(memory_space=pltpu.VMEM)
    return pl.pallas_call(
        functools.partial(exchange_kernel, ep_count, capacity),
        out_shape=(
            jax.ShapeDtypeStruct((mix_block, width), bf16),
            jax.ShapeDtypeStruct((tok, width), bf16),
        ),
        in_specs=[any_spec, vmem_spec, vmem_spec] + [any_spec] * 7,
        out_specs=(vmem_spec, vmem_spec),
        scratch_shapes=[pltpu.VMEM(shape, dtype) for shape, dtype in shapes]
        + [
            pltpu.SemaphoreType.DMA((8,)),
            pltpu.SemaphoreType.DMA((count,)),
            pltpu.SemaphoreType.DMA((count,)),
        ],
        compiler_params=pltpu.CompilerParams(
            collective_id=0, has_side_effects=True, vmem_limit_bytes=60 * 1024 * 1024
        ),
        name="moe_exchange",
    )(rows, meta, gain, mix_term, gate, up, down, sgate, sup, sdown)


def direct(
    head_inputs_unfiltered,
    group_write_vectors,
    group_read_vectors,
    output_gate_inputs,
    step_preactivation,
    extra_decay_logs,
    head_decay_logs,
    head_filter_taps,
    write_filter_taps,
    read_filter_taps,
    grouped_norm_gain,
    mixer_output_weight,
    expert_input_rows,
    expert_norm_gain,
    routes,
    router_chosen_scores,
    routed_gate_weight,
    routed_up_weight,
    routed_down_weight,
    shared_gate_weight,
    shared_up_weight,
    shared_down_weight,
):
    tp_count = lax.axis_size("tp")
    ep_count = lax.axis_size("ep")
    tok_local, model_width = expert_input_rows.shape
    experts = ep_count
    capacity = 3 * tok_local * routes.shape[1] // (2 * experts)
    score_float = router_chosen_scores.astype(jnp.float32)
    weights = score_float / jnp.sum(score_float, axis=1, keepdims=True) * route_scale
    choice = routes[None, :, :] == jnp.arange(experts, dtype=jnp.int32)[:, None, None]
    named = jnp.any(choice, axis=2)
    row_order = jnp.arange(tok_local, dtype=jnp.int32)
    earlier_rows = (row_order[:, None] < row_order[None, :]).astype(jnp.bfloat16)
    rank = jnp.dot(named.astype(jnp.bfloat16), earlier_rows, preferred_element_type=jnp.float32)
    place = jnp.sum(jnp.where(choice, rank[:, :, None], 0.0), axis=0) + (routes * capacity).astype(jnp.float32)
    meta = jnp.pad(jnp.concatenate([place.T, weights.T], axis=0), ((0, 4), (0, 0)))

    earlier = tail_rows_from_behind(
        head_inputs_unfiltered, group_write_vectors, group_read_vectors, head_filter_taps.shape[0]
    )
    mixer_normed = mixer_rows(
        earlier,
        head_inputs_unfiltered,
        group_write_vectors,
        group_read_vectors,
        output_gate_inputs,
        step_preactivation,
        extra_decay_logs,
        head_decay_logs,
        head_filter_taps,
        write_filter_taps,
        read_filter_taps,
        grouped_norm_gain,
    )
    mix_block = mixer_normed.shape[0] // tp_count
    mix_term = jnp.dot(
        mixer_normed, mixer_output_weight, preferred_element_type=jnp.float32
    ).astype(jnp.bfloat16).reshape(tp_count, mix_block, model_width)
    return exchange(
        ep_count,
        capacity,
        expert_input_rows,
        meta,
        expert_norm_gain.reshape(1, -1),
        mix_term,
        routed_gate_weight[0],
        routed_up_weight[0],
        routed_down_weight[0],
        shared_gate_weight,
        shared_up_weight,
        shared_down_weight,
    )


def fits_direct(mesh, tok_local, top_count, local_experts):
    ep_count = mesh.shape["ep"]
    experts = ep_count * local_experts
    capacity = 3 * tok_local * top_count // (2 * experts)
    return (
        mesh.shape["tp"] == 4
        and ep_count % 2 == 0
        and ep_count <= 8
        and local_experts == 1
        and top_count == 2
        and capacity % 16 == 0
        and tok_local == 128
    )


def solution(mesh):
    in_specs = (
        P("ep", "tp"),
        P("ep", "tp"),
        P("ep", "tp"),
        P("ep", "tp"),
        P("tp", "ep"),
        P("tp", "ep"),
        P("tp"),
        P(None, "tp"),
        P(None, "tp"),
        P(None, "tp"),
        P("tp"),
        P("tp", None),
        P(("ep", "tp"), None),
        P(),
        P(("ep", "tp"), None),
        P(("ep", "tp"), None),
        P("ep", None, "tp"),
        P("ep", None, "tp"),
        P("ep", "tp", None),
        P(None, "tp"),
        P(None, "tp"),
        P("tp", None),
    )
    out_specs = (P(("ep", "tp"), None), P(("ep", "tp"), None))
    def step(*args):
        devices = mesh.shape["ep"] * mesh.shape["tp"]
        body = (
            direct
            if fits_direct(mesh, args[12].shape[0] // devices, args[14].shape[1], args[16].shape[0] // mesh.shape["ep"])
            else local
        )
        return jax.shard_map(
            body, mesh=mesh, in_specs=in_specs, out_specs=out_specs, check_vma=False
        )(*args)

    return step
```

```python
import functools

import jax
import jax.numpy as jnp
from jax import lax
from jax.experimental import pallas as pl
from jax.experimental.pallas import tpu as pltpu
from jax.sharding import PartitionSpec as P

MESH = pl.DeviceIdType.MESH
HEAD_DIM = 64
STATE = 128
BLOCK = 64


eps_norm = 1e-06
route_scale = 2.5
highest = lax.Precision.HIGHEST


def from_behind(value, axis, by):
    devices = lax.axis_size(axis)
    pairs = [(i, i + by) for i in range(devices) if 0 <= i + by < devices]
    return lax.ppermute(value, axis, pairs)


def sent_state(decay, state, axis, by):
    heads, width = decay.shape[0], state.shape[-1]
    parts, rest = [], decay
    for _ in range(3):
        part = lax.reduce_precision(rest, exponent_bits=8, mantissa_bits=7)
        parts.append(part)
        rest = rest - part
    decay_rows = jnp.pad(jnp.stack(parts, axis=1), ((0, 0), (0, width - 3)))
    packed = jnp.concatenate([state.reshape(-1, width), decay_rows], axis=0).astype(jnp.bfloat16)
    packed = from_behind(packed, axis, by).astype(jnp.float32)
    return jnp.sum(packed[-heads:, :3], axis=-1), packed[:-heads].reshape(state.shape)


def carried_in(decay, state, axis):
    shape = state.shape
    own = (decay.reshape(-1), state.reshape((-1,) + shape[-2:]))
    before, by = None, 1
    while by < lax.axis_size(axis):
        span = own if before is None else combine_states(before, own)
        received = sent_state(*span, axis, by)
        before = received if before is None else combine_states(received, before)
        by *= 2
    if before is None:
        return jnp.zeros_like(state)
    return before[1].reshape(shape)


def combine_states(earlier_part, later_part):
    return (
        earlier_part[0] + later_part[0],
        later_part[1] + jnp.exp(later_part[0])[..., None, None] * earlier_part[1],
    )


def conv_silu(values, weights):
    taps = weights.shape[0]
    length = values.shape[0] - taps + 1
    running_sum = jnp.zeros((length, values.shape[1]), jnp.float32)
    for offset in range(taps):
        running_sum = running_sum + weights[offset].astype(jnp.float32) * values[
            offset : offset + length
        ].astype(jnp.float32)
    return jax.nn.silu(running_sum)


def tail_rows_from_behind(head_inputs, write_vectors, read_vectors, taps):
    start = head_inputs.shape[0] - taps + 1
    tail_rows = jnp.concatenate([head_inputs[start:], write_vectors[start:], read_vectors[start:]], axis=1)
    return from_behind(tail_rows, "ep", 1)


def mixer_rows(
    earlier,
    head_inputs_unfiltered,
    group_write_vectors,
    group_read_vectors,
    output_gate_inputs,
    step_preactivation,
    extra_decay_logs,
    head_decay_logs,
    head_filter_taps,
    write_filter_taps,
    read_filter_taps,
    grouped_norm_gain,
):
    row_total = head_inputs_unfiltered.shape[0]
    head_chans = head_inputs_unfiltered.shape[1]
    write_chans = group_write_vectors.shape[1]
    padded_heads = jnp.concatenate([earlier[:, :head_chans], head_inputs_unfiltered], axis=0)
    padded_write = jnp.concatenate(
        [earlier[:, head_chans : head_chans + write_chans], group_write_vectors], axis=0
    )
    padded_read = jnp.concatenate(
        [earlier[:, head_chans + write_chans :], group_read_vectors], axis=0
    )
    heads_local = step_preactivation.shape[0]
    groups_local = write_chans // STATE
    per_group = heads_local // groups_local
    block_count = row_total // BLOCK
    head_values = conv_silu(padded_heads, head_filter_taps).reshape(
        block_count, BLOCK, groups_local, per_group, HEAD_DIM
    )
    write_values = conv_silu(padded_write, write_filter_taps).reshape(
        block_count, BLOCK, groups_local, STATE
    )
    read_values = conv_silu(padded_read, read_filter_taps).reshape(
        block_count, BLOCK, groups_local, STATE
    )
    step_length_value = jax.nn.softplus(step_preactivation)
    decay_rate_logs = -jnp.exp(head_decay_logs)[:, None] * step_length_value + extra_decay_logs
    step_blocks = step_length_value.reshape(groups_local, per_group, block_count, BLOCK)
    cumulative = jnp.cumsum(
        decay_rate_logs.reshape(groups_local, per_group, block_count, BLOCK), axis=3
    )
    weighted = head_values * jnp.transpose(step_blocks, (2, 3, 0, 1))[..., None]
    lower_mask = jnp.tril(jnp.ones((BLOCK, BLOCK), bool))
    gap_logs = cumulative[..., :, None] - cumulative[..., None, :]
    within = jnp.exp(jnp.where(lower_mask, gap_logs, -jnp.inf))
    affinity = jnp.einsum("blgn,bsgn->gbls", read_values, write_values, precision=highest)
    local_part = jnp.einsum(
        "gebls,bsgep->blgep", affinity[:, None] * within, weighted, precision=highest
    )
    to_end = jnp.exp(cumulative[..., -1:] - cumulative)
    block_states = jnp.einsum(
        "bsgn,bsgep,gebs->bgepn", write_values, weighted, to_end, precision=highest
    )
    block_decay = cumulative[..., -1]
    running = jnp.cumsum(block_decay, axis=2)
    entering = running - block_decay
    earlier_blocks = jnp.tril(jnp.ones((block_count, block_count), bool), -1)
    block_ratio = entering[..., :, None] - running[..., None, :]
    carry_weights = jnp.exp(jnp.where(earlier_blocks, block_ratio, -jnp.inf))
    inside = jnp.einsum("gebc,cgepn->bgepn", carry_weights, block_states, precision=highest)
    device_decay = running[..., -1]
    device_state = jnp.einsum(
        "gec,cgepn->gepn",
        jnp.exp(device_decay[..., None] - running),
        block_states,
        precision=highest,
    )
    incoming = carried_in(device_decay, device_state, "ep")
    states_in = (
        inside + jnp.exp(jnp.transpose(entering, (2, 0, 1)))[..., None, None] * incoming[None]
    )
    carried_part = (
        jnp.einsum("blgn,bgepn->blgep", read_values, states_in, precision=highest)
        * jnp.transpose(jnp.exp(cumulative), (2, 3, 0, 1))[..., None]
    )
    scan_out = (local_part + carried_part).reshape(row_total, groups_local, per_group * HEAD_DIM)
    gate_values = jax.nn.silu(output_gate_inputs.astype(jnp.float32)).reshape(
        row_total, groups_local, per_group * HEAD_DIM
    )
    gated_rows = scan_out * gate_values
    gated_rows = gated_rows * lax.rsqrt(
        jnp.mean(gated_rows * gated_rows, axis=-1, keepdims=True) + eps_norm
    )
    return (gated_rows.reshape(row_total, head_chans) * grouped_norm_gain).astype(jnp.bfloat16)


def local(
    head_inputs_unfiltered,
    group_write_vectors,
    group_read_vectors,
    output_gate_inputs,
    step_preactivation,
    extra_decay_logs,
    head_decay_logs,
    head_filter_taps,
    write_filter_taps,
    read_filter_taps,
    grouped_norm_gain,
    mixer_output_weight,
    expert_input_rows,
    expert_norm_gain,
    routes,
    router_chosen_scores,
    routed_gate_weight,
    routed_up_weight,
    routed_down_weight,
    shared_gate_weight,
    shared_up_weight,
    shared_down_weight,
):
    earlier = tail_rows_from_behind(
        head_inputs_unfiltered, group_write_vectors, group_read_vectors, head_filter_taps.shape[0]
    )
    tp_count = lax.axis_size("tp")
    ep_count = lax.axis_size("ep")
    tok_local = expert_input_rows.shape[0]
    model_width = expert_input_rows.shape[1]
    top_count = routes.shape[1]
    local_experts = routed_gate_weight.shape[0]
    experts = local_experts * ep_count
    capacity = 3 * tok_local * top_count // (2 * experts)
    rows_float = expert_input_rows.astype(jnp.float32)
    normed = (
        rows_float
        * lax.rsqrt(jnp.mean(rows_float * rows_float, axis=-1, keepdims=True) + eps_norm)
        * expert_norm_gain
    ).astype(jnp.bfloat16)
    score_float = router_chosen_scores.astype(jnp.float32)
    weights = score_float / jnp.sum(score_float, axis=1, keepdims=True) * route_scale
    choice = routes[None, :, :] == jnp.arange(experts, dtype=jnp.int32)[:, None, None]
    named = jnp.any(choice, axis=2)
    weight_of = jnp.sum(jnp.where(choice, weights[None], 0.0), axis=2)
    row_order = jnp.arange(tok_local, dtype=jnp.int32)
    earlier_rows = (row_order[:, None] < row_order[None, :]).astype(jnp.bfloat16)
    rank = jnp.dot(
        named.astype(jnp.bfloat16), earlier_rows, preferred_element_type=jnp.float32
    ).astype(jnp.int32)

    cuts = [0, capacity // 2, capacity] if capacity > 1 else [0, capacity]
    picks, outgoing = [], []
    for low, high in zip(cuts[:-1], cuts[1:]):
        places = jnp.arange(low, high, dtype=jnp.int32)
        picked = named[:, None, :] & (rank[:, None, :] == places[None, :, None])
        picks.append(picked)
        outgoing.append(
            jnp.dot(
                picked.reshape(-1, tok_local).astype(jnp.bfloat16),
                normed,
                preferred_element_type=jnp.float32,
            ).astype(jnp.bfloat16)
        )
    group_rows = lax.all_gather(normed, "tp", axis=0, tiled=True)
    earlier, group_rows, outgoing[0] = lax.optimization_barrier((earlier, group_rows, outgoing[0]))

    arrived = []
    for block in outgoing:
        arrived.append(lax.all_to_all(block, "ep", split_axis=0, concat_axis=0, tiled=True))
    gathered = [lax.all_gather(block, "tp", axis=0) for block in arrived]

    shared_hidden = (
        jax.nn.silu(jnp.dot(group_rows, shared_gate_weight, preferred_element_type=jnp.float32))
        * jnp.dot(group_rows, shared_up_weight, preferred_element_type=jnp.float32)
    ).astype(jnp.bfloat16)
    shared_part = jnp.dot(shared_hidden, shared_down_weight, preferred_element_type=jnp.float32)

    mixer_normed = mixer_rows(
        earlier,
        head_inputs_unfiltered,
        group_write_vectors,
        group_read_vectors,
        output_gate_inputs,
        step_preactivation,
        extra_decay_logs,
        head_decay_logs,
        head_filter_taps,
        write_filter_taps,
        read_filter_taps,
        grouped_norm_gain,
    )

    def expert_rows(block):
        sources = block.reshape(tp_count, ep_count, local_experts, -1, model_width)
        gate_value = jnp.einsum(
            "osecd,edf->osecf", sources, routed_gate_weight, preferred_element_type=jnp.float32
        )
        up_value = jnp.einsum(
            "osecd,edf->osecf", sources, routed_up_weight, preferred_element_type=jnp.float32
        )
        hidden = (jax.nn.silu(gate_value) * up_value).astype(jnp.bfloat16)
        partial_value = jnp.einsum(
            "osecf,efd->osecd", hidden, routed_down_weight, preferred_element_type=jnp.float32
        ).astype(jnp.bfloat16)
        return lax.psum_scatter(
            partial_value.reshape(-1, model_width), "tp", scatter_dimension=0, tiled=True
        )

    own_term = jnp.zeros((tok_local, model_width), jnp.float32)
    for block, picked in zip(gathered, picks):
        returned = lax.all_to_all(
            expert_rows(block), "ep", split_axis=0, concat_axis=0, tiled=True
        )
        mixing = jnp.where(picked, weight_of[:, None, :], 0.0).reshape(-1, tok_local)
        own_term = own_term + jnp.einsum(
            "sr,sd->rd", mixing, returned.astype(jnp.float32), precision=highest
        )
    mix_block = mixer_normed.shape[0] // tp_count
    block_rows = mix_block + tok_local
    mix_term = jnp.dot(
        mixer_normed, mixer_output_weight, preferred_element_type=jnp.float32
    ).astype(jnp.bfloat16).reshape(tp_count, mix_block, model_width)
    moe_term = shared_part.astype(jnp.bfloat16).reshape(tp_count, tok_local, model_width)
    row_sums = lax.psum_scatter(
        jnp.concatenate([mix_term, moe_term], axis=1).reshape(tp_count * block_rows, model_width),
        "tp",
        scatter_dimension=0,
        tiled=True,
    )
    mixer_result = row_sums[:mix_block]
    moe_total = row_sums[mix_block:].astype(jnp.float32) + own_term
    return (mixer_result.astype(jnp.bfloat16), moe_total.astype(jnp.bfloat16))


def message_names(half):
    names = ["meta_core", "meta_y", "meta_far", "rows_core", "rows_y", "rows_fwd", "shared", "dense", "mix_core", "mix_far", "mix_y"]
    names += ["halo_h", "halo_w", "halo_r"]
    for r in range((2 * half - 1).bit_length()):
        names += [f"state{r}", f"decay{r}"]
    for d in range(half):
        names += [f"{kind}{d}" for kind in ("a", "ay", "ac", "ra", "ry", "fa", "b", "bc", "rb", "fb")]
    return {name: i for i, name in enumerate(names)}


def exchange_kernel(
    ep_count,
    capacity,
    rows_hbm,
    meta_ref,
    gain_ref,
    heads_hbm,
    write_hbm,
    read_hbm,
    ogate_hbm,
    proj_hbm,
    step_ref,
    extra_ref,
    decay_ref,
    htaps_ref,
    wtaps_ref,
    rtaps_ref,
    mgain_ref,
    gate_hbm,
    up_hbm,
    down_hbm,
    sgate_hbm,
    sup_hbm,
    sdown_hbm,
    mix_out,
    moe_out,
    rows_v,
    mix_v,
    heads_v,
    write_v,
    read_v,
    ogate_v,
    proj_v,
    halo_h,
    halo_w,
    halo_r,
    ext_h,
    ext_w,
    ext_r,
    hval,
    y_v,
    read_b,
    grow_v,
    own_s,
    own_d,
    bef_s,
    bef_d,
    out_s,
    out_d,
    in_s,
    in_d,
    gate_v,
    up_v,
    down_v,
    sgate_v,
    sup_v,
    sdown_v,
    meta_v,
    grp,
    pack_a,
    pack_b,
    xa,
    xb,
    ya,
    yb,
    ra,
    rb,
    sa,
    sb,
    ry,
    fa,
    ret_a,
    ret_b,
    sp,
    rsp,
    dense,
    dense_s,
    dense_r,
    mix_r,
    mix_s,
    mix_ry,
    load_sem,
    send_sem,
    recv_sem,
):
    half = ep_count // 2
    cap = capacity
    tok, width = rows_v.shape
    tok_m, chans = heads_v.shape
    heads = step_ref.shape[0]
    head_dim = chans // heads
    col = 512
    ids = message_names(half)
    e = lax.axis_index("ep")
    t = lax.axis_index("tp")
    base = (e // half) * half
    q = e - base
    other = half - base
    t_core = t + 1 - 2 * (t % 2)
    t_y = (t + 2) % 4
    t_far = (t_core + 2) % 4
    core, ydev, far = (e, t_core), (e, t_y), (e, t_far)

    def to_a(d):
        return (other + (q + d) % half, t)

    def from_a(d):
        return (other + (q + half - d) % half, t)

    def to_b(d):
        return (base + (q + d) % half, t)

    def from_b(d):
        return (base + (q + half - d) % half, t)

    loads = {}
    for i, (name, src, dst) in enumerate(
        (
            ("rows", rows_hbm, rows_v),
            ("sgate", sgate_hbm, sgate_v),
            ("sup", sup_hbm, sup_v),
            ("sdown", sdown_hbm, sdown_v),
            ("gate", gate_hbm, gate_v),
            ("up", up_hbm, up_v),
            ("down", down_hbm, down_v),
            ("heads", heads_hbm, heads_v),
            ("write", write_hbm, write_v),
            ("read", read_hbm, read_v),
            ("ogate", ogate_hbm, ogate_v),
            ("proj", proj_hbm, proj_v),
        )
    ):
        loads[name] = pltpu.make_async_copy(src, dst, load_sem.at[i])
        loads[name].start()

    copies = {}

    def prepare(name, src, dst, device):
        i = ids[name]
        copies[name] = pltpu.make_async_remote_copy(
            src_ref=src,
            dst_ref=dst,
            send_sem=send_sem.at[i],
            recv_sem=recv_sem.at[i],
            device_id=device,
            device_id_type=MESH,
        )

    def send(name, src, dst, device):
        prepare(name, src, dst, device)
        copies[name].start()

    def arrived(name):
        copies[name].wait_recv()

    barrier = pltpu.get_barrier_semaphore()
    peers = [core, ydev, far] + [to_a(d) for d in range(half)] + [to_b(d) for d in range(1, half)]
    for peer in peers:
        pl.semaphore_signal(barrier, inc=1, device_id=peer, device_id_type=MESH)

    meta_v[0] = meta_ref[...]
    f32, bf16 = jnp.float32, jnp.bfloat16
    loads["rows"].wait()

    def norm_rows(i, carry):
        at = pl.ds(pl.multiple_of(i * 16, 16), 16)
        x = rows_v[at, :].astype(jnp.float32)
        scale = lax.rsqrt(jnp.mean(x * x, axis=-1, keepdims=True) + eps_norm)
        grp[0, at, :] = (x * scale * gain_ref[...]).astype(jnp.bfloat16)
        return carry

    lax.fori_loop(0, tok // 16, norm_rows, 0)
    pl.semaphore_wait(barrier, len(peers))

    send("meta_y", meta_v.at[0], meta_v.at[1], ydev)
    send("meta_core", meta_v.at[0], meta_v.at[2], core)
    send("meta_far", meta_v.at[0], meta_v.at[3], far)
    send("rows_y", grp.at[0], grp.at[1], ydev)
    send("rows_core", grp.at[0], grp.at[2], core)


    nxt = ((e + 1) % ep_count, t)
    halo_rows = halo_h.shape[0]
    tail = pl.ds(tok_m - halo_rows, halo_rows)
    for name in ("heads", "write", "read"):
        loads[name].wait()
    send("halo_h", heads_v.at[tail], halo_h, nxt)
    send("halo_w", write_v.at[tail], halo_w, nxt)
    send("halo_r", read_v.at[tail], halo_r, nxt)

    def pack(pos, expert, put):
        places = lax.broadcasted_iota(jnp.int32, (cap, tok), 0) + expert * cap
        places = places.astype(jnp.float32)
        chosen = (places == meta_v[pos, 0:1, :]) | (places == meta_v[pos, 1:2, :])
        chosen = jnp.where(chosen, 1.0, 0.0).astype(jnp.bfloat16)
        for n in range(0, width, col):
            put(
                n,
                jnp.dot(chosen, grp[pos, :, n : n + col], preferred_element_type=jnp.float32).astype(
                    jnp.bfloat16
                ),
            )

    def put_in(ref, *lead):
        def put(n, value):
            ref[(*lead, slice(n, n + col))] = value

        return put

    for d in range(half):
        pack(0, other + (q + d) % half, put_in(pack_a, d, slice(None)))
        send(f"a{d}", pack_a.at[d], xa.at[d, pl.ds(0, cap)], to_a(d))

    def shared_rows(pos):
        x = grp[pos]
        g = jnp.dot(x, sgate_v[...], preferred_element_type=jnp.float32)
        u = jnp.dot(x, sup_v[...], preferred_element_type=jnp.float32)
        h = (jax.nn.silu(g) * u).astype(jnp.bfloat16)
        for n in range(0, width, col):
            sp[pos, :, n : n + col] = jnp.dot(
                h, sdown_v[:, n : n + col], preferred_element_type=jnp.float32
            ).astype(jnp.bfloat16)

    def expert(x_ref, y_ref):
        x = x_ref[...]
        g = jnp.dot(x, gate_v[...], preferred_element_type=jnp.float32)
        u = jnp.dot(x, up_v[...], preferred_element_type=jnp.float32)
        h = (jax.nn.silu(g) * u).astype(jnp.bfloat16)
        for n in range(0, width, col):
            y_ref[:, n : n + col] = jnp.dot(
                h, down_v[:, n : n + col], preferred_element_type=jnp.float32
            ).astype(jnp.bfloat16)

    def a1(d):
        arrived(f"a{d}")
        send(f"ay{d}", xa.at[d, pl.ds(0, cap)], xa.at[d, pl.ds(cap, cap)], ydev)

    def a2(d):
        arrived(f"ay{d}")
        send(f"ac{d}", xa.at[d, pl.ds(0, 2 * cap)], xa.at[d, pl.ds(2 * cap, 2 * cap)], core)

    def a3(d):
        arrived(f"ac{d}")
        expert(xa.at[d], ya.at[d])
        send(f"ra{d}", ya.at[d, pl.ds(2 * cap, 2 * cap)], ra.at[d], core)

    def a4(d):
        arrived(f"ra{d}")
        sa[d] = (ya[d, 0 : 2 * cap].astype(f32) + ra[d].astype(f32)).astype(jnp.bfloat16)
        send(f"ry{d}", sa.at[d, pl.ds(cap, cap)], ry.at[d], ydev)

    def a5(d):
        arrived(f"ry{d}")
        fa[d] = (sa[d, 0:cap].astype(f32) + ry[d].astype(f32)).astype(jnp.bfloat16)
        send(f"fa{d}", fa.at[d], ret_a.at[pl.ds(d * cap, cap)], from_a(d))

    def b1(d):
        for p in range(2):
            pack(p, base + (q + d) % half, put_in(pack_b, d - 1, slice(p * cap, (p + 1) * cap)))
        send(f"b{d}", pack_b.at[d - 1], xb.at[d, pl.ds(0, 2 * cap)], to_b(d))

    def b2(d):
        arrived(f"b{d}")
        send(f"bc{d}", xb.at[d, pl.ds(0, 2 * cap)], xb.at[d, pl.ds(2 * cap, 2 * cap)], core)

    def b3(d):
        if d:
            arrived(f"bc{d}")
        expert(xb.at[d], yb.at[d])
        send(f"rb{d}", yb.at[d, pl.ds(2 * cap, 2 * cap)], rb.at[d], core)

    def b4(d):
        arrived(f"rb{d}")
        for p in range(2):
            at = slice(p * cap, (p + 1) * cap)
            total = (yb[d, at].astype(f32) + rb[d, at].astype(f32)).astype(jnp.bfloat16)
            if d:
                sb[d - 1, p] = total
            else:
                ret_b[p, 0:cap] = total
        if d:
            send(f"fb{d}", sb.at[d - 1], ret_b.at[:, pl.ds(d * cap, cap)], from_b(d))

    def chosen_slots(columns, first):
        lanes = lax.broadcasted_iota(jnp.int32, (1, half * cap), 1)
        code = lanes + (first + q) * cap
        for d in range(1, half):
            moved = (first + (q + d) % half - d) * cap
            code = jnp.where(lanes >= d * cap, lanes + moved, code)
        code = code.astype(f32)
        return [jnp.where(columns[:, k : k + 1] == code, 1.0, 0.0).astype(jnp.bfloat16) for k in range(2)]

    def mixed(columns, picks, returned):
        total = None
        for k in range(2):
            part = columns[:, 2 + k : 3 + k] * jnp.dot(picks[k], returned, preferred_element_type=f32)
            total = part if total is None else total + part
        return total

    def dense_rows(p):
        columns = jnp.transpose(meta_v[p])
        picks = chosen_slots(columns, base)
        for n in range(0, width, col):
            at = slice(n, n + col)
            value = (
                mixed(columns, picks, ret_b[p, :, at])
                + sp[p, :, at].astype(f32)
                + rsp[p, :, at].astype(f32)
            )
            if p:
                dense_s[:, at] = value.astype(jnp.bfloat16)
            else:
                dense[:, at] = value


    def conv(x_v, halo, ext, taps_ref, n, size):
        at = slice(n, n + size)
        taps = taps_ref.shape[0]
        edge = ext.shape[0] - tok_m
        first = halo.shape[0] - edge
        there = jnp.where(e > 0, 1.0, 0.0).astype(f32)
        ext[0:edge, at] = halo[first:, at].astype(f32) * there
        ext[edge:, at] = x_v[:, at].astype(f32)
        total = None
        for j in range(taps):
            low = edge - taps + 1 + j
            part = taps_ref[j : j + 1, at].astype(f32) * ext[low : low + tok_m, at]
            total = part if total is None else total + part
        return jax.nn.silu(total)

    head_row = lax.broadcasted_iota(jnp.int32, (heads, chans), 0)
    lane_head = lax.broadcasted_iota(jnp.int32, (heads, chans), 1) - head_row * head_dim
    spread_b = jnp.where((lane_head >= 0) & (lane_head < head_dim), 1.0, 0.0).astype(bf16)

    def spread(value, terms):
        total, rest = None, value
        for _ in range(terms):
            part = rest.astype(bf16)
            rest = rest - part.astype(f32)
            add = jnp.dot(part, spread_b, preferred_element_type=f32)
            total = add if total is None else total + add
        return total

    def mixer_local():
        for name in ("halo_h", "halo_w", "halo_r"):
            arrived(name)
        for n in range(0, chans, 256):
            hval[:, n : n + 256] = conv(heads_v, halo_h, ext_h, htaps_ref, n, 256)
        states = write_v.shape[1]
        write = conv(write_v, halo_w, ext_w, wtaps_ref, 0, states)
        read = conv(read_v, halo_r, ext_r, rtaps_ref, 0, states)
        read_b[...] = read.astype(bf16)
        step = jax.nn.softplus(step_ref[...])
        rate = step * -jnp.exp(decay_ref[...]) + extra_ref[...]
        row = lax.broadcasted_iota(jnp.int32, (tok_m, tok_m), 0)
        lane = lax.broadcasted_iota(jnp.int32, (tok_m, tok_m), 1)
        upto = jnp.where(row <= lane, 1.0, 0.0).astype(f32)
        cum = jnp.dot(rate, upto, precision=highest, preferred_element_type=f32)
        cum_t = jnp.transpose(cum)
        to_end = jnp.exp(cum[:, tok_m - 1 : tok_m] - cum) * step
        affinity = lax.dot_general(
            read, write, (((1,), (1,)), ((), ())), precision=highest, preferred_element_type=f32
        )
        weights = spread(jnp.transpose(to_end), 2)
        weighted = (hval[...] * weights).astype(bf16)
        own_s[...] = jnp.dot(
            jnp.transpose(write).astype(bf16), weighted, preferred_element_type=f32
        )
        own_d[...] = jnp.broadcast_to(spread(cum_t[tok_m - 8 : tok_m], 3)[7:8], own_d.shape)
        state_send(0)
        grow_v[...] = spread(jnp.exp(cum_t), 2)
        causal = row >= lane
        for pair in range(heads // 2):
            at = slice(pair * 2 * head_dim, (pair + 1) * 2 * head_dim)
            parts = []
            for h in (2 * pair, 2 * pair + 1):
                gap = jnp.where(causal, cum_t[:, h : h + 1] - cum[h : h + 1, :], -jnp.inf)
                parts.append((affinity * jnp.exp(gap) * step[h : h + 1, :]).astype(bf16))
            both = hval[:, at].astype(bf16)
            side = lax.broadcasted_iota(jnp.int32, both.shape, 1) < head_dim
            zero = jnp.zeros_like(both)
            y_v[:, at] = jnp.dot(
                parts[0], jnp.where(side, both, zero), preferred_element_type=f32
            ) + jnp.dot(parts[1], jnp.where(side, zero, both), preferred_element_type=f32)

    rounds = (ep_count - 1).bit_length()

    def state_send(r):
        by = 2**r
        if r == 0:
            out_s[r] = own_s[...].astype(bf16)
            out_d[r] = own_d[...]
        else:
            grown = jnp.exp(own_d[0:1, :])
            out_s[r] = (own_s[...] + grown * bef_s[...]).astype(bf16)
            out_d[r] = own_d[...] + bef_d[...]

        later = ((e + by) % ep_count, t)
        prepare(f"state{r}", out_s.at[r], in_s.at[r], later)
        prepare(f"decay{r}", out_d.at[r], in_d.at[r], later)

        @pl.when(e + by < ep_count)
        def _():
            copies[f"state{r}"].start()
            copies[f"decay{r}"].start()

    def state_arrive(r):
        by = 2**r

        @pl.when(e < by)
        def _():
            in_s[r] = jnp.zeros(in_s.shape[1:], bf16)
            in_d[r] = jnp.zeros(in_d.shape[1:], f32)

        @pl.when(e >= by)
        def _():
            arrived(f"state{r}")
            arrived(f"decay{r}")

        if r == 0:
            bef_s[...] = in_s[0].astype(f32)
            bef_d[...] = in_d[0]
        else:
            bef_s[...] = bef_s[...] + jnp.exp(bef_d[0:1, :]) * in_s[r].astype(f32)
            bef_d[...] = bef_d[...] + in_d[r]
        if r + 1 < rounds:
            state_send(r + 1)

    def mixer_finish():
        square = jnp.zeros((tok_m, 1), f32)
        for n in range(0, chans, 256):
            at = slice(n, n + 256)
            carried = jnp.dot(read_b[...], bef_s[:, at].astype(bf16), preferred_element_type=f32)
            value = (y_v[:, at] + carried * grow_v[:, at]) * jax.nn.silu(ogate_v[:, at].astype(f32))
            y_v[:, at] = value
            square = square + jnp.sum(value * value, axis=-1, keepdims=True)
        scale = lax.rsqrt(square / chans + eps_norm)
        normed = (y_v[...] * scale * mgain_ref[...]).astype(bf16)
        block = mix_v.shape[1]
        for n in range(0, width, col):
            part = jnp.dot(normed, proj_v[:, n : n + col], preferred_element_type=f32).astype(bf16)
            for i in range(4):
                mix_v[i, :, n : n + col] = part[i * block : (i + 1) * block]
        send("mix_core", mix_v.at[t_core], mix_r.at[0], core)
        send("mix_far", mix_v.at[t_far], mix_r.at[1], core)

    loads["sgate"].wait()
    loads["sup"].wait()
    loads["sdown"].wait()
    shared_rows(0)
    mixer_local()
    arrived("meta_y")
    arrived("rows_y")
    send("rows_fwd", grp.at[1], grp.at[3], core)
    for d in range(1, half):
        b1(d)
    arrived("meta_core")
    arrived("meta_far")
    arrived("rows_core")
    a1(0)
    shared_rows(1)
    shared_rows(2)
    for p in (0, 1, 2):
        pack(p, e, put_in(xb, 0, slice(p * cap, (p + 1) * cap)))
    arrived("rows_fwd")
    shared_rows(3)
    send("shared", sp.at[pl.ds(2, 2)], rsp, core)
    pack(3, e, put_in(xb, 0, slice(3 * cap, 4 * cap)))
    a2(0)
    loads["gate"].wait()
    loads["up"].wait()
    loads["down"].wait()
    b3(0)
    state_arrive(0)
    a3(0)
    a1(1)
    b2(1)
    b4(0)
    a4(0)
    b3(1)
    a2(1)
    b4(1)
    b2(2)
    a3(1)
    a5(0)
    state_arrive(1)
    a1(2)
    a4(1)
    b3(2)
    a2(2)
    b4(2)
    b2(3)
    a3(2)
    a5(1)
    a1(3)
    a4(2)
    b3(3)
    a2(3)
    b4(3)
    state_arrive(2)
    a3(3)
    a5(2)
    loads["ogate"].wait()
    loads["proj"].wait()
    mixer_finish()
    a4(3)
    a5(3)
    arrived("mix_core")
    arrived("mix_far")
    mix_s[...] = (mix_v[t_y].astype(f32) + mix_r[1].astype(f32)).astype(jnp.bfloat16)
    send("mix_y", mix_s, mix_ry, ydev)
    for d in range(1, half):
        arrived(f"fb{d}")
    arrived("shared")
    dense_rows(1)
    send("dense", dense_s, dense_r, ydev)
    dense_rows(0)
    arrived("mix_y")
    mix_out[...] = (
        mix_v[t].astype(f32) + mix_r[0].astype(f32) + mix_ry[...].astype(f32)
    ).astype(jnp.bfloat16)
    for d in range(half):
        arrived(f"fa{d}")
    arrived("dense")
    columns = jnp.transpose(meta_v[0])
    picks = chosen_slots(columns, other)
    for n in range(0, width, col):
        at = slice(n, n + col)
        value = mixed(columns, picks, ret_a[:, at]) + dense[:, at] + dense_r[:, at].astype(f32)
        moe_out[:, at] = value.astype(jnp.bfloat16)
    for r in range(rounds):

        @pl.when(e + 2**r < ep_count)
        def _():
            copies[f"state{r}"].wait_send()
            copies[f"decay{r}"].wait_send()

    for name in copies:
        if not name.startswith(("state", "decay")):
            copies[name].wait_send()


def exchange(ep_count, capacity, small, large):
    (rows, heads, write, read, ogate, proj, gate, up, down, sgate, sup, sdown) = large
    half = ep_count // 2
    tok, width = rows.shape
    bf16, f32 = jnp.bfloat16, jnp.float32
    cap = capacity
    tok_m, chans = heads.shape
    state = write.shape[1]
    mix_block = tok_m // 4
    count = len(message_names(half))
    rounds = (ep_count - 1).bit_length()
    shapes = [
        ((tok, width), bf16),
        ((4, mix_block, width), bf16),
        (heads.shape, bf16),
        (write.shape, bf16),
        (read.shape, bf16),
        (ogate.shape, bf16),
        (proj.shape, bf16),
        ((16, chans), bf16),
        ((16, state), bf16),
        ((16, state), bf16),
        ((tok_m + 8, chans), f32),
        ((tok_m + 8, state), f32),
        ((tok_m + 8, state), f32),
        ((tok_m, chans), f32),
        ((tok_m, chans), f32),
        ((tok_m, state), bf16),
        ((tok_m, chans), f32),
        ((state, chans), f32),
        ((8, chans), f32),
        ((state, chans), f32),
        ((8, chans), f32),
        ((rounds, state, chans), bf16),
        ((rounds, 8, chans), f32),
        ((rounds, state, chans), bf16),
        ((rounds, 8, chans), f32),
        (gate.shape, bf16),
        (up.shape, bf16),
        (down.shape, bf16),
        (sgate.shape, bf16),
        (sup.shape, bf16),
        (sdown.shape, bf16),
        ((4, 8, tok), f32),
        ((4, tok, width), bf16),
        ((half, cap, width), bf16),
        ((half - 1, 2 * cap, width), bf16),
        ((half, 4 * cap, width), bf16),
        ((half, 4 * cap, width), bf16),
        ((half, 4 * cap, width), bf16),
        ((half, 4 * cap, width), bf16),
        ((half, 2 * cap, width), bf16),
        ((half, 2 * cap, width), bf16),
        ((half, 2 * cap, width), bf16),
        ((half - 1, 2, cap, width), bf16),
        ((half, cap, width), bf16),
        ((half, cap, width), bf16),
        ((half * cap, width), bf16),
        ((2, half * cap, width), bf16),
        ((4, tok, width), bf16),
        ((2, tok, width), bf16),
        ((tok, width), f32),
        ((tok, width), bf16),
        ((tok, width), bf16),
        ((2, mix_block, width), bf16),
        ((mix_block, width), bf16),
        ((mix_block, width), bf16),
    ]
    any_spec = pl.BlockSpec(memory_space=pl.ANY)
    vmem_spec = pl.BlockSpec(memory_space=pltpu.VMEM)
    return pl.pallas_call(
        functools.partial(exchange_kernel, ep_count, capacity),
        out_shape=(
            jax.ShapeDtypeStruct((mix_block, width), bf16),
            jax.ShapeDtypeStruct((tok, width), bf16),
        ),
        in_specs=[any_spec] + [vmem_spec] * 2 + [any_spec] * 5 + [vmem_spec] * 7 + [any_spec] * 6,
        out_specs=(vmem_spec, vmem_spec),
        scratch_shapes=[pltpu.VMEM(shape, dtype) for shape, dtype in shapes]
        + [
            pltpu.SemaphoreType.DMA((12,)),
            pltpu.SemaphoreType.DMA((count,)),
            pltpu.SemaphoreType.DMA((count,)),
        ],
        compiler_params=pltpu.CompilerParams(
            collective_id=0, has_side_effects=True, vmem_limit_bytes=62 * 1024 * 1024
        ),
        name="mixer_and_experts",
    )(rows, *small[:2], heads, write, read, ogate, proj, *small[2:], gate, up, down, sgate, sup, sdown)


def direct(
    head_inputs_unfiltered,
    group_write_vectors,
    group_read_vectors,
    output_gate_inputs,
    step_preactivation,
    extra_decay_logs,
    head_decay_logs,
    head_filter_taps,
    write_filter_taps,
    read_filter_taps,
    grouped_norm_gain,
    mixer_output_weight,
    expert_input_rows,
    expert_norm_gain,
    routes,
    router_chosen_scores,
    routed_gate_weight,
    routed_up_weight,
    routed_down_weight,
    shared_gate_weight,
    shared_up_weight,
    shared_down_weight,
):
    ep_count = lax.axis_size("ep")
    tok_local = expert_input_rows.shape[0]
    experts = ep_count
    capacity = 3 * tok_local * routes.shape[1] // (2 * experts)
    score_float = router_chosen_scores.astype(jnp.float32)
    weights = score_float / jnp.sum(score_float, axis=1, keepdims=True) * route_scale
    choice = routes[None, :, :] == jnp.arange(experts, dtype=jnp.int32)[:, None, None]
    named = jnp.any(choice, axis=2)
    row_order = jnp.arange(tok_local, dtype=jnp.int32)
    earlier_rows = (row_order[:, None] < row_order[None, :]).astype(jnp.bfloat16)
    rank = jnp.dot(named.astype(jnp.bfloat16), earlier_rows, preferred_element_type=jnp.float32)
    place = jnp.sum(jnp.where(choice, rank[:, :, None], 0.0), axis=0) + (routes * capacity).astype(jnp.float32)
    meta = jnp.pad(jnp.concatenate([place.T, weights.T], axis=0), ((0, 4), (0, 0)))

    small = (
        meta,
        expert_norm_gain.reshape(1, -1),
        step_preactivation,
        extra_decay_logs,
        head_decay_logs.reshape(-1, 1),
        head_filter_taps,
        write_filter_taps,
        read_filter_taps,
        grouped_norm_gain.reshape(1, -1),
    )
    large = (
        expert_input_rows,
        head_inputs_unfiltered,
        group_write_vectors,
        group_read_vectors,
        output_gate_inputs,
        mixer_output_weight,
        routed_gate_weight[0],
        routed_up_weight[0],
        routed_down_weight[0],
        shared_gate_weight,
        shared_up_weight,
        shared_down_weight,
    )
    return exchange(ep_count, capacity, small, large)


def fits_direct(mesh, tok_local, top_count, local_experts):
    ep_count = mesh.shape["ep"]
    experts = ep_count * local_experts
    capacity = 3 * tok_local * top_count // (2 * experts)
    return (
        mesh.shape["tp"] == 4
        and ep_count % 2 == 0
        and ep_count <= 8
        and local_experts == 1
        and top_count == 2
        and capacity % 16 == 0
        and tok_local == 128
    )


def solution(mesh):
    in_specs = (
        P("ep", "tp"),
        P("ep", "tp"),
        P("ep", "tp"),
        P("ep", "tp"),
        P("tp", "ep"),
        P("tp", "ep"),
        P("tp"),
        P(None, "tp"),
        P(None, "tp"),
        P(None, "tp"),
        P("tp"),
        P("tp", None),
        P(("ep", "tp"), None),
        P(),
        P(("ep", "tp"), None),
        P(("ep", "tp"), None),
        P("ep", None, "tp"),
        P("ep", None, "tp"),
        P("ep", "tp", None),
        P(None, "tp"),
        P(None, "tp"),
        P("tp", None),
    )
    out_specs = (P(("ep", "tp"), None), P(("ep", "tp"), None))
    def step(*args):
        devices = mesh.shape["ep"] * mesh.shape["tp"]
        body = (
            direct
            if fits_direct(mesh, args[12].shape[0] // devices, args[14].shape[1], args[16].shape[0] // mesh.shape["ep"])
            else local
        )
        return jax.shard_map(
            body, mesh=mesh, in_specs=in_specs, out_specs=out_specs, check_vma=False
        )(*args)

    return step
```

```python
import functools

import jax
import jax.numpy as jnp
from jax import lax
from jax.experimental import pallas as pl
from jax.experimental.pallas import tpu as pltpu
from jax.sharding import PartitionSpec as P

MESH = pl.DeviceIdType.MESH
HEAD_DIM = 64
STATE = 128
BLOCK = 64


eps_norm = 1e-06
route_scale = 2.5
highest = lax.Precision.HIGHEST


def from_behind(value, axis, by):
    devices = lax.axis_size(axis)
    pairs = [(i, i + by) for i in range(devices) if 0 <= i + by < devices]
    return lax.ppermute(value, axis, pairs)


def sent_state(decay, state, axis, by):
    heads, width = decay.shape[0], state.shape[-1]
    parts, rest = [], decay
    for _ in range(3):
        part = lax.reduce_precision(rest, exponent_bits=8, mantissa_bits=7)
        parts.append(part)
        rest = rest - part
    decay_rows = jnp.pad(jnp.stack(parts, axis=1), ((0, 0), (0, width - 3)))
    packed = jnp.concatenate([state.reshape(-1, width), decay_rows], axis=0).astype(jnp.bfloat16)
    packed = from_behind(packed, axis, by).astype(jnp.float32)
    return jnp.sum(packed[-heads:, :3], axis=-1), packed[:-heads].reshape(state.shape)


def carried_in(decay, state, axis):
    shape = state.shape
    own = (decay.reshape(-1), state.reshape((-1,) + shape[-2:]))
    before, by = None, 1
    while by < lax.axis_size(axis):
        span = own if before is None else combine_states(before, own)
        received = sent_state(*span, axis, by)
        before = received if before is None else combine_states(received, before)
        by *= 2
    if before is None:
        return jnp.zeros_like(state)
    return before[1].reshape(shape)


def combine_states(earlier_part, later_part):
    return (
        earlier_part[0] + later_part[0],
        later_part[1] + jnp.exp(later_part[0])[..., None, None] * earlier_part[1],
    )


def conv_silu(values, weights):
    taps = weights.shape[0]
    length = values.shape[0] - taps + 1
    running_sum = jnp.zeros((length, values.shape[1]), jnp.float32)
    for offset in range(taps):
        running_sum = running_sum + weights[offset].astype(jnp.float32) * values[
            offset : offset + length
        ].astype(jnp.float32)
    return jax.nn.silu(running_sum)


def tail_rows_from_behind(head_inputs, write_vectors, read_vectors, taps):
    start = head_inputs.shape[0] - taps + 1
    tail_rows = jnp.concatenate([head_inputs[start:], write_vectors[start:], read_vectors[start:]], axis=1)
    return from_behind(tail_rows, "ep", 1)


def mixer_rows(
    earlier,
    head_inputs_unfiltered,
    group_write_vectors,
    group_read_vectors,
    output_gate_inputs,
    step_preactivation,
    extra_decay_logs,
    head_decay_logs,
    head_filter_taps,
    write_filter_taps,
    read_filter_taps,
    grouped_norm_gain,
):
    row_total = head_inputs_unfiltered.shape[0]
    head_chans = head_inputs_unfiltered.shape[1]
    write_chans = group_write_vectors.shape[1]
    padded_heads = jnp.concatenate([earlier[:, :head_chans], head_inputs_unfiltered], axis=0)
    padded_write = jnp.concatenate(
        [earlier[:, head_chans : head_chans + write_chans], group_write_vectors], axis=0
    )
    padded_read = jnp.concatenate(
        [earlier[:, head_chans + write_chans :], group_read_vectors], axis=0
    )
    heads_local = step_preactivation.shape[0]
    groups_local = write_chans // STATE
    per_group = heads_local // groups_local
    block_count = row_total // BLOCK
    head_values = conv_silu(padded_heads, head_filter_taps).reshape(
        block_count, BLOCK, groups_local, per_group, HEAD_DIM
    )
    write_values = conv_silu(padded_write, write_filter_taps).reshape(
        block_count, BLOCK, groups_local, STATE
    )
    read_values = conv_silu(padded_read, read_filter_taps).reshape(
        block_count, BLOCK, groups_local, STATE
    )
    step_length_value = jax.nn.softplus(step_preactivation)
    decay_rate_logs = -jnp.exp(head_decay_logs)[:, None] * step_length_value + extra_decay_logs
    step_blocks = step_length_value.reshape(groups_local, per_group, block_count, BLOCK)
    cumulative = jnp.cumsum(
        decay_rate_logs.reshape(groups_local, per_group, block_count, BLOCK), axis=3
    )
    weighted = head_values * jnp.transpose(step_blocks, (2, 3, 0, 1))[..., None]
    lower_mask = jnp.tril(jnp.ones((BLOCK, BLOCK), bool))
    gap_logs = cumulative[..., :, None] - cumulative[..., None, :]
    within = jnp.exp(jnp.where(lower_mask, gap_logs, -jnp.inf))
    affinity = jnp.einsum("blgn,bsgn->gbls", read_values, write_values, precision=highest)
    local_part = jnp.einsum(
        "gebls,bsgep->blgep", affinity[:, None] * within, weighted, precision=highest
    )
    to_end = jnp.exp(cumulative[..., -1:] - cumulative)
    block_states = jnp.einsum(
        "bsgn,bsgep,gebs->bgepn", write_values, weighted, to_end, precision=highest
    )
    block_decay = cumulative[..., -1]
    running = jnp.cumsum(block_decay, axis=2)
    entering = running - block_decay
    earlier_blocks = jnp.tril(jnp.ones((block_count, block_count), bool), -1)
    block_ratio = entering[..., :, None] - running[..., None, :]
    carry_weights = jnp.exp(jnp.where(earlier_blocks, block_ratio, -jnp.inf))
    inside = jnp.einsum("gebc,cgepn->bgepn", carry_weights, block_states, precision=highest)
    device_decay = running[..., -1]
    device_state = jnp.einsum(
        "gec,cgepn->gepn",
        jnp.exp(device_decay[..., None] - running),
        block_states,
        precision=highest,
    )
    incoming = carried_in(device_decay, device_state, "ep")
    states_in = (
        inside + jnp.exp(jnp.transpose(entering, (2, 0, 1)))[..., None, None] * incoming[None]
    )
    carried_part = (
        jnp.einsum("blgn,bgepn->blgep", read_values, states_in, precision=highest)
        * jnp.transpose(jnp.exp(cumulative), (2, 3, 0, 1))[..., None]
    )
    scan_out = (local_part + carried_part).reshape(row_total, groups_local, per_group * HEAD_DIM)
    gate_values = jax.nn.silu(output_gate_inputs.astype(jnp.float32)).reshape(
        row_total, groups_local, per_group * HEAD_DIM
    )
    gated_rows = scan_out * gate_values
    gated_rows = gated_rows * lax.rsqrt(
        jnp.mean(gated_rows * gated_rows, axis=-1, keepdims=True) + eps_norm
    )
    return (gated_rows.reshape(row_total, head_chans) * grouped_norm_gain).astype(jnp.bfloat16)


def local(
    head_inputs_unfiltered,
    group_write_vectors,
    group_read_vectors,
    output_gate_inputs,
    step_preactivation,
    extra_decay_logs,
    head_decay_logs,
    head_filter_taps,
    write_filter_taps,
    read_filter_taps,
    grouped_norm_gain,
    mixer_output_weight,
    expert_input_rows,
    expert_norm_gain,
    routes,
    router_chosen_scores,
    routed_gate_weight,
    routed_up_weight,
    routed_down_weight,
    shared_gate_weight,
    shared_up_weight,
    shared_down_weight,
):
    earlier = tail_rows_from_behind(
        head_inputs_unfiltered, group_write_vectors, group_read_vectors, head_filter_taps.shape[0]
    )
    tp_count = lax.axis_size("tp")
    ep_count = lax.axis_size("ep")
    tok_local = expert_input_rows.shape[0]
    model_width = expert_input_rows.shape[1]
    top_count = routes.shape[1]
    local_experts = routed_gate_weight.shape[0]
    experts = local_experts * ep_count
    capacity = 3 * tok_local * top_count // (2 * experts)
    rows_float = expert_input_rows.astype(jnp.float32)
    normed = (
        rows_float
        * lax.rsqrt(jnp.mean(rows_float * rows_float, axis=-1, keepdims=True) + eps_norm)
        * expert_norm_gain
    ).astype(jnp.bfloat16)
    score_float = router_chosen_scores.astype(jnp.float32)
    weights = score_float / jnp.sum(score_float, axis=1, keepdims=True) * route_scale
    choice = routes[None, :, :] == jnp.arange(experts, dtype=jnp.int32)[:, None, None]
    named = jnp.any(choice, axis=2)
    weight_of = jnp.sum(jnp.where(choice, weights[None], 0.0), axis=2)
    row_order = jnp.arange(tok_local, dtype=jnp.int32)
    earlier_rows = (row_order[:, None] < row_order[None, :]).astype(jnp.bfloat16)
    rank = jnp.dot(
        named.astype(jnp.bfloat16), earlier_rows, preferred_element_type=jnp.float32
    ).astype(jnp.int32)

    cuts = [0, capacity // 2, capacity] if capacity > 1 else [0, capacity]
    picks, outgoing = [], []
    for low, high in zip(cuts[:-1], cuts[1:]):
        places = jnp.arange(low, high, dtype=jnp.int32)
        picked = named[:, None, :] & (rank[:, None, :] == places[None, :, None])
        picks.append(picked)
        outgoing.append(
            jnp.dot(
                picked.reshape(-1, tok_local).astype(jnp.bfloat16),
                normed,
                preferred_element_type=jnp.float32,
            ).astype(jnp.bfloat16)
        )
    group_rows = lax.all_gather(normed, "tp", axis=0, tiled=True)
    earlier, group_rows, outgoing[0] = lax.optimization_barrier((earlier, group_rows, outgoing[0]))

    arrived = []
    for block in outgoing:
        arrived.append(lax.all_to_all(block, "ep", split_axis=0, concat_axis=0, tiled=True))
    gathered = [lax.all_gather(block, "tp", axis=0) for block in arrived]

    shared_hidden = (
        jax.nn.silu(jnp.dot(group_rows, shared_gate_weight, preferred_element_type=jnp.float32))
        * jnp.dot(group_rows, shared_up_weight, preferred_element_type=jnp.float32)
    ).astype(jnp.bfloat16)
    shared_part = jnp.dot(shared_hidden, shared_down_weight, preferred_element_type=jnp.float32)

    mixer_normed = mixer_rows(
        earlier,
        head_inputs_unfiltered,
        group_write_vectors,
        group_read_vectors,
        output_gate_inputs,
        step_preactivation,
        extra_decay_logs,
        head_decay_logs,
        head_filter_taps,
        write_filter_taps,
        read_filter_taps,
        grouped_norm_gain,
    )

    def expert_rows(block):
        sources = block.reshape(tp_count, ep_count, local_experts, -1, model_width)
        gate_value = jnp.einsum(
            "osecd,edf->osecf", sources, routed_gate_weight, preferred_element_type=jnp.float32
        )
        up_value = jnp.einsum(
            "osecd,edf->osecf", sources, routed_up_weight, preferred_element_type=jnp.float32
        )
        hidden = (jax.nn.silu(gate_value) * up_value).astype(jnp.bfloat16)
        partial_value = jnp.einsum(
            "osecf,efd->osecd", hidden, routed_down_weight, preferred_element_type=jnp.float32
        ).astype(jnp.bfloat16)
        return lax.psum_scatter(
            partial_value.reshape(-1, model_width), "tp", scatter_dimension=0, tiled=True
        )

    own_term = jnp.zeros((tok_local, model_width), jnp.float32)
    for block, picked in zip(gathered, picks):
        returned = lax.all_to_all(
            expert_rows(block), "ep", split_axis=0, concat_axis=0, tiled=True
        )
        mixing = jnp.where(picked, weight_of[:, None, :], 0.0).reshape(-1, tok_local)
        own_term = own_term + jnp.einsum(
            "sr,sd->rd", mixing, returned.astype(jnp.float32), precision=highest
        )
    mix_block = mixer_normed.shape[0] // tp_count
    block_rows = mix_block + tok_local
    mix_term = jnp.dot(
        mixer_normed, mixer_output_weight, preferred_element_type=jnp.float32
    ).astype(jnp.bfloat16).reshape(tp_count, mix_block, model_width)
    moe_term = shared_part.astype(jnp.bfloat16).reshape(tp_count, tok_local, model_width)
    row_sums = lax.psum_scatter(
        jnp.concatenate([mix_term, moe_term], axis=1).reshape(tp_count * block_rows, model_width),
        "tp",
        scatter_dimension=0,
        tiled=True,
    )
    mixer_result = row_sums[:mix_block]
    moe_total = row_sums[mix_block:].astype(jnp.float32) + own_term
    return (mixer_result.astype(jnp.bfloat16), moe_total.astype(jnp.bfloat16))


def message_names(half):
    names = ["meta_y", "rows_y", "dense", "mix_core", "mix_far", "mix_y", "halo_h", "halo_w", "halo_r"]
    names += ["gate", "up", "down", "sgate", "sup", "sdown"]
    names += ["pair_s", "pair_d", "plane_s", "plane_d", "last_s"]
    for d in range(half):
        names += [f"{kind}{d}" for kind in ("a", "ay", "ry", "fa", "bo", "by", "fb")]
    return {name: i for i, name in enumerate(names)}


def exchange_kernel(
    ep_count,
    capacity,
    order,
    rows_hbm,
    heads_hbm,
    write_hbm,
    read_hbm,
    ogate_hbm,
    proj_hbm,
    gate_hbm,
    up_hbm,
    down_hbm,
    sgate_hbm,
    sup_hbm,
    sdown_hbm,
    routes_ref,
    scores_ref,
    gain_ref,
    step_ref,
    extra_ref,
    decay_ref,
    htaps_ref,
    wtaps_ref,
    rtaps_ref,
    mgain_ref,
    mix_out,
    moe_out,
    rows_v,
    heads_v,
    write_v,
    read_v,
    ogate_v,
    proj_v,
    gate_v,
    up_v,
    down_v,
    sgate_v,
    sup_v,
    sdown_v,
    halo_h,
    halo_w,
    halo_r,
    ext_h,
    ext_w,
    ext_r,
    hval,
    y_v,
    read_b,
    grow_v,
    own_s,
    own_d,
    plane_s,
    plane_d,
    bef_s,
    out_s,
    out_d,
    in_s,
    in_d,
    mix_v,
    mix_r,
    mix_s,
    mix_ry,
    meta_v,
    grp,
    pack_a,
    pack_b,
    xa,
    xb,
    ya,
    yb,
    ry,
    fa,
    ret_a,
    ret_b,
    dense,
    dense_s,
    dense_r,
    load_sem,
    send_sem,
    recv_sem,
):
    f32, bf16 = jnp.float32, jnp.bfloat16
    half = ep_count // 2
    cap = capacity
    tok, width = rows_v.shape
    tok_m, chans = heads_v.shape
    heads = step_ref.shape[0]
    head_dim = chans // heads
    col = 512
    ids = message_names(half)
    e = lax.axis_index("ep")
    t = lax.axis_index("tp")
    base = (e // half) * half
    q = e - base
    other = half - base
    t_core = t + 1 - 2 * (t % 2)
    t_y = (t + 2) % 4
    t_far = (t_core + 2) % 4
    core, ydev = (e, t_core), (e, t_y)

    def to_a(d):
        return (other + (q + d) % half, t)

    def from_a(d):
        return (other + (q + half - d) % half, t)

    def to_b(d):
        return (base + (q + d) % half, t)

    def from_b(d):
        return (base + (q + half - d) % half, t)

    loads = {}
    for i, (name, src, dst) in enumerate(
        (
            ("rows", rows_hbm, rows_v),
            ("heads", heads_hbm, heads_v),
            ("write", write_hbm, write_v),
            ("read", read_hbm, read_v),
            ("sgate", sgate_hbm, sgate_v.at[0]),
            ("sup", sup_hbm, sup_v.at[0]),
            ("sdown", sdown_hbm, sdown_v.at[0]),
            ("gate", gate_hbm, gate_v.at[0]),
            ("up", up_hbm, up_v.at[0]),
            ("down", down_hbm, down_v.at[0]),
            ("ogate", ogate_hbm, ogate_v),
            ("proj", proj_hbm, proj_v),
        )
    ):
        loads[name] = pltpu.make_async_copy(src, dst, load_sem.at[i])
        loads[name].start()

    copies = {}

    def prepare(name, src, dst, device):
        i = ids[name]
        copies[name] = pltpu.make_async_remote_copy(
            src_ref=src,
            dst_ref=dst,
            send_sem=send_sem.at[i],
            recv_sem=recv_sem.at[i],
            device_id=device,
            device_id_type=MESH,
        )

    def send(name, src, dst, device):
        prepare(name, src, dst, device)
        copies[name].start()

    def arrived(name):
        copies[name].wait_recv()

    guarded = []

    def send_if(name, src, dst, device, here):
        prepare(name, src, dst, device)
        guarded.append((name, here))

        @pl.when(here)
        def _():
            copies[name].start()

    barrier = pltpu.get_barrier_semaphore()
    peers = [core, ydev] + [to_a(d) for d in range(half)] + [to_b(d) for d in range(1, half)]
    for peer in peers:
        pl.semaphore_signal(barrier, inc=1, device_id=peer, device_id_type=MESH)

    row = lax.broadcasted_iota(jnp.int32, (tok, tok), 0)
    lane = lax.broadcasted_iota(jnp.int32, (tok, tok), 1)
    routed = [routes_ref[k : k + 1, :] for k in range(2)]
    expert_row = lax.broadcasted_iota(jnp.int32, (ep_count, tok), 0)
    chosen = [routed[k] == expert_row for k in range(2)]
    named = jnp.where(chosen[0] | chosen[1], 1.0, 0.0).astype(bf16)
    rank = jnp.dot(
        named, jnp.where(row < lane, 1.0, 0.0).astype(bf16), preferred_element_type=f32
    )
    scores = scores_ref[...].astype(f32)
    total_score = jnp.sum(scores, axis=0, keepdims=True)
    meta_v[0] = jnp.zeros(meta_v.shape[1:], f32)
    for k in range(2):
        meta_v[0, k : k + 1, :] = jnp.sum(
            jnp.where(chosen[k], rank, 0.0), axis=0, keepdims=True
        ) + (routed[k] * cap).astype(f32)
        meta_v[0, 2 + k : 3 + k, :] = scores[k : k + 1, :] / total_score * route_scale

    loads["rows"].wait()

    def norm_rows(i, carry):
        at = pl.ds(pl.multiple_of(i * 16, 16), 16)
        x = rows_v[at, :].astype(f32)
        scale = lax.rsqrt(jnp.mean(x * x, axis=-1, keepdims=True) + eps_norm)
        grp[0, at, :] = (x * scale * gain_ref[...]).astype(bf16)
        return carry

    lax.fori_loop(0, tok // 16, norm_rows, 0)
    pl.semaphore_wait(barrier, len(peers))

    def pack(pos, expert_at, ref, lead, low):
        places = lax.broadcasted_iota(jnp.int32, (cap, tok), 0) + expert_at * cap
        places = places.astype(f32)
        picked = (places == meta_v[pos, 0:1, :]) | (places == meta_v[pos, 1:2, :])
        picked = jnp.where(picked, 1.0, 0.0).astype(bf16)
        for n in range(0, width, col):
            ref[lead, low : low + cap, n : n + col] = jnp.dot(
                picked, grp[pos, :, n : n + col], preferred_element_type=f32
            ).astype(bf16)

    def rows_out():
        send("meta_y", meta_v.at[0], meta_v.at[1], ydev)
        send("rows_y", grp.at[0], grp.at[1], ydev)

    def halo_out():
        following = ((e + 1) % ep_count, t)
        kept = halo_h.shape[0]
        tail = pl.ds(tok_m - kept, kept)
        for name in ("heads", "write", "read"):
            loads[name].wait()
        send("halo_h", heads_v.at[tail], halo_h, following)
        send("halo_w", write_v.at[tail], halo_w, following)
        send("halo_r", read_v.at[tail], halo_r, following)

    def weights_out():
        send("sgate", sgate_hbm, sgate_v.at[1], core)
        send("sup", sup_hbm, sup_v.at[1], core)
        send("sdown", sdown_hbm, sdown_v.at[1], core)
        send("gate", gate_hbm, gate_v.at[1], core)
        send("up", up_hbm, up_v.at[1], core)
        send("down", down_hbm, down_v.at[1], core)

    def weights_in(names):
        for name in names:
            loads[name].wait()
            arrived(name)

    def gated_product(x, first_v, second_v, third_v, put):
        hidden = []
        for s in range(2):
            g = jnp.dot(x, first_v[s], preferred_element_type=f32)
            u = jnp.dot(x, second_v[s], preferred_element_type=f32)
            hidden.append((jax.nn.silu(g) * u).astype(bf16))
        for n in range(0, width, col):
            at = slice(n, n + col)
            put(
                at,
                jnp.dot(hidden[0], third_v[0, :, at], preferred_element_type=f32)
                + jnp.dot(hidden[1], third_v[1, :, at], preferred_element_type=f32),
            )

    def shared_rows(pos):
        def put(at, value):
            dense[pos, :, at] = value

        gated_product(grp[pos], sgate_v, sup_v, sdown_v, put)

    def a0(d):
        pack(0, other + (q + d) % half, pack_a, d, 0)
        send(f"a{d}", pack_a.at[d], xa.at[d, pl.ds(0, cap)], to_a(d))

    def a1(d):
        arrived(f"a{d}")
        send(f"ay{d}", xa.at[d, pl.ds(0, cap)], xa.at[d, pl.ds(cap, cap)], ydev)

    def a3(d):
        arrived(f"ay{d}")

        def put(at, value):
            ya[d, :, at] = value.astype(bf16)

        gated_product(xa[d], gate_v, up_v, down_v, put)
        send(f"ry{d}", ya.at[d, pl.ds(cap, cap)], ry.at[d], ydev)

    def a5(d):
        arrived(f"ry{d}")
        fa[d] = (ya[d, 0:cap].astype(f32) + ry[d].astype(f32)).astype(bf16)
        send(f"fa{d}", fa.at[d], ret_a.at[pl.ds(d * cap, cap)], from_a(d))

    def bo(d):
        pack(0, base + (q + d) % half, pack_b, d - 1, 0)
        send(f"bo{d}", pack_b.at[d - 1, pl.ds(0, cap)], xb.at[d, pl.ds(0, cap)], to_b(d))

    def by(d):
        pack(1, base + (q + d) % half, pack_b, d - 1, cap)
        send(f"by{d}", pack_b.at[d - 1, pl.ds(cap, cap)], xb.at[d, pl.ds(cap, cap)], to_b(d))

    def b3(d):
        if d:
            arrived(f"bo{d}")
            arrived(f"by{d}")
        else:
            pack(0, e, xb, 0, 0)
            pack(1, e, xb, 0, cap)

        def put(at, value):
            for p in range(2):
                part = value[p * cap : (p + 1) * cap].astype(bf16)
                if d:
                    yb[d - 1, p, :, at] = part
                else:
                    ret_b[p, 0:cap, at] = part

        gated_product(xb[d], gate_v, up_v, down_v, put)
        if d:
            send(f"fb{d}", yb.at[d - 1], ret_b.at[:, pl.ds(d * cap, cap)], from_b(d))

    def chosen_slots(columns, first):
        lanes = lax.broadcasted_iota(jnp.int32, (1, half * cap), 1)
        code = lanes + (first + q) * cap
        for d in range(1, half):
            moved = (first + (q + d) % half - d) * cap
            code = jnp.where(lanes >= d * cap, lanes + moved, code)
        code = code.astype(f32)
        return [jnp.where(columns[:, k : k + 1] == code, 1.0, 0.0).astype(bf16) for k in range(2)]

    def mixed(columns, picks, returned):
        total = None
        for k in range(2):
            part = columns[:, 2 + k : 3 + k] * jnp.dot(picks[k], returned, preferred_element_type=f32)
            total = part if total is None else total + part
        return total

    def dense_rows(p):
        columns = jnp.transpose(meta_v[p])
        picks = chosen_slots(columns, base)
        for n in range(0, width, col):
            at = slice(n, n + col)
            value = mixed(columns, picks, ret_b[p, :, at]) + dense[p, :, at]
            if p:
                dense_s[:, at] = value.astype(bf16)
            else:
                dense[0, :, at] = value

    def dense_out():
        for d in range(1, half):
            arrived(f"fb{d}")
        dense_rows(1)
        send("dense", dense_s, dense_r, ydev)
        dense_rows(0)

    def conv(x_v, halo, ext, taps_ref, n, size):
        at = slice(n, n + size)
        taps = taps_ref.shape[0]
        edge = ext.shape[0] - tok_m
        first = halo.shape[0] - edge
        there = jnp.where(e > 0, 1.0, 0.0).astype(f32)
        ext[0:edge, at] = halo[first:, at].astype(f32) * there
        ext[edge:, at] = x_v[:, at].astype(f32)
        total = None
        for j in range(taps):
            low = edge - taps + 1 + j
            part = taps_ref[j : j + 1, at].astype(f32) * ext[low : low + tok_m, at]
            total = part if total is None else total + part
        return jax.nn.silu(total)

    head_row = lax.broadcasted_iota(jnp.int32, (heads, chans), 0)
    lane_head = lax.broadcasted_iota(jnp.int32, (heads, chans), 1) - head_row * head_dim
    spread_b = jnp.where((lane_head >= 0) & (lane_head < head_dim), 1.0, 0.0).astype(bf16)

    def spread(value, terms):
        total, rest = None, value
        for _ in range(terms):
            part = rest.astype(bf16)
            rest = rest - part.astype(f32)
            add = jnp.dot(part, spread_b, preferred_element_type=f32)
            total = add if total is None else total + add
        return total

    local = {}

    def mixer_states():
        for name in ("halo_h", "halo_w", "halo_r"):
            arrived(name)
        for n in range(0, chans, 256):
            hval[:, n : n + 256] = conv(heads_v, halo_h, ext_h, htaps_ref, n, 256)
        states = write_v.shape[1]
        write = conv(write_v, halo_w, ext_w, wtaps_ref, 0, states)
        read = conv(read_v, halo_r, ext_r, rtaps_ref, 0, states)
        read_b[...] = read.astype(bf16)
        step = jax.nn.softplus(step_ref[...])
        square_row = lax.broadcasted_iota(jnp.int32, (heads, heads), 0)
        square_lane = lax.broadcasted_iota(jnp.int32, (heads, heads), 1)
        speed = jnp.sum(
            jnp.where(square_row == square_lane, jnp.exp(decay_ref[...]), 0.0), axis=1, keepdims=True
        )
        rate = step * -speed + extra_ref[...]
        upto = jnp.where(row <= lane, 1.0, 0.0).astype(f32)
        cum = jnp.dot(rate, upto, precision=highest, preferred_element_type=f32)
        cum_t = jnp.transpose(cum)
        to_end = jnp.exp(cum[:, tok_m - 1 : tok_m] - cum) * step
        affinity = lax.dot_general(
            read, write, (((1,), (1,)), ((), ())), precision=highest, preferred_element_type=f32
        )
        weights = spread(jnp.transpose(to_end), 2)
        weighted = (hval[...] * weights).astype(bf16)
        own_s[...] = jnp.dot(jnp.transpose(write).astype(bf16), weighted, preferred_element_type=f32)
        own_d[...] = spread(cum_t[tok_m - 8 : tok_m], 3)[7:8]
        local.update(cum=cum, cum_t=cum_t, step=step, affinity=affinity)

    def mixer_rows_local():
        cum, cum_t, step, affinity = (local[k] for k in ("cum", "cum_t", "step", "affinity"))
        grow_v[...] = spread(jnp.exp(cum_t), 2)
        causal = row >= lane
        for pair in range(heads // 2):
            at = slice(pair * 2 * head_dim, (pair + 1) * 2 * head_dim)
            parts = []
            for h in (2 * pair, 2 * pair + 1):
                gap = jnp.where(causal, cum_t[:, h : h + 1] - cum[h : h + 1, :], -jnp.inf)
                parts.append((affinity * jnp.exp(gap) * step[h : h + 1, :]).astype(bf16))
            both = hval[:, at].astype(bf16)
            side = lax.broadcasted_iota(jnp.int32, both.shape, 1) < head_dim
            zero = jnp.zeros_like(both)
            y_v[:, at] = jnp.dot(
                parts[0], jnp.where(side, both, zero), preferred_element_type=f32
            ) + jnp.dot(parts[1], jnp.where(side, zero, both), preferred_element_type=f32)

    side_x, plane, planes = e % 2, e // 2, ep_count // 2
    is_head = side_x == 1 - t % 2
    is_tail = side_x == t % 2
    later_head = is_head & (side_x == 1)
    early_head = is_head & (side_x == 0)
    beside = (e + 1 - 2 * side_x, t)
    above = ((e + 2) % ep_count, t)

    def states_pair():
        @pl.when(is_tail)
        def _():
            out_s[0] = own_s[...].astype(bf16)
            out_d[0] = own_d[...]

        send_if("pair_s", out_s.at[0], in_s.at[0], beside, is_tail)
        send_if("pair_d", out_d.at[0], in_d.at[0], beside, is_tail)

    def states_plane():
        prepare("plane_s", out_s.at[1], in_s.at[1], above)
        prepare("plane_d", out_d.at[1], in_d.at[1], above)
        guarded.append(("plane_s", is_head & (plane < planes - 1)))
        guarded.append(("plane_d", is_head & (plane < planes - 1)))

        @pl.when(is_head)
        def _():
            arrived("pair_s")
            arrived("pair_d")

        @pl.when(later_head)
        def _():
            plane_s[...] = own_s[...] + jnp.exp(own_d[...]) * in_s[0].astype(f32)

        @pl.when(early_head)
        def _():
            plane_s[...] = in_s[0].astype(f32) + jnp.exp(in_d[0]) * own_s[...]

        @pl.when(is_head)
        def _():
            plane_d[...] = own_d[...] + in_d[0]

        @pl.when(is_head & (plane == 0))
        def _():
            in_s[1] = jnp.zeros(in_s.shape[1:], bf16)
            in_d[1] = jnp.zeros(in_d.shape[1:], f32)
            out_s[1] = plane_s[...].astype(bf16)
            out_d[1] = plane_d[...]
            copies["plane_s"].start()
            copies["plane_d"].start()

    def states_up(k):
        @pl.when(is_head & (plane == k))
        def _():
            arrived("plane_s")
            arrived("plane_d")
            if k < planes - 1:
                out_s[1] = (plane_s[...] + jnp.exp(plane_d[...]) * in_s[1].astype(f32)).astype(bf16)
                out_d[1] = plane_d[...] + in_d[1]
                copies["plane_s"].start()
                copies["plane_d"].start()

    def states_last():
        @pl.when(later_head)
        def _():
            bef_s[...] = in_s[0].astype(f32) + jnp.exp(in_d[0]) * in_s[1].astype(f32)
            out_s[2] = in_s[1]

        @pl.when(early_head)
        def _():
            bef_s[...] = in_s[1].astype(f32)
            out_s[2] = (own_s[...] + jnp.exp(own_d[...]) * in_s[1].astype(f32)).astype(bf16)

        send_if("last_s", out_s.at[2], in_s.at[2], beside, is_head)

    def states_in():
        @pl.when(is_tail)
        def _():
            arrived("last_s")
            bef_s[...] = in_s[2].astype(f32)

    def mixer_finish():
        square = jnp.zeros((tok_m, 1), f32)
        for n in range(0, chans, 256):
            at = slice(n, n + 256)
            carried = jnp.dot(read_b[...], bef_s[:, at].astype(bf16), preferred_element_type=f32)
            value = (y_v[:, at] + carried * grow_v[:, at]) * jax.nn.silu(ogate_v[:, at].astype(f32))
            y_v[:, at] = value
            square = square + jnp.sum(value * value, axis=-1, keepdims=True)
        scale = lax.rsqrt(square / chans + eps_norm)
        normed = (y_v[...] * scale * mgain_ref[...]).astype(bf16)
        block = mix_v.shape[1]
        for n in range(0, width, col):
            part = jnp.dot(normed, proj_v[:, n : n + col], preferred_element_type=f32).astype(bf16)
            for i in range(4):
                mix_v[i, :, n : n + col] = part[i * block : (i + 1) * block]
        send("mix_core", mix_v.at[t_core], mix_r.at[0], core)
        send("mix_far", mix_v.at[t_far], mix_r.at[1], core)

    def mix_across():
        arrived("mix_core")
        arrived("mix_far")
        mix_s[...] = (mix_v[t_y].astype(f32) + mix_r[1].astype(f32)).astype(bf16)
        send("mix_y", mix_s, mix_ry, ydev)

    def rows_in():
        arrived("meta_y")
        arrived("rows_y")

    steps = {
        "rows_out": rows_out,
        "halo_out": halo_out,
        "weights_out": weights_out,
        "shared_in": lambda: weights_in(("sgate", "sup", "sdown")),
        "expert_in": lambda: weights_in(("gate", "up", "down")),
        "mix_in": lambda: [loads[name].wait() for name in ("ogate", "proj")],
        "rows_in": rows_in,
        "states": mixer_states,
        "local": mixer_rows_local,
        "pair": states_pair,
        "plane": states_plane,
        "last": states_last,
        "before": states_in,
        "finish": mixer_finish,
        "across": mix_across,
        "dense": dense_out,
    }
    numbered = {"a0": a0, "a1": a1, "a3": a3, "a5": a5, "bo": bo, "by": by, "b3": b3, "up": states_up}
    numbered["shared"] = shared_rows
    for name in order.split():
        if name in steps:
            steps[name]()
        else:
            stem, number = name.split(":")
            numbered[stem](int(number))

    arrived("mix_y")
    mix_out[...] = (mix_v[t].astype(f32) + mix_r[0].astype(f32) + mix_ry[...].astype(f32)).astype(bf16)
    for d in range(half):
        arrived(f"fa{d}")
    arrived("dense")
    columns = jnp.transpose(meta_v[0])
    picks = chosen_slots(columns, other)
    for n in range(0, width, col):
        at = slice(n, n + col)
        value = mixed(columns, picks, ret_a[:, at]) + dense[0, :, at] + dense_r[:, at].astype(f32)
        moe_out[:, at] = value.astype(bf16)
    for name, here in guarded:

        @pl.when(here)
        def _(name=name):
            copies[name].wait_send()

    kept_back = [name for name, _ in guarded]
    for name in copies:
        if name not in kept_back:
            copies[name].wait_send()


def exchange_order(half):
    before = ["rows_out", "halo_out", "a0:0"]
    before += [f"bo:{d}" for d in range(1, half)]
    before += ["weights_out", "states", "pair"]
    if half > 1:
        before += ["a0:1"]
    before += ["plane", "local", "up:1"]
    before += [f"a0:{d}" for d in range(2, half)]
    after = {0: ["rows_in"] + [f"by:{d}" for d in range(1, half)]}
    after[0] += ["shared_in", "shared:1", "shared:0", "expert_in", "b3:0"]
    after.setdefault(1, []).extend(["up:2"])
    for d in range(1, half):
        after.setdefault(d, []).append(f"b3:{d}")
    for k in range(3, half):
        after.setdefault(k - 1, []).append(f"up:{k}")
    after.setdefault(half - 2, []).append("last")
    after.setdefault(half - 1, []).extend(["before", "mix_in", "finish"])
    after[half] = ["across"]
    after[half + 1] = ["dense"]
    steps = list(before)
    for at in range(half + 2):
        for kind, lag in (("a5", 2), ("a3", 1), ("a1", 0)):
            if 0 <= at - lag < half:
                steps.append(f"{kind}:{at - lag}")
        steps += after.get(at, [])
    return " ".join(steps)


def exchange(ep_count, capacity, small, large):
    (rows, heads, write, read, ogate, proj, gate, up, down, sgate, sup, sdown) = large
    half = ep_count // 2
    tok, width = rows.shape
    bf16, f32 = jnp.bfloat16, jnp.float32
    cap = capacity
    tok_m, chans = heads.shape
    state = write.shape[1]
    mix_block = tok_m // 4
    count = len(message_names(half))
    shapes = [(array.shape, bf16) for array in (rows, heads, write, read, ogate, proj)]
    shapes += [((2, *array.shape), bf16) for array in (gate, up, down, sgate, sup, sdown)]
    shapes += [
        ((16, chans), bf16),
        ((16, state), bf16),
        ((16, state), bf16),
        ((tok_m + 8, chans), f32),
        ((tok_m + 8, state), f32),
        ((tok_m + 8, state), f32),
        ((tok_m, chans), f32),
        ((tok_m, chans), f32),
        ((tok_m, state), bf16),
        ((tok_m, chans), f32),
        ((state, chans), f32),
        ((1, chans), f32),
        ((state, chans), f32),
        ((1, chans), f32),
        ((state, chans), f32),
        ((3, state, chans), bf16),
        ((2, 1, chans), f32),
        ((3, state, chans), bf16),
        ((2, 1, chans), f32),
        ((4, mix_block, width), bf16),
        ((2, mix_block, width), bf16),
        ((mix_block, width), bf16),
        ((mix_block, width), bf16),
        ((2, 8, tok), f32),
        ((2, tok, width), bf16),
        ((half, cap, width), bf16),
        ((half - 1, 2 * cap, width), bf16),
        ((half, 2 * cap, width), bf16),
        ((half, 2 * cap, width), bf16),
        ((half, 2 * cap, width), bf16),
        ((half - 1, 2, cap, width), bf16),
        ((half, cap, width), bf16),
        ((half, cap, width), bf16),
        ((half * cap, width), bf16),
        ((2, half * cap, width), bf16),
        ((2, tok, width), f32),
        ((tok, width), bf16),
        ((tok, width), bf16),
    ]
    any_spec = pl.BlockSpec(memory_space=pl.ANY)
    vmem_spec = pl.BlockSpec(memory_space=pltpu.VMEM)
    return pl.pallas_call(
        functools.partial(exchange_kernel, ep_count, capacity, exchange_order(half)),
        out_shape=(
            jax.ShapeDtypeStruct((mix_block, width), bf16),
            jax.ShapeDtypeStruct((tok, width), bf16),
        ),
        in_specs=[any_spec] * len(large) + [vmem_spec] * len(small),
        out_specs=(vmem_spec, vmem_spec),
        scratch_shapes=[pltpu.VMEM(shape, dtype) for shape, dtype in shapes]
        + [
            pltpu.SemaphoreType.DMA((len(large),)),
            pltpu.SemaphoreType.DMA((count,)),
            pltpu.SemaphoreType.DMA((count,)),
        ],
        compiler_params=pltpu.CompilerParams(
            collective_id=0, has_side_effects=True, vmem_limit_bytes=62 * 1024 * 1024
        ),
        name="mixer_and_experts",
    )(*large, *small)


def direct(
    head_inputs_unfiltered,
    group_write_vectors,
    group_read_vectors,
    output_gate_inputs,
    step_preactivation,
    extra_decay_logs,
    head_decay_logs,
    head_filter_taps,
    write_filter_taps,
    read_filter_taps,
    grouped_norm_gain,
    mixer_output_weight,
    expert_input_rows,
    expert_norm_gain,
    routes,
    router_chosen_scores,
    routed_gate_weight,
    routed_up_weight,
    routed_down_weight,
    shared_gate_weight,
    shared_up_weight,
    shared_down_weight,
):
    ep_count = lax.axis_size("ep")
    capacity = 3 * expert_input_rows.shape[0] * routes.shape[1] // (2 * ep_count)
    small = (
        routes.T,
        router_chosen_scores.T,
        expert_norm_gain.reshape(1, -1),
        step_preactivation,
        extra_decay_logs,
        head_decay_logs.reshape(1, -1),
        head_filter_taps,
        write_filter_taps,
        read_filter_taps,
        grouped_norm_gain.reshape(1, -1),
    )
    large = (
        expert_input_rows,
        head_inputs_unfiltered,
        group_write_vectors,
        group_read_vectors,
        output_gate_inputs,
        mixer_output_weight,
        routed_gate_weight[0],
        routed_up_weight[0],
        routed_down_weight[0],
        shared_gate_weight,
        shared_up_weight,
        shared_down_weight,
    )
    return exchange(ep_count, capacity, small, large)


def fits_direct(mesh, rows, mix_rows, top_count, experts, groups):
    ep_count, tp_count = mesh.shape["ep"], mesh.shape["tp"]
    tok_local = rows // (ep_count * tp_count)
    capacity = 3 * tok_local * top_count // (2 * experts)
    return (
        tp_count == 4
        and groups == tp_count
        and experts == ep_count
        and ep_count in (4, 8)
        and top_count == 2
        and capacity % 16 == 0
        and tok_local == 128
        and mix_rows == tok_local * ep_count
    )


def solution(mesh):
    in_specs = (
        P("ep", "tp"),
        P("ep", "tp"),
        P("ep", "tp"),
        P("ep", "tp"),
        P("tp", "ep"),
        P("tp", "ep"),
        P("tp"),
        P(None, "tp"),
        P(None, "tp"),
        P(None, "tp"),
        P("tp"),
        P("tp", None),
        P(("ep", "tp"), None),
        P(),
        P(("ep", "tp"), None),
        P(("ep", "tp"), None),
        P("ep", None, "tp"),
        P("ep", None, "tp"),
        P("ep", "tp", None),
        P(None, "tp"),
        P(None, "tp"),
        P("tp", None),
    )
    out_specs = (P(("ep", "tp"), None), P(("ep", "tp"), None))
    def step(*args):
        direct_form = fits_direct(
            mesh,
            args[12].shape[0],
            args[0].shape[0],
            args[14].shape[1],
            args[16].shape[0],
            args[1].shape[1] // STATE,
        )
        return jax.shard_map(
            direct if direct_form else local,
            mesh=mesh,
            in_specs=in_specs,
            out_specs=out_specs,
            check_vma=False,
        )(*args)

    return step
```

```python
import functools

import jax
import jax.numpy as jnp
from jax import lax
from jax.experimental import pallas as pl
from jax.experimental.pallas import tpu as pltpu
from jax.sharding import PartitionSpec as P

MESH = pl.DeviceIdType.MESH
HEAD_DIM = 64
STATE = 128
BLOCK = 64


eps_norm = 1e-06
route_scale = 2.5
highest = lax.Precision.HIGHEST


def from_behind(value, axis, by):
    devices = lax.axis_size(axis)
    pairs = [(i, i + by) for i in range(devices) if 0 <= i + by < devices]
    return lax.ppermute(value, axis, pairs)


def sent_state(decay, state, axis, by):
    heads, width = decay.shape[0], state.shape[-1]
    parts, rest = [], decay
    for _ in range(3):
        part = lax.reduce_precision(rest, exponent_bits=8, mantissa_bits=7)
        parts.append(part)
        rest = rest - part
    decay_rows = jnp.pad(jnp.stack(parts, axis=1), ((0, 0), (0, width - 3)))
    packed = jnp.concatenate([state.reshape(-1, width), decay_rows], axis=0).astype(jnp.bfloat16)
    packed = from_behind(packed, axis, by).astype(jnp.float32)
    return jnp.sum(packed[-heads:, :3], axis=-1), packed[:-heads].reshape(state.shape)


def carried_in(decay, state, axis):
    shape = state.shape
    own = (decay.reshape(-1), state.reshape((-1,) + shape[-2:]))
    before, by = None, 1
    while by < lax.axis_size(axis):
        span = own if before is None else combine_states(before, own)
        received = sent_state(*span, axis, by)
        before = received if before is None else combine_states(received, before)
        by *= 2
    if before is None:
        return jnp.zeros_like(state)
    return before[1].reshape(shape)


def combine_states(earlier_part, later_part):
    return (
        earlier_part[0] + later_part[0],
        later_part[1] + jnp.exp(later_part[0])[..., None, None] * earlier_part[1],
    )


def conv_silu(values, weights):
    taps = weights.shape[0]
    length = values.shape[0] - taps + 1
    running_sum = jnp.zeros((length, values.shape[1]), jnp.float32)
    for offset in range(taps):
        running_sum = running_sum + weights[offset].astype(jnp.float32) * values[
            offset : offset + length
        ].astype(jnp.float32)
    return jax.nn.silu(running_sum)


def tail_rows_from_behind(head_inputs, write_vectors, read_vectors, taps):
    start = head_inputs.shape[0] - taps + 1
    tail_rows = jnp.concatenate([head_inputs[start:], write_vectors[start:], read_vectors[start:]], axis=1)
    return from_behind(tail_rows, "ep", 1)


def mixer_rows(
    earlier,
    head_inputs_unfiltered,
    group_write_vectors,
    group_read_vectors,
    output_gate_inputs,
    step_preactivation,
    extra_decay_logs,
    head_decay_logs,
    head_filter_taps,
    write_filter_taps,
    read_filter_taps,
    grouped_norm_gain,
):
    row_total = head_inputs_unfiltered.shape[0]
    head_chans = head_inputs_unfiltered.shape[1]
    write_chans = group_write_vectors.shape[1]
    padded_heads = jnp.concatenate([earlier[:, :head_chans], head_inputs_unfiltered], axis=0)
    padded_write = jnp.concatenate(
        [earlier[:, head_chans : head_chans + write_chans], group_write_vectors], axis=0
    )
    padded_read = jnp.concatenate(
        [earlier[:, head_chans + write_chans :], group_read_vectors], axis=0
    )
    heads_local = step_preactivation.shape[0]
    groups_local = write_chans // STATE
    per_group = heads_local // groups_local
    block_count = row_total // BLOCK
    head_values = conv_silu(padded_heads, head_filter_taps).reshape(
        block_count, BLOCK, groups_local, per_group, HEAD_DIM
    )
    write_values = conv_silu(padded_write, write_filter_taps).reshape(
        block_count, BLOCK, groups_local, STATE
    )
    read_values = conv_silu(padded_read, read_filter_taps).reshape(
        block_count, BLOCK, groups_local, STATE
    )
    step_length_value = jax.nn.softplus(step_preactivation)
    decay_rate_logs = -jnp.exp(head_decay_logs)[:, None] * step_length_value + extra_decay_logs
    step_blocks = step_length_value.reshape(groups_local, per_group, block_count, BLOCK)
    cumulative = jnp.cumsum(
        decay_rate_logs.reshape(groups_local, per_group, block_count, BLOCK), axis=3
    )
    weighted = head_values * jnp.transpose(step_blocks, (2, 3, 0, 1))[..., None]
    lower_mask = jnp.tril(jnp.ones((BLOCK, BLOCK), bool))
    gap_logs = cumulative[..., :, None] - cumulative[..., None, :]
    within = jnp.exp(jnp.where(lower_mask, gap_logs, -jnp.inf))
    affinity = jnp.einsum("blgn,bsgn->gbls", read_values, write_values, precision=highest)
    local_part = jnp.einsum(
        "gebls,bsgep->blgep", affinity[:, None] * within, weighted, precision=highest
    )
    to_end = jnp.exp(cumulative[..., -1:] - cumulative)
    block_states = jnp.einsum(
        "bsgn,bsgep,gebs->bgepn", write_values, weighted, to_end, precision=highest
    )
    block_decay = cumulative[..., -1]
    running = jnp.cumsum(block_decay, axis=2)
    entering = running - block_decay
    earlier_blocks = jnp.tril(jnp.ones((block_count, block_count), bool), -1)
    block_ratio = entering[..., :, None] - running[..., None, :]
    carry_weights = jnp.exp(jnp.where(earlier_blocks, block_ratio, -jnp.inf))
    inside = jnp.einsum("gebc,cgepn->bgepn", carry_weights, block_states, precision=highest)
    device_decay = running[..., -1]
    device_state = jnp.einsum(
        "gec,cgepn->gepn",
        jnp.exp(device_decay[..., None] - running),
        block_states,
        precision=highest,
    )
    incoming = carried_in(device_decay, device_state, "ep")
    states_in = (
        inside + jnp.exp(jnp.transpose(entering, (2, 0, 1)))[..., None, None] * incoming[None]
    )
    carried_part = (
        jnp.einsum("blgn,bgepn->blgep", read_values, states_in, precision=highest)
        * jnp.transpose(jnp.exp(cumulative), (2, 3, 0, 1))[..., None]
    )
    scan_out = (local_part + carried_part).reshape(row_total, groups_local, per_group * HEAD_DIM)
    gate_values = jax.nn.silu(output_gate_inputs.astype(jnp.float32)).reshape(
        row_total, groups_local, per_group * HEAD_DIM
    )
    gated_rows = scan_out * gate_values
    gated_rows = gated_rows * lax.rsqrt(
        jnp.mean(gated_rows * gated_rows, axis=-1, keepdims=True) + eps_norm
    )
    return (gated_rows.reshape(row_total, head_chans) * grouped_norm_gain).astype(jnp.bfloat16)


def local(
    head_inputs_unfiltered,
    group_write_vectors,
    group_read_vectors,
    output_gate_inputs,
    step_preactivation,
    extra_decay_logs,
    head_decay_logs,
    head_filter_taps,
    write_filter_taps,
    read_filter_taps,
    grouped_norm_gain,
    mixer_output_weight,
    expert_input_rows,
    expert_norm_gain,
    routes,
    router_chosen_scores,
    routed_gate_weight,
    routed_up_weight,
    routed_down_weight,
    shared_gate_weight,
    shared_up_weight,
    shared_down_weight,
):
    earlier = tail_rows_from_behind(
        head_inputs_unfiltered, group_write_vectors, group_read_vectors, head_filter_taps.shape[0]
    )
    tp_count = lax.axis_size("tp")
    ep_count = lax.axis_size("ep")
    tok_local = expert_input_rows.shape[0]
    model_width = expert_input_rows.shape[1]
    top_count = routes.shape[1]
    local_experts = routed_gate_weight.shape[0]
    experts = local_experts * ep_count
    capacity = 3 * tok_local * top_count // (2 * experts)
    rows_float = expert_input_rows.astype(jnp.float32)
    normed = (
        rows_float
        * lax.rsqrt(jnp.mean(rows_float * rows_float, axis=-1, keepdims=True) + eps_norm)
        * expert_norm_gain
    ).astype(jnp.bfloat16)
    score_float = router_chosen_scores.astype(jnp.float32)
    weights = score_float / jnp.sum(score_float, axis=1, keepdims=True) * route_scale
    choice = routes[None, :, :] == jnp.arange(experts, dtype=jnp.int32)[:, None, None]
    named = jnp.any(choice, axis=2)
    weight_of = jnp.sum(jnp.where(choice, weights[None], 0.0), axis=2)
    row_order = jnp.arange(tok_local, dtype=jnp.int32)
    earlier_rows = (row_order[:, None] < row_order[None, :]).astype(jnp.bfloat16)
    rank = jnp.dot(
        named.astype(jnp.bfloat16), earlier_rows, preferred_element_type=jnp.float32
    ).astype(jnp.int32)

    cuts = [0, capacity // 2, capacity] if capacity > 1 else [0, capacity]
    picks, outgoing = [], []
    for low, high in zip(cuts[:-1], cuts[1:]):
        places = jnp.arange(low, high, dtype=jnp.int32)
        picked = named[:, None, :] & (rank[:, None, :] == places[None, :, None])
        picks.append(picked)
        outgoing.append(
            jnp.dot(
                picked.reshape(-1, tok_local).astype(jnp.bfloat16),
                normed,
                preferred_element_type=jnp.float32,
            ).astype(jnp.bfloat16)
        )
    group_rows = lax.all_gather(normed, "tp", axis=0, tiled=True)
    earlier, group_rows, outgoing[0] = lax.optimization_barrier((earlier, group_rows, outgoing[0]))

    arrived = []
    for block in outgoing:
        arrived.append(lax.all_to_all(block, "ep", split_axis=0, concat_axis=0, tiled=True))
    gathered = [lax.all_gather(block, "tp", axis=0) for block in arrived]

    shared_hidden = (
        jax.nn.silu(jnp.dot(group_rows, shared_gate_weight, preferred_element_type=jnp.float32))
        * jnp.dot(group_rows, shared_up_weight, preferred_element_type=jnp.float32)
    ).astype(jnp.bfloat16)
    shared_part = jnp.dot(shared_hidden, shared_down_weight, preferred_element_type=jnp.float32)

    mixer_normed = mixer_rows(
        earlier,
        head_inputs_unfiltered,
        group_write_vectors,
        group_read_vectors,
        output_gate_inputs,
        step_preactivation,
        extra_decay_logs,
        head_decay_logs,
        head_filter_taps,
        write_filter_taps,
        read_filter_taps,
        grouped_norm_gain,
    )

    def expert_rows(block):
        sources = block.reshape(tp_count, ep_count, local_experts, -1, model_width)
        gate_value = jnp.einsum(
            "osecd,edf->osecf", sources, routed_gate_weight, preferred_element_type=jnp.float32
        )
        up_value = jnp.einsum(
            "osecd,edf->osecf", sources, routed_up_weight, preferred_element_type=jnp.float32
        )
        hidden = (jax.nn.silu(gate_value) * up_value).astype(jnp.bfloat16)
        partial_value = jnp.einsum(
            "osecf,efd->osecd", hidden, routed_down_weight, preferred_element_type=jnp.float32
        ).astype(jnp.bfloat16)
        return lax.psum_scatter(
            partial_value.reshape(-1, model_width), "tp", scatter_dimension=0, tiled=True
        )

    own_term = jnp.zeros((tok_local, model_width), jnp.float32)
    for block, picked in zip(gathered, picks):
        returned = lax.all_to_all(
            expert_rows(block), "ep", split_axis=0, concat_axis=0, tiled=True
        )
        mixing = jnp.where(picked, weight_of[:, None, :], 0.0).reshape(-1, tok_local)
        own_term = own_term + jnp.einsum(
            "sr,sd->rd", mixing, returned.astype(jnp.float32), precision=highest
        )
    mix_block = mixer_normed.shape[0] // tp_count
    block_rows = mix_block + tok_local
    mix_term = jnp.dot(
        mixer_normed, mixer_output_weight, preferred_element_type=jnp.float32
    ).astype(jnp.bfloat16).reshape(tp_count, mix_block, model_width)
    moe_term = shared_part.astype(jnp.bfloat16).reshape(tp_count, tok_local, model_width)
    row_sums = lax.psum_scatter(
        jnp.concatenate([mix_term, moe_term], axis=1).reshape(tp_count * block_rows, model_width),
        "tp",
        scatter_dimension=0,
        tiled=True,
    )
    mixer_result = row_sums[:mix_block]
    moe_total = row_sums[mix_block:].astype(jnp.float32) + own_term
    return (mixer_result.astype(jnp.bfloat16), moe_total.astype(jnp.bfloat16))


(
    M_META_Y,
    M_ROWS_Y,
    M_DENSE,
    M_MIX_CORE,
    M_MIX_FAR,
    M_MIX_Y,
    M_HALO_H,
    M_HALO_W,
    M_HALO_R,
    M_GATE,
    M_UP,
    M_DOWN,
    M_SGATE,
    M_SUP,
    M_SDOWN,
    M_PAIR_S,
    M_PAIR_D,
    M_PLANE_S,
    M_PLANE_D,
    M_LAST_S,
) = range(20)
B_A, B_AY, B_RY, B_FA, B_BO, B_BY, B_FB = range(7)
SINGLE = 20
BLOCK_KINDS = 7


def block_message(kind, d):
    return SINGLE + BLOCK_KINDS * d + kind


def exchange_kernel(
    ep_count,
    capacity,
    rows_hbm,
    heads_hbm,
    write_hbm,
    read_hbm,
    ogate_hbm,
    proj_hbm,
    gate_hbm,
    up_hbm,
    down_hbm,
    sgate_hbm,
    sup_hbm,
    sdown_hbm,
    routes_ref,
    scores_ref,
    gain_ref,
    step_ref,
    extra_ref,
    decay_ref,
    htaps_ref,
    wtaps_ref,
    rtaps_ref,
    mgain_ref,
    mix_out,
    moe_out,
    rows_v,
    heads_v,
    write_v,
    read_v,
    ogate_v,
    proj_v,
    gate_v,
    up_v,
    down_v,
    sgate_v,
    sup_v,
    sdown_v,
    halo_h,
    halo_w,
    halo_r,
    ext_h,
    ext_w,
    ext_r,
    hval,
    y_v,
    read_b,
    grow_v,
    own_s,
    own_d,
    plane_s,
    plane_d,
    bef_s,
    out_s,
    out_d,
    in_s,
    in_d,
    mix_v,
    mix_r,
    mix_s,
    mix_ry,
    meta_v,
    grp,
    pack_a,
    pack_b,
    xa,
    xb,
    ya,
    yb,
    ry,
    fa,
    ret_a,
    ret_b,
    dense,
    dense_s,
    dense_r,
    load_sem,
    send_sem,
    recv_sem,
):
    f32, bf16 = jnp.float32, jnp.bfloat16
    half = ep_count // 2
    cap = capacity
    tok, width = rows_v.shape
    tok_m, chans = heads_v.shape
    heads = step_ref.shape[0]
    head_dim = chans // heads
    col = 512
    e = lax.axis_index("ep")
    t = lax.axis_index("tp")
    base = (e // half) * half
    q = e - base
    other = half - base
    t_core = t + 1 - 2 * (t % 2)
    t_y = (t + 2) % 4
    t_far = (t_core + 2) % 4
    core, ydev = (e, t_core), (e, t_y)

    def to_a(d):
        return (other + (q + d) % half, t)

    def from_a(d):
        return (other + (q + half - d) % half, t)

    def to_b(d):
        return (base + (q + d) % half, t)

    def from_b(d):
        return (base + (q + half - d) % half, t)

    loads = []
    for src, dst in (
        (rows_hbm, rows_v),
        (heads_hbm, heads_v),
        (write_hbm, write_v),
        (read_hbm, read_v),
        (sgate_hbm, sgate_v.at[0]),
        (sup_hbm, sup_v.at[0]),
        (sdown_hbm, sdown_v.at[0]),
        (gate_hbm, gate_v.at[0]),
        (up_hbm, up_v.at[0]),
        (down_hbm, down_v.at[0]),
        (ogate_hbm, ogate_v),
        (proj_hbm, proj_v),
    ):
        loads.append(pltpu.make_async_copy(src, dst, load_sem.at[len(loads)]))
        loads[-1].start()

    copies = {}

    def prepare(name, src, dst, device):
        copies[name] = pltpu.make_async_remote_copy(
            src_ref=src,
            dst_ref=dst,
            send_sem=send_sem.at[name],
            recv_sem=recv_sem.at[name],
            device_id=device,
            device_id_type=MESH,
        )

    def send(name, src, dst, device):
        prepare(name, src, dst, device)
        copies[name].start()

    def arrived(name):
        copies[name].wait_recv()

    guarded = []

    def send_if(name, src, dst, device, here):
        prepare(name, src, dst, device)
        guarded.append((name, here))

        @pl.when(here)
        def _():
            copies[name].start()

    barrier = pltpu.get_barrier_semaphore()
    peers = [core, ydev] + [to_a(d) for d in range(half)] + [to_b(d) for d in range(1, half)]
    for peer in peers:
        pl.semaphore_signal(barrier, inc=1, device_id=peer, device_id_type=MESH)

    row = lax.broadcasted_iota(jnp.int32, (tok, tok), 0)
    lane = lax.broadcasted_iota(jnp.int32, (tok, tok), 1)
    routed = [routes_ref[k : k + 1, :] for k in range(2)]
    expert_row = lax.broadcasted_iota(jnp.int32, (ep_count, tok), 0)
    chosen = [routed[k] == expert_row for k in range(2)]
    named = jnp.where(chosen[0] | chosen[1], 1.0, 0.0).astype(bf16)
    rank = jnp.dot(
        named, jnp.where(row < lane, 1.0, 0.0).astype(bf16), preferred_element_type=f32
    )
    scores = scores_ref[...].astype(f32)
    total_score = jnp.sum(scores, axis=0, keepdims=True)
    meta_v[0] = jnp.zeros(meta_v.shape[1:], f32)
    for k in range(2):
        meta_v[0, k : k + 1, :] = jnp.sum(
            jnp.where(chosen[k], rank, 0.0), axis=0, keepdims=True
        ) + (routed[k] * cap).astype(f32)
        meta_v[0, 2 + k : 3 + k, :] = scores[k : k + 1, :] / total_score * route_scale

    loads[0].wait()

    def norm_rows(i, carry):
        at = pl.ds(pl.multiple_of(i * 16, 16), 16)
        x = rows_v[at, :].astype(f32)
        scale = lax.rsqrt(jnp.mean(x * x, axis=-1, keepdims=True) + eps_norm)
        grp[0, at, :] = (x * scale * gain_ref[...]).astype(bf16)
        return carry

    lax.fori_loop(0, tok // 16, norm_rows, 0)
    pl.semaphore_wait(barrier, len(peers))

    def pack(pos, expert_at, ref, lead, low):
        places = lax.broadcasted_iota(jnp.int32, (cap, tok), 0) + expert_at * cap
        places = places.astype(f32)
        picked = (places == meta_v[pos, 0:1, :]) | (places == meta_v[pos, 1:2, :])
        picked = jnp.where(picked, 1.0, 0.0).astype(bf16)
        for n in range(0, width, col):
            ref[lead, low : low + cap, n : n + col] = jnp.dot(
                picked, grp[pos, :, n : n + col], preferred_element_type=f32
            ).astype(bf16)

    def rows_out():
        send(M_META_Y, meta_v.at[0], meta_v.at[1], ydev)
        send(M_ROWS_Y, grp.at[0], grp.at[1], ydev)

    def halo_out():
        following = ((e + 1) % ep_count, t)
        kept = halo_h.shape[0]
        tail = pl.ds(tok_m - kept, kept)
        for load in loads[1:4]:
            load.wait()
        send(M_HALO_H, heads_v.at[tail], halo_h, following)
        send(M_HALO_W, write_v.at[tail], halo_w, following)
        send(M_HALO_R, read_v.at[tail], halo_r, following)

    def weights_out():
        send(M_SGATE, sgate_hbm, sgate_v.at[1], core)
        send(M_SUP, sup_hbm, sup_v.at[1], core)
        send(M_SDOWN, sdown_hbm, sdown_v.at[1], core)
        send(M_GATE, gate_hbm, gate_v.at[1], core)
        send(M_UP, up_hbm, up_v.at[1], core)
        send(M_DOWN, down_hbm, down_v.at[1], core)

    def shared_in():
        for load, name in zip(loads[4:7], (M_SGATE, M_SUP, M_SDOWN)):
            load.wait()
            arrived(name)

    def expert_in():
        for load, name in zip(loads[7:10], (M_GATE, M_UP, M_DOWN)):
            load.wait()
            arrived(name)

    def mix_in():
        for load in loads[10:12]:
            load.wait()

    def gated_product(x, first_v, second_v, third_v, put):
        hidden = []
        for s in range(2):
            g = jnp.dot(x, first_v[s], preferred_element_type=f32)
            u = jnp.dot(x, second_v[s], preferred_element_type=f32)
            hidden.append((jax.nn.silu(g) * u).astype(bf16))
        for n in range(0, width, col):
            at = slice(n, n + col)
            put(
                at,
                jnp.dot(hidden[0], third_v[0, :, at], preferred_element_type=f32)
                + jnp.dot(hidden[1], third_v[1, :, at], preferred_element_type=f32),
            )

    def shared_rows(pos):
        def put(at, value):
            dense[pos, :, at] = value

        gated_product(grp[pos], sgate_v, sup_v, sdown_v, put)

    def a0(d):
        pack(0, other + (q + d) % half, pack_a, d, 0)
        send(block_message(B_A, d), pack_a.at[d], xa.at[d, pl.ds(0, cap)], to_a(d))

    def a1(d):
        arrived(block_message(B_A, d))
        send(block_message(B_AY, d), xa.at[d, pl.ds(0, cap)], xa.at[d, pl.ds(cap, cap)], ydev)

    def a3(d):
        arrived(block_message(B_AY, d))

        def put(at, value):
            ya[d, :, at] = value.astype(bf16)

        gated_product(xa[d], gate_v, up_v, down_v, put)
        send(block_message(B_RY, d), ya.at[d, pl.ds(cap, cap)], ry.at[d], ydev)

    def a5(d):
        arrived(block_message(B_RY, d))
        fa[d] = (ya[d, 0:cap].astype(f32) + ry[d].astype(f32)).astype(bf16)
        send(block_message(B_FA, d), fa.at[d], ret_a.at[pl.ds(d * cap, cap)], from_a(d))

    def bo(d):
        pack(0, base + (q + d) % half, pack_b, d - 1, 0)
        send(block_message(B_BO, d), pack_b.at[d - 1, pl.ds(0, cap)], xb.at[d, pl.ds(0, cap)], to_b(d))

    def by(d):
        pack(1, base + (q + d) % half, pack_b, d - 1, cap)
        send(block_message(B_BY, d), pack_b.at[d - 1, pl.ds(cap, cap)], xb.at[d, pl.ds(cap, cap)], to_b(d))

    def b3(d):
        if d:
            arrived(block_message(B_BO, d))
            arrived(block_message(B_BY, d))
        else:
            pack(0, e, xb, 0, 0)
            pack(1, e, xb, 0, cap)

        def put(at, value):
            for p in range(2):
                part = value[p * cap : (p + 1) * cap].astype(bf16)
                if d:
                    yb[d - 1, p, :, at] = part
                else:
                    ret_b[p, 0:cap, at] = part

        gated_product(xb[d], gate_v, up_v, down_v, put)
        if d:
            send(block_message(B_FB, d), yb.at[d - 1], ret_b.at[:, pl.ds(d * cap, cap)], from_b(d))

    def chosen_slots(columns, first):
        lanes = lax.broadcasted_iota(jnp.int32, (1, half * cap), 1)
        code = lanes + (first + q) * cap
        for d in range(1, half):
            moved = (first + (q + d) % half - d) * cap
            code = jnp.where(lanes >= d * cap, lanes + moved, code)
        code = code.astype(f32)
        return [jnp.where(columns[:, k : k + 1] == code, 1.0, 0.0).astype(bf16) for k in range(2)]

    def mixed(columns, picks, returned):
        total = None
        for k in range(2):
            part = columns[:, 2 + k : 3 + k] * jnp.dot(picks[k], returned, preferred_element_type=f32)
            total = part if total is None else total + part
        return total

    def dense_rows(p):
        columns = jnp.transpose(meta_v[p])
        picks = chosen_slots(columns, base)
        for n in range(0, width, col):
            at = slice(n, n + col)
            value = mixed(columns, picks, ret_b[p, :, at]) + dense[p, :, at]
            if p:
                dense_s[:, at] = value.astype(bf16)
            else:
                dense[0, :, at] = value

    def dense_out():
        for d in range(1, half):
            arrived(block_message(B_FB, d))
        dense_rows(1)
        send(M_DENSE, dense_s, dense_r, ydev)
        dense_rows(0)

    def conv(x_v, halo, ext, taps_ref, n, size):
        at = slice(n, n + size)
        taps = taps_ref.shape[0]
        edge = ext.shape[0] - tok_m
        first = halo.shape[0] - edge
        there = jnp.where(e > 0, 1.0, 0.0).astype(f32)
        ext[0:edge, at] = halo[first:, at].astype(f32) * there
        ext[edge:, at] = x_v[:, at].astype(f32)
        total = None
        for j in range(taps):
            low = edge - taps + 1 + j
            part = taps_ref[j : j + 1, at].astype(f32) * ext[low : low + tok_m, at]
            total = part if total is None else total + part
        return jax.nn.silu(total)

    head_row = lax.broadcasted_iota(jnp.int32, (heads, chans), 0)
    lane_head = lax.broadcasted_iota(jnp.int32, (heads, chans), 1) - head_row * head_dim
    spread_b = jnp.where((lane_head >= 0) & (lane_head < head_dim), 1.0, 0.0).astype(bf16)

    def spread(value, terms):
        total, rest = None, value
        for _ in range(terms):
            part = rest.astype(bf16)
            rest = rest - part.astype(f32)
            add = jnp.dot(part, spread_b, preferred_element_type=f32)
            total = add if total is None else total + add
        return total

    local = {}

    def mixer_states():
        for name in (M_HALO_H, M_HALO_W, M_HALO_R):
            arrived(name)
        for n in range(0, chans, 256):
            hval[:, n : n + 256] = conv(heads_v, halo_h, ext_h, htaps_ref, n, 256)
        states = write_v.shape[1]
        write = conv(write_v, halo_w, ext_w, wtaps_ref, 0, states)
        read = conv(read_v, halo_r, ext_r, rtaps_ref, 0, states)
        read_b[...] = read.astype(bf16)
        step = jax.nn.softplus(step_ref[...])
        square_row = lax.broadcasted_iota(jnp.int32, (heads, heads), 0)
        square_lane = lax.broadcasted_iota(jnp.int32, (heads, heads), 1)
        speed = jnp.sum(
            jnp.where(square_row == square_lane, jnp.exp(decay_ref[...]), 0.0), axis=1, keepdims=True
        )
        rate = step * -speed + extra_ref[...]
        upto = jnp.where(row <= lane, 1.0, 0.0).astype(f32)
        cum = jnp.dot(rate, upto, precision=highest, preferred_element_type=f32)
        cum_t = jnp.transpose(cum)
        to_end = jnp.exp(cum[:, tok_m - 1 : tok_m] - cum) * step
        affinity = lax.dot_general(
            read, write, (((1,), (1,)), ((), ())), precision=highest, preferred_element_type=f32
        )
        weights = spread(jnp.transpose(to_end), 2)
        weighted = (hval[...] * weights).astype(bf16)
        own_s[...] = jnp.dot(jnp.transpose(write).astype(bf16), weighted, preferred_element_type=f32)
        own_d[...] = spread(cum_t[tok_m - 8 : tok_m], 3)[7:8]
        local[0] = (cum, cum_t, step, affinity)

    def mixer_rows_local():
        cum, cum_t, step, affinity = local[0]
        grow_v[...] = spread(jnp.exp(cum_t), 2)
        causal = row >= lane
        for pair in range(heads // 2):
            at = slice(pair * 2 * head_dim, (pair + 1) * 2 * head_dim)
            parts = []
            for h in (2 * pair, 2 * pair + 1):
                gap = jnp.where(causal, cum_t[:, h : h + 1] - cum[h : h + 1, :], -jnp.inf)
                parts.append((affinity * jnp.exp(gap) * step[h : h + 1, :]).astype(bf16))
            both = hval[:, at].astype(bf16)
            side = lax.broadcasted_iota(jnp.int32, both.shape, 1) < head_dim
            zero = jnp.zeros_like(both)
            y_v[:, at] = jnp.dot(
                parts[0], jnp.where(side, both, zero), preferred_element_type=f32
            ) + jnp.dot(parts[1], jnp.where(side, zero, both), preferred_element_type=f32)

    side_x, plane, planes = e % 2, e // 2, ep_count // 2
    is_head = side_x == 1 - t % 2
    is_tail = side_x == t % 2
    later_head = is_head & (side_x == 1)
    early_head = is_head & (side_x == 0)
    beside = (e + 1 - 2 * side_x, t)
    above = ((e + 2) % ep_count, t)

    def states_pair():
        @pl.when(is_tail)
        def _():
            out_s[0] = own_s[...].astype(bf16)
            out_d[0] = own_d[...]

        send_if(M_PAIR_S, out_s.at[0], in_s.at[0], beside, is_tail)
        send_if(M_PAIR_D, out_d.at[0], in_d.at[0], beside, is_tail)

    def states_plane():
        prepare(M_PLANE_S, out_s.at[1], in_s.at[1], above)
        prepare(M_PLANE_D, out_d.at[1], in_d.at[1], above)
        guarded.append((M_PLANE_S, is_head & (plane < planes - 1)))
        guarded.append((M_PLANE_D, is_head & (plane < planes - 1)))

        @pl.when(is_head)
        def _():
            arrived(M_PAIR_S)
            arrived(M_PAIR_D)

        @pl.when(later_head)
        def _():
            plane_s[...] = own_s[...] + jnp.exp(own_d[...]) * in_s[0].astype(f32)

        @pl.when(early_head)
        def _():
            plane_s[...] = in_s[0].astype(f32) + jnp.exp(in_d[0]) * own_s[...]

        @pl.when(is_head)
        def _():
            plane_d[...] = own_d[...] + in_d[0]

        @pl.when(is_head & (plane == 0))
        def _():
            in_s[1] = jnp.zeros(in_s.shape[1:], bf16)
            in_d[1] = jnp.zeros(in_d.shape[1:], f32)
            out_s[1] = plane_s[...].astype(bf16)
            out_d[1] = plane_d[...]
            copies[M_PLANE_S].start()
            copies[M_PLANE_D].start()

    def states_up(k):
        @pl.when(is_head & (plane == k))
        def _():
            arrived(M_PLANE_S)
            arrived(M_PLANE_D)
            if k < planes - 1:
                out_s[1] = (plane_s[...] + jnp.exp(plane_d[...]) * in_s[1].astype(f32)).astype(bf16)
                out_d[1] = plane_d[...] + in_d[1]
                copies[M_PLANE_S].start()
                copies[M_PLANE_D].start()

    def states_last():
        @pl.when(later_head)
        def _():
            bef_s[...] = in_s[0].astype(f32) + jnp.exp(in_d[0]) * in_s[1].astype(f32)
            out_s[2] = in_s[1]

        @pl.when(early_head)
        def _():
            bef_s[...] = in_s[1].astype(f32)
            out_s[2] = (own_s[...] + jnp.exp(own_d[...]) * in_s[1].astype(f32)).astype(bf16)

        send_if(M_LAST_S, out_s.at[2], in_s.at[2], beside, is_head)

    def states_in():
        @pl.when(is_tail)
        def _():
            arrived(M_LAST_S)
            bef_s[...] = in_s[2].astype(f32)

    def mixer_finish():
        square = jnp.zeros((tok_m, 1), f32)
        for n in range(0, chans, 256):
            at = slice(n, n + 256)
            carried = jnp.dot(read_b[...], bef_s[:, at].astype(bf16), preferred_element_type=f32)
            value = (y_v[:, at] + carried * grow_v[:, at]) * jax.nn.silu(ogate_v[:, at].astype(f32))
            y_v[:, at] = value
            square = square + jnp.sum(value * value, axis=-1, keepdims=True)
        scale = lax.rsqrt(square / chans + eps_norm)
        normed = (y_v[...] * scale * mgain_ref[...]).astype(bf16)
        block = mix_v.shape[1]
        for n in range(0, width, col):
            part = jnp.dot(normed, proj_v[:, n : n + col], preferred_element_type=f32).astype(bf16)
            for i in range(4):
                mix_v[i, :, n : n + col] = part[i * block : (i + 1) * block]
        send(M_MIX_CORE, mix_v.at[t_core], mix_r.at[0], core)
        send(M_MIX_FAR, mix_v.at[t_far], mix_r.at[1], core)

    def mix_across():
        arrived(M_MIX_CORE)
        arrived(M_MIX_FAR)
        mix_s[...] = (mix_v[t_y].astype(f32) + mix_r[1].astype(f32)).astype(bf16)
        send(M_MIX_Y, mix_s, mix_ry, ydev)

    def rows_in():
        arrived(M_META_Y)
        arrived(M_ROWS_Y)

    halo_out()
    a0(0)
    rows_out()
    bo(1)
    bo(2)
    bo(3)
    mixer_states()
    weights_out()
    states_pair()
    a0(1)
    states_plane()
    mixer_rows_local()
    a0(2)
    a1(0)
    rows_in()
    by(1)
    by(2)
    states_up(1)
    a1(1)
    by(3)
    shared_in()
    shared_rows(0)
    shared_rows(1)
    a0(3)
    expert_in()
    b3(0)
    a3(0)
    states_up(2)
    b3(1)
    b3(2)
    a5(0)
    a3(1)
    a1(2)
    states_up(3)
    states_last()
    a3(2)
    a1(3)
    a5(1)
    b3(3)
    states_in()
    mix_in()
    mixer_finish()
    a5(2)
    a3(3)
    mix_across()
    a5(3)
    dense_out()

    arrived(M_MIX_Y)
    mix_out[...] = (mix_v[t].astype(f32) + mix_r[0].astype(f32) + mix_ry[...].astype(f32)).astype(bf16)
    for d in range(half):
        arrived(block_message(B_FA, d))
    arrived(M_DENSE)
    columns = jnp.transpose(meta_v[0])
    picks = chosen_slots(columns, other)
    for n in range(0, width, col):
        at = slice(n, n + col)
        value = mixed(columns, picks, ret_a[:, at]) + dense[0, :, at] + dense_r[:, at].astype(f32)
        moe_out[:, at] = value.astype(bf16)
    for name, here in guarded:

        @pl.when(here)
        def _(name=name):
            copies[name].wait_send()

    kept_back = [name for name, _ in guarded]
    for name in copies:
        if name not in kept_back:
            copies[name].wait_send()


def settle_kernel(mix_ref, moe_ref, mix_out, moe_out, sem):
    copies = [
        pltpu.make_async_copy(mix_ref, mix_out, sem.at[0]),
        pltpu.make_async_copy(moe_ref, moe_out, sem.at[1]),
    ]
    for copy in copies:
        copy.start()
    for copy in copies:
        copy.wait()


def settle(mix, moe):
    return pl.pallas_call(
        settle_kernel,
        out_shape=tuple(jax.ShapeDtypeStruct(x.shape, x.dtype) for x in (mix, moe)),
        in_specs=[pl.BlockSpec(memory_space=pltpu.VMEM)] * 2,
        out_specs=tuple([pl.BlockSpec(memory_space=pl.ANY)] * 2),
        scratch_shapes=[pltpu.SemaphoreType.DMA((2,))],
        name="settle",
    )(mix, moe)


def exchange(ep_count, capacity, small, large):
    (rows, heads, write, read, ogate, proj, gate, up, down, sgate, sup, sdown) = large
    half = ep_count // 2
    tok, width = rows.shape
    bf16, f32 = jnp.bfloat16, jnp.float32
    cap = capacity
    tok_m, chans = heads.shape
    state = write.shape[1]
    mix_block = tok_m // 4
    count = SINGLE + BLOCK_KINDS * half
    shapes = [(array.shape, bf16) for array in (rows, heads, write, read, ogate, proj)]
    shapes += [((2, *array.shape), bf16) for array in (gate, up, down, sgate, sup, sdown)]
    shapes += [
        ((16, chans), bf16),
        ((16, state), bf16),
        ((16, state), bf16),
        ((tok_m + 8, chans), f32),
        ((tok_m + 8, state), f32),
        ((tok_m + 8, state), f32),
        ((tok_m, chans), f32),
        ((tok_m, chans), f32),
        ((tok_m, state), bf16),
        ((tok_m, chans), f32),
        ((state, chans), f32),
        ((1, chans), f32),
        ((state, chans), f32),
        ((1, chans), f32),
        ((state, chans), f32),
        ((3, state, chans), bf16),
        ((2, 1, chans), f32),
        ((3, state, chans), bf16),
        ((2, 1, chans), f32),
        ((4, mix_block, width), bf16),
        ((2, mix_block, width), bf16),
        ((mix_block, width), bf16),
        ((mix_block, width), bf16),
        ((2, 8, tok), f32),
        ((2, tok, width), bf16),
        ((half, cap, width), bf16),
        ((half - 1, 2 * cap, width), bf16),
        ((half, 2 * cap, width), bf16),
        ((half, 2 * cap, width), bf16),
        ((half, 2 * cap, width), bf16),
        ((half - 1, 2, cap, width), bf16),
        ((half, cap, width), bf16),
        ((half, cap, width), bf16),
        ((half * cap, width), bf16),
        ((2, half * cap, width), bf16),
        ((2, tok, width), f32),
        ((tok, width), bf16),
        ((tok, width), bf16),
    ]
    any_spec = pl.BlockSpec(memory_space=pl.ANY)
    vmem_spec = pl.BlockSpec(memory_space=pltpu.VMEM)
    return pl.pallas_call(
        functools.partial(exchange_kernel, ep_count, capacity),
        out_shape=(
            jax.ShapeDtypeStruct((mix_block, width), bf16),
            jax.ShapeDtypeStruct((tok, width), bf16),
        ),
        in_specs=[any_spec] * len(large) + [vmem_spec] * len(small),
        out_specs=(vmem_spec, vmem_spec),
        scratch_shapes=[pltpu.VMEM(shape, dtype) for shape, dtype in shapes]
        + [
            pltpu.SemaphoreType.DMA((len(large),)),
            pltpu.SemaphoreType.DMA((count,)),
            pltpu.SemaphoreType.DMA((count,)),
        ],
        compiler_params=pltpu.CompilerParams(
            collective_id=0, has_side_effects=True, vmem_limit_bytes=62 * 1024 * 1024
        ),
        name="mixer_and_experts",
    )(*large, *small)


def direct(
    head_inputs_unfiltered,
    group_write_vectors,
    group_read_vectors,
    output_gate_inputs,
    step_preactivation,
    extra_decay_logs,
    head_decay_logs,
    head_filter_taps,
    write_filter_taps,
    read_filter_taps,
    grouped_norm_gain,
    mixer_output_weight,
    expert_input_rows,
    expert_norm_gain,
    routes,
    router_chosen_scores,
    routed_gate_weight,
    routed_up_weight,
    routed_down_weight,
    shared_gate_weight,
    shared_up_weight,
    shared_down_weight,
):
    ep_count = lax.axis_size("ep")
    capacity = 3 * expert_input_rows.shape[0] * routes.shape[1] // (2 * ep_count)
    small = (
        routes.T,
        router_chosen_scores.T,
        expert_norm_gain.reshape(1, -1),
        step_preactivation,
        extra_decay_logs,
        head_decay_logs.reshape(1, -1),
        head_filter_taps,
        write_filter_taps,
        read_filter_taps,
        grouped_norm_gain.reshape(1, -1),
    )
    large = (
        expert_input_rows,
        head_inputs_unfiltered,
        group_write_vectors,
        group_read_vectors,
        output_gate_inputs,
        mixer_output_weight,
        routed_gate_weight[0],
        routed_up_weight[0],
        routed_down_weight[0],
        shared_gate_weight,
        shared_up_weight,
        shared_down_weight,
    )
    return settle(*exchange(ep_count, capacity, small, large))


def fits_direct(mesh, rows, mix_rows, top_count, experts, groups):
    ep_count, tp_count = mesh.shape["ep"], mesh.shape["tp"]
    tok_local = rows // (ep_count * tp_count)
    capacity = 3 * tok_local * top_count // (2 * experts)
    return (
        tp_count == 4
        and groups == tp_count
        and experts == ep_count
        and ep_count == 8
        and top_count == 2
        and capacity % 16 == 0
        and tok_local == 128
        and mix_rows == tok_local * ep_count
    )


def solution(mesh):
    in_specs = (
        P("ep", "tp"),
        P("ep", "tp"),
        P("ep", "tp"),
        P("ep", "tp"),
        P("tp", "ep"),
        P("tp", "ep"),
        P("tp"),
        P(None, "tp"),
        P(None, "tp"),
        P(None, "tp"),
        P("tp"),
        P("tp", None),
        P(("ep", "tp"), None),
        P(),
        P(("ep", "tp"), None),
        P(("ep", "tp"), None),
        P("ep", None, "tp"),
        P("ep", None, "tp"),
        P("ep", "tp", None),
        P(None, "tp"),
        P(None, "tp"),
        P("tp", None),
    )
    out_specs = (P(("ep", "tp"), None), P(("ep", "tp"), None))
    def step(*args):
        direct_form = fits_direct(
            mesh,
            args[12].shape[0],
            args[0].shape[0],
            args[14].shape[1],
            args[16].shape[0],
            args[1].shape[1] // STATE,
        )
        return jax.shard_map(
            direct if direct_form else local,
            mesh=mesh,
            in_specs=in_specs,
            out_specs=out_specs,
            check_vma=False,
        )(*args)

    return step
```

```python
import functools

import jax
import jax.numpy as jnp
from jax import lax
from jax.experimental import pallas as pl
from jax.experimental.pallas import tpu as pltpu
from jax.sharding import PartitionSpec as P

MESH = pl.DeviceIdType.MESH
HEAD_DIM = 64
STATE = 128
BLOCK = 64


eps_norm = 1e-06
route_scale = 2.5
highest = lax.Precision.HIGHEST


def from_behind(value, axis, by):
    devices = lax.axis_size(axis)
    pairs = [(i, i + by) for i in range(devices) if 0 <= i + by < devices]
    return lax.ppermute(value, axis, pairs)


def sent_state(decay, state, axis, by):
    heads, width = decay.shape[0], state.shape[-1]
    parts, rest = [], decay
    for _ in range(3):
        part = lax.reduce_precision(rest, exponent_bits=8, mantissa_bits=7)
        parts.append(part)
        rest = rest - part
    decay_rows = jnp.pad(jnp.stack(parts, axis=1), ((0, 0), (0, width - 3)))
    packed = jnp.concatenate([state.reshape(-1, width), decay_rows], axis=0).astype(jnp.bfloat16)
    packed = from_behind(packed, axis, by).astype(jnp.float32)
    return jnp.sum(packed[-heads:, :3], axis=-1), packed[:-heads].reshape(state.shape)


def carried_in(decay, state, axis):
    shape = state.shape
    own = (decay.reshape(-1), state.reshape((-1,) + shape[-2:]))
    before, by = None, 1
    while by < lax.axis_size(axis):
        span = own if before is None else combine_states(before, own)
        received = sent_state(*span, axis, by)
        before = received if before is None else combine_states(received, before)
        by *= 2
    if before is None:
        return jnp.zeros_like(state)
    return before[1].reshape(shape)


def combine_states(earlier_part, later_part):
    return (
        earlier_part[0] + later_part[0],
        later_part[1] + jnp.exp(later_part[0])[..., None, None] * earlier_part[1],
    )


def conv_silu(values, weights):
    taps = weights.shape[0]
    length = values.shape[0] - taps + 1
    running_sum = jnp.zeros((length, values.shape[1]), jnp.float32)
    for offset in range(taps):
        running_sum = running_sum + weights[offset].astype(jnp.float32) * values[
            offset : offset + length
        ].astype(jnp.float32)
    return jax.nn.silu(running_sum)


def tail_rows_from_behind(head_inputs, write_vectors, read_vectors, taps):
    start = head_inputs.shape[0] - taps + 1
    tail_rows = jnp.concatenate([head_inputs[start:], write_vectors[start:], read_vectors[start:]], axis=1)
    return from_behind(tail_rows, "ep", 1)


def mixer_rows(
    earlier,
    head_inputs_unfiltered,
    group_write_vectors,
    group_read_vectors,
    output_gate_inputs,
    step_preactivation,
    extra_decay_logs,
    head_decay_logs,
    head_filter_taps,
    write_filter_taps,
    read_filter_taps,
    grouped_norm_gain,
):
    row_total = head_inputs_unfiltered.shape[0]
    head_chans = head_inputs_unfiltered.shape[1]
    write_chans = group_write_vectors.shape[1]
    padded_heads = jnp.concatenate([earlier[:, :head_chans], head_inputs_unfiltered], axis=0)
    padded_write = jnp.concatenate(
        [earlier[:, head_chans : head_chans + write_chans], group_write_vectors], axis=0
    )
    padded_read = jnp.concatenate(
        [earlier[:, head_chans + write_chans :], group_read_vectors], axis=0
    )
    heads_local = step_preactivation.shape[0]
    groups_local = write_chans // STATE
    per_group = heads_local // groups_local
    block_count = row_total // BLOCK
    head_values = conv_silu(padded_heads, head_filter_taps).reshape(
        block_count, BLOCK, groups_local, per_group, HEAD_DIM
    )
    write_values = conv_silu(padded_write, write_filter_taps).reshape(
        block_count, BLOCK, groups_local, STATE
    )
    read_values = conv_silu(padded_read, read_filter_taps).reshape(
        block_count, BLOCK, groups_local, STATE
    )
    step_length_value = jax.nn.softplus(step_preactivation)
    decay_rate_logs = -jnp.exp(head_decay_logs)[:, None] * step_length_value + extra_decay_logs
    step_blocks = step_length_value.reshape(groups_local, per_group, block_count, BLOCK)
    cumulative = jnp.cumsum(
        decay_rate_logs.reshape(groups_local, per_group, block_count, BLOCK), axis=3
    )
    weighted = head_values * jnp.transpose(step_blocks, (2, 3, 0, 1))[..., None]
    lower_mask = jnp.tril(jnp.ones((BLOCK, BLOCK), bool))
    gap_logs = cumulative[..., :, None] - cumulative[..., None, :]
    within = jnp.exp(jnp.where(lower_mask, gap_logs, -jnp.inf))
    affinity = jnp.einsum("blgn,bsgn->gbls", read_values, write_values, precision=highest)
    local_part = jnp.einsum(
        "gebls,bsgep->blgep", affinity[:, None] * within, weighted, precision=highest
    )
    to_end = jnp.exp(cumulative[..., -1:] - cumulative)
    block_states = jnp.einsum(
        "bsgn,bsgep,gebs->bgepn", write_values, weighted, to_end, precision=highest
    )
    block_decay = cumulative[..., -1]
    running = jnp.cumsum(block_decay, axis=2)
    entering = running - block_decay
    earlier_blocks = jnp.tril(jnp.ones((block_count, block_count), bool), -1)
    block_ratio = entering[..., :, None] - running[..., None, :]
    carry_weights = jnp.exp(jnp.where(earlier_blocks, block_ratio, -jnp.inf))
    inside = jnp.einsum("gebc,cgepn->bgepn", carry_weights, block_states, precision=highest)
    device_decay = running[..., -1]
    device_state = jnp.einsum(
        "gec,cgepn->gepn",
        jnp.exp(device_decay[..., None] - running),
        block_states,
        precision=highest,
    )
    incoming = carried_in(device_decay, device_state, "ep")
    states_in = (
        inside + jnp.exp(jnp.transpose(entering, (2, 0, 1)))[..., None, None] * incoming[None]
    )
    carried_part = (
        jnp.einsum("blgn,bgepn->blgep", read_values, states_in, precision=highest)
        * jnp.transpose(jnp.exp(cumulative), (2, 3, 0, 1))[..., None]
    )
    scan_out = (local_part + carried_part).reshape(row_total, groups_local, per_group * HEAD_DIM)
    gate_values = jax.nn.silu(output_gate_inputs.astype(jnp.float32)).reshape(
        row_total, groups_local, per_group * HEAD_DIM
    )
    gated_rows = scan_out * gate_values
    gated_rows = gated_rows * lax.rsqrt(
        jnp.mean(gated_rows * gated_rows, axis=-1, keepdims=True) + eps_norm
    )
    return (gated_rows.reshape(row_total, head_chans) * grouped_norm_gain).astype(jnp.bfloat16)


def local(
    head_inputs_unfiltered,
    group_write_vectors,
    group_read_vectors,
    output_gate_inputs,
    step_preactivation,
    extra_decay_logs,
    head_decay_logs,
    head_filter_taps,
    write_filter_taps,
    read_filter_taps,
    grouped_norm_gain,
    mixer_output_weight,
    expert_input_rows,
    expert_norm_gain,
    routes,
    router_chosen_scores,
    routed_gate_weight,
    routed_up_weight,
    routed_down_weight,
    shared_gate_weight,
    shared_up_weight,
    shared_down_weight,
):
    earlier = tail_rows_from_behind(
        head_inputs_unfiltered, group_write_vectors, group_read_vectors, head_filter_taps.shape[0]
    )
    tp_count = lax.axis_size("tp")
    ep_count = lax.axis_size("ep")
    tok_local = expert_input_rows.shape[0]
    model_width = expert_input_rows.shape[1]
    top_count = routes.shape[1]
    local_experts = routed_gate_weight.shape[0]
    experts = local_experts * ep_count
    capacity = 3 * tok_local * top_count // (2 * experts)
    rows_float = expert_input_rows.astype(jnp.float32)
    normed = (
        rows_float
        * lax.rsqrt(jnp.mean(rows_float * rows_float, axis=-1, keepdims=True) + eps_norm)
        * expert_norm_gain
    ).astype(jnp.bfloat16)
    score_float = router_chosen_scores.astype(jnp.float32)
    weights = score_float / jnp.sum(score_float, axis=1, keepdims=True) * route_scale
    choice = routes[None, :, :] == jnp.arange(experts, dtype=jnp.int32)[:, None, None]
    named = jnp.any(choice, axis=2)
    weight_of = jnp.sum(jnp.where(choice, weights[None], 0.0), axis=2)
    row_order = jnp.arange(tok_local, dtype=jnp.int32)
    earlier_rows = (row_order[:, None] < row_order[None, :]).astype(jnp.bfloat16)
    rank = jnp.dot(
        named.astype(jnp.bfloat16), earlier_rows, preferred_element_type=jnp.float32
    ).astype(jnp.int32)

    cuts = [0, capacity // 2, capacity] if capacity > 1 else [0, capacity]
    picks, outgoing = [], []
    for low, high in zip(cuts[:-1], cuts[1:]):
        places = jnp.arange(low, high, dtype=jnp.int32)
        picked = named[:, None, :] & (rank[:, None, :] == places[None, :, None])
        picks.append(picked)
        outgoing.append(
            jnp.dot(
                picked.reshape(-1, tok_local).astype(jnp.bfloat16),
                normed,
                preferred_element_type=jnp.float32,
            ).astype(jnp.bfloat16)
        )
    group_rows = lax.all_gather(normed, "tp", axis=0, tiled=True)
    earlier, group_rows, outgoing[0] = lax.optimization_barrier((earlier, group_rows, outgoing[0]))

    arrived = []
    for block in outgoing:
        arrived.append(lax.all_to_all(block, "ep", split_axis=0, concat_axis=0, tiled=True))
    gathered = [lax.all_gather(block, "tp", axis=0) for block in arrived]

    shared_hidden = (
        jax.nn.silu(jnp.dot(group_rows, shared_gate_weight, preferred_element_type=jnp.float32))
        * jnp.dot(group_rows, shared_up_weight, preferred_element_type=jnp.float32)
    ).astype(jnp.bfloat16)
    shared_part = jnp.dot(shared_hidden, shared_down_weight, preferred_element_type=jnp.float32)

    mixer_normed = mixer_rows(
        earlier,
        head_inputs_unfiltered,
        group_write_vectors,
        group_read_vectors,
        output_gate_inputs,
        step_preactivation,
        extra_decay_logs,
        head_decay_logs,
        head_filter_taps,
        write_filter_taps,
        read_filter_taps,
        grouped_norm_gain,
    )

    def expert_rows(block):
        sources = block.reshape(tp_count, ep_count, local_experts, -1, model_width)
        gate_value = jnp.einsum(
            "osecd,edf->osecf", sources, routed_gate_weight, preferred_element_type=jnp.float32
        )
        up_value = jnp.einsum(
            "osecd,edf->osecf", sources, routed_up_weight, preferred_element_type=jnp.float32
        )
        hidden = (jax.nn.silu(gate_value) * up_value).astype(jnp.bfloat16)
        partial_value = jnp.einsum(
            "osecf,efd->osecd", hidden, routed_down_weight, preferred_element_type=jnp.float32
        ).astype(jnp.bfloat16)
        return lax.psum_scatter(
            partial_value.reshape(-1, model_width), "tp", scatter_dimension=0, tiled=True
        )

    own_term = jnp.zeros((tok_local, model_width), jnp.float32)
    for block, picked in zip(gathered, picks):
        returned = lax.all_to_all(
            expert_rows(block), "ep", split_axis=0, concat_axis=0, tiled=True
        )
        mixing = jnp.where(picked, weight_of[:, None, :], 0.0).reshape(-1, tok_local)
        own_term = own_term + jnp.einsum(
            "sr,sd->rd", mixing, returned.astype(jnp.float32), precision=highest
        )
    mix_block = mixer_normed.shape[0] // tp_count
    block_rows = mix_block + tok_local
    mix_term = jnp.dot(
        mixer_normed, mixer_output_weight, preferred_element_type=jnp.float32
    ).astype(jnp.bfloat16).reshape(tp_count, mix_block, model_width)
    moe_term = shared_part.astype(jnp.bfloat16).reshape(tp_count, tok_local, model_width)
    row_sums = lax.psum_scatter(
        jnp.concatenate([mix_term, moe_term], axis=1).reshape(tp_count * block_rows, model_width),
        "tp",
        scatter_dimension=0,
        tiled=True,
    )
    mixer_result = row_sums[:mix_block]
    moe_total = row_sums[mix_block:].astype(jnp.float32) + own_term
    return (mixer_result.astype(jnp.bfloat16), moe_total.astype(jnp.bfloat16))


(
    M_META_Y,
    M_ROWS_Y,
    M_DENSE,
    M_MIX_CORE,
    M_MIX_FAR,
    M_MIX_Y,
    M_HALO_H,
    M_HALO_W,
    M_HALO_R,
    M_GATE,
    M_UP,
    M_DOWN,
    M_SGATE,
    M_SUP,
    M_SDOWN,
    M_PAIR_S,
    M_PAIR_D,
    M_PLANE_S,
    M_PLANE_D,
    M_LAST_S,
) = range(20)
B_A, B_AY, B_RY, B_FA, B_BO, B_BY, B_FB = range(7)
SINGLE = 20
BLOCK_KINDS = 7


def block_message(kind, d):
    return SINGLE + BLOCK_KINDS * d + kind


def exchange_kernel(
    ep_count,
    capacity,
    rows_hbm,
    heads_hbm,
    write_hbm,
    read_hbm,
    ogate_hbm,
    proj_hbm,
    gate_hbm,
    up_hbm,
    down_hbm,
    sgate_hbm,
    sup_hbm,
    sdown_hbm,
    routes_ref,
    scores_ref,
    gain_ref,
    step_ref,
    extra_ref,
    decay_ref,
    htaps_ref,
    wtaps_ref,
    rtaps_ref,
    mgain_ref,
    mix_out,
    moe_out,
    rows_v,
    heads_v,
    write_v,
    read_v,
    ogate_v,
    proj_v,
    gate_v,
    up_v,
    down_v,
    sgate_v,
    sup_v,
    sdown_v,
    halo_h,
    halo_w,
    halo_r,
    ext_h,
    ext_w,
    ext_r,
    hval,
    write_f,
    read_f,
    weights_f,
    y_v,
    read_b,
    grow_v,
    own_s,
    own_d,
    plane_s,
    plane_d,
    bef_s,
    out_s,
    out_d,
    in_s,
    in_d,
    mix_v,
    mix_r,
    mix_s,
    mix_ry,
    meta_v,
    grp,
    pack_a,
    pack_b,
    xa,
    xb,
    ya,
    yb,
    ry,
    fa,
    ret_a,
    ret_b,
    dense,
    dense_s,
    dense_r,
    load_sem,
    send_sem,
    recv_sem,
):
    f32, bf16 = jnp.float32, jnp.bfloat16
    half = ep_count // 2
    cap = capacity
    tok, width = rows_v.shape
    tok_m, chans = heads_v.shape
    heads = step_ref.shape[0]
    head_dim = chans // heads
    col = 512
    e = lax.axis_index("ep")
    t = lax.axis_index("tp")
    base = (e // half) * half
    q = e - base
    other = half - base
    t_core = t + 1 - 2 * (t % 2)
    t_y = (t + 2) % 4
    t_far = (t_core + 2) % 4
    core, ydev = (e, t_core), (e, t_y)

    def to_a(d):
        return (other + (q + d) % half, t)

    def from_a(d):
        return (other + (q + half - d) % half, t)

    def to_b(d):
        return (base + (q + d) % half, t)

    def from_b(d):
        return (base + (q + half - d) % half, t)

    loads = []
    for src, dst in (
        (rows_hbm, rows_v),
        (heads_hbm, heads_v),
        (write_hbm, write_v),
        (read_hbm, read_v),
        (sgate_hbm, sgate_v.at[0]),
        (sup_hbm, sup_v.at[0]),
        (sdown_hbm, sdown_v.at[0]),
        (gate_hbm, gate_v.at[0]),
        (up_hbm, up_v.at[0]),
        (down_hbm, down_v.at[0]),
        (ogate_hbm, ogate_v),
        (proj_hbm, proj_v),
    ):
        loads.append(pltpu.make_async_copy(src, dst, load_sem.at[len(loads)]))
        loads[-1].start()

    copies = {}

    def prepare(name, src, dst, device):
        copies[name] = pltpu.make_async_remote_copy(
            src_ref=src,
            dst_ref=dst,
            send_sem=send_sem.at[name],
            recv_sem=recv_sem.at[name],
            device_id=device,
            device_id_type=MESH,
        )

    def send(name, src, dst, device):
        prepare(name, src, dst, device)
        copies[name].start()

    def arrived(name):
        copies[name].wait_recv()

    guarded = []

    def send_if(name, src, dst, device, here):
        prepare(name, src, dst, device)
        guarded.append((name, here))

        @pl.when(here)
        def _():
            copies[name].start()

    barrier = pltpu.get_barrier_semaphore()
    peers = [core, ydev] + [to_a(d) for d in range(half)] + [to_b(d) for d in range(1, half)]
    for peer in peers:
        pl.semaphore_signal(barrier, inc=1, device_id=peer, device_id_type=MESH)

    row = lax.broadcasted_iota(jnp.int32, (tok, tok), 0)
    lane = lax.broadcasted_iota(jnp.int32, (tok, tok), 1)
    routed = [routes_ref[k : k + 1, :] for k in range(2)]
    expert_row = lax.broadcasted_iota(jnp.int32, (ep_count, tok), 0)
    chosen = [routed[k] == expert_row for k in range(2)]
    named = jnp.where(chosen[0] | chosen[1], 1.0, 0.0).astype(bf16)
    rank = jnp.dot(
        named, jnp.where(row < lane, 1.0, 0.0).astype(bf16), preferred_element_type=f32
    )
    scores = scores_ref[...].astype(f32)
    total_score = jnp.sum(scores, axis=0, keepdims=True)
    meta_v[0] = jnp.zeros(meta_v.shape[1:], f32)
    for k in range(2):
        meta_v[0, k : k + 1, :] = jnp.sum(
            jnp.where(chosen[k], rank, 0.0), axis=0, keepdims=True
        ) + (routed[k] * cap).astype(f32)
        meta_v[0, 2 + k : 3 + k, :] = scores[k : k + 1, :] / total_score * route_scale

    loads[0].wait()

    def norm_rows(i, carry):
        at = pl.ds(pl.multiple_of(i * 16, 16), 16)
        x = rows_v[at, :].astype(f32)
        scale = lax.rsqrt(jnp.mean(x * x, axis=-1, keepdims=True) + eps_norm)
        grp[0, at, :] = (x * scale * gain_ref[...]).astype(bf16)
        return carry

    lax.fori_loop(0, tok // 16, norm_rows, 0)

    def pack(pos, expert_at, ref, lead, low):
        places = lax.broadcasted_iota(jnp.int32, (cap, tok), 0) + expert_at * cap
        places = places.astype(f32)
        picked = (places == meta_v[pos, 0:1, :]) | (places == meta_v[pos, 1:2, :])
        picked = jnp.where(picked, 1.0, 0.0).astype(bf16)
        for n in range(0, width, col):
            ref[lead, low : low + cap, n : n + col] = jnp.dot(
                picked, grp[pos, :, n : n + col], preferred_element_type=f32
            ).astype(bf16)

    def rows_out():
        send(M_META_Y, meta_v.at[0], meta_v.at[1], ydev)
        send(M_ROWS_Y, grp.at[0], grp.at[1], ydev)

    def halo_out():
        following = ((e + 1) % ep_count, t)
        kept = halo_h.shape[0]
        tail = pl.ds(tok_m - kept, kept)
        for load in loads[1:4]:
            load.wait()
        send(M_HALO_H, heads_v.at[tail], halo_h, following)
        send(M_HALO_W, write_v.at[tail], halo_w, following)
        send(M_HALO_R, read_v.at[tail], halo_r, following)

    def weights_out():
        send(M_SGATE, sgate_hbm, sgate_v.at[1], core)
        send(M_SUP, sup_hbm, sup_v.at[1], core)
        send(M_SDOWN, sdown_hbm, sdown_v.at[1], core)
        send(M_GATE, gate_hbm, gate_v.at[1], core)
        send(M_UP, up_hbm, up_v.at[1], core)
        send(M_DOWN, down_hbm, down_v.at[1], core)

    def shared_in():
        for load, name in zip(loads[4:7], (M_SGATE, M_SUP, M_SDOWN)):
            load.wait()
            arrived(name)

    def expert_in():
        for load, name in zip(loads[7:10], (M_GATE, M_UP, M_DOWN)):
            load.wait()
            arrived(name)

    def mix_in():
        for load in loads[10:12]:
            load.wait()

    def gated_product(x, first_v, second_v, third_v, put):
        hidden = []
        for s in range(2):
            g = jnp.dot(x, first_v[s], preferred_element_type=f32)
            u = jnp.dot(x, second_v[s], preferred_element_type=f32)
            hidden.append((jax.nn.silu(g) * u).astype(bf16))
        for n in range(0, width, col):
            at = slice(n, n + col)
            put(
                at,
                jnp.dot(hidden[0], third_v[0, :, at], preferred_element_type=f32)
                + jnp.dot(hidden[1], third_v[1, :, at], preferred_element_type=f32),
            )

    def shared_rows(pos):
        def put(at, value):
            dense[pos, :, at] = value

        gated_product(grp[pos], sgate_v, sup_v, sdown_v, put)

    def a0(d):
        pack(0, other + (q + d) % half, pack_a, d, 0)
        send(block_message(B_A, d), pack_a.at[d], xa.at[d, pl.ds(0, cap)], to_a(d))

    def a1(d):
        arrived(block_message(B_A, d))
        send(block_message(B_AY, d), xa.at[d, pl.ds(0, cap)], xa.at[d, pl.ds(cap, cap)], ydev)

    def a3(d):
        arrived(block_message(B_AY, d))

        def put(at, value):
            ya[d, :, at] = value.astype(bf16)

        gated_product(xa[d], gate_v, up_v, down_v, put)
        send(block_message(B_RY, d), ya.at[d, pl.ds(cap, cap)], ry.at[d], ydev)

    def a5(d):
        arrived(block_message(B_RY, d))
        fa[d] = (ya[d, 0:cap].astype(f32) + ry[d].astype(f32)).astype(bf16)
        send(block_message(B_FA, d), fa.at[d], ret_a.at[pl.ds(d * cap, cap)], from_a(d))

    def bo(d):
        pack(0, base + (q + d) % half, pack_b, d - 1, 0)
        send(block_message(B_BO, d), pack_b.at[d - 1, pl.ds(0, cap)], xb.at[d, pl.ds(0, cap)], to_b(d))

    def by(d):
        pack(1, base + (q + d) % half, pack_b, d - 1, cap)
        send(block_message(B_BY, d), pack_b.at[d - 1, pl.ds(cap, cap)], xb.at[d, pl.ds(cap, cap)], to_b(d))

    def b3(d):
        if d:
            arrived(block_message(B_BO, d))
            arrived(block_message(B_BY, d))
        else:
            pack(0, e, xb, 0, 0)
            pack(1, e, xb, 0, cap)

        def put(at, value):
            for p in range(2):
                part = value[p * cap : (p + 1) * cap].astype(bf16)
                if d:
                    yb[d - 1, p, :, at] = part
                else:
                    ret_b[p, 0:cap, at] = part

        gated_product(xb[d], gate_v, up_v, down_v, put)
        if d:
            send(block_message(B_FB, d), yb.at[d - 1], ret_b.at[:, pl.ds(d * cap, cap)], from_b(d))

    def chosen_slots(columns, first):
        lanes = lax.broadcasted_iota(jnp.int32, (1, half * cap), 1)
        code = lanes + (first + q) * cap
        for d in range(1, half):
            moved = (first + (q + d) % half - d) * cap
            code = jnp.where(lanes >= d * cap, lanes + moved, code)
        code = code.astype(f32)
        return [jnp.where(columns[:, k : k + 1] == code, 1.0, 0.0).astype(bf16) for k in range(2)]

    def mixed(columns, picks, returned):
        total = None
        for k in range(2):
            part = columns[:, 2 + k : 3 + k] * jnp.dot(picks[k], returned, preferred_element_type=f32)
            total = part if total is None else total + part
        return total

    def dense_rows(p):
        columns = jnp.transpose(meta_v[p])
        picks = chosen_slots(columns, base)
        for n in range(0, width, col):
            at = slice(n, n + col)
            value = mixed(columns, picks, ret_b[p, :, at]) + dense[p, :, at]
            if p:
                dense_s[:, at] = value.astype(bf16)
            else:
                dense[0, :, at] = value

    def dense_out():
        for d in range(1, half):
            arrived(block_message(B_FB, d))
        dense_rows(1)
        send(M_DENSE, dense_s, dense_r, ydev)
        dense_rows(0)

    def taps_sum(ext, taps_ref, at, length):
        taps = taps_ref.shape[0]
        edge = ext.shape[0] - tok_m
        total = None
        for j in range(taps):
            low = edge - taps + 1 + j
            part = taps_ref[j : j + 1, at].astype(f32) * ext[low : low + length, at]
            total = part if total is None else total + part
        return jax.nn.silu(total)

    def conv(x_v, ext, taps_ref, n, size):
        at = slice(n, n + size)
        edge = ext.shape[0] - tok_m
        ext[0:edge, at] = jnp.zeros((edge, size), f32)
        ext[edge:, at] = x_v[:, at].astype(f32)
        return taps_sum(ext, taps_ref, at, tok_m)

    def conv_first(halo, ext, taps_ref, n, size):
        at = slice(n, n + size)
        edge = ext.shape[0] - tok_m
        there = jnp.where(e > 0, 1.0, 0.0).astype(f32)
        ext[0:edge, at] = halo[halo.shape[0] - edge :, at].astype(f32) * there
        return taps_sum(ext, taps_ref, at, edge)

    head_row = lax.broadcasted_iota(jnp.int32, (heads, chans), 0)
    lane_head = lax.broadcasted_iota(jnp.int32, (heads, chans), 1) - head_row * head_dim
    spread_b = jnp.where((lane_head >= 0) & (lane_head < head_dim), 1.0, 0.0).astype(bf16)

    def spread(value, terms):
        total, rest = None, value
        for _ in range(terms):
            part = rest.astype(bf16)
            rest = rest - part.astype(f32)
            add = jnp.dot(part, spread_b, preferred_element_type=f32)
            total = add if total is None else total + add
        return total

    local = {}

    def mixer_early():
        for n in range(0, chans, 256):
            hval[:, n : n + 256] = conv(heads_v, ext_h, htaps_ref, n, 256)
        states = write_v.shape[1]
        write_f[...] = conv(write_v, ext_w, wtaps_ref, 0, states)
        read_f[...] = conv(read_v, ext_r, rtaps_ref, 0, states)
        step = jax.nn.softplus(step_ref[...])
        square_row = lax.broadcasted_iota(jnp.int32, (heads, heads), 0)
        square_lane = lax.broadcasted_iota(jnp.int32, (heads, heads), 1)
        speed = jnp.sum(
            jnp.where(square_row == square_lane, jnp.exp(decay_ref[...]), 0.0), axis=1, keepdims=True
        )
        rate = step * -speed + extra_ref[...]
        upto = jnp.where(row <= lane, 1.0, 0.0).astype(f32)
        cum = jnp.dot(rate, upto, precision=highest, preferred_element_type=f32)
        cum_t = jnp.transpose(cum)
        to_end = jnp.exp(cum[:, tok_m - 1 : tok_m] - cum) * step
        weights_f[...] = spread(jnp.transpose(to_end), 2)
        own_d[...] = spread(cum_t[tok_m - 8 : tok_m], 3)[7:8]
        grow_v[...] = spread(jnp.exp(cum_t), 2)
        local[0] = (cum, cum_t, step)

    def mixer_states():
        for name in (M_HALO_H, M_HALO_W, M_HALO_R):
            arrived(name)
        edge = ext_h.shape[0] - tok_m
        for n in range(0, chans, 256):
            hval[0:edge, n : n + 256] = conv_first(halo_h, ext_h, htaps_ref, n, 256)
        states = write_v.shape[1]
        write_f[0:edge, :] = conv_first(halo_w, ext_w, wtaps_ref, 0, states)
        read_f[0:edge, :] = conv_first(halo_r, ext_r, rtaps_ref, 0, states)
        weighted = (hval[...] * weights_f[...]).astype(bf16)
        own_s[...] = jnp.dot(
            jnp.transpose(write_f[...]).astype(bf16), weighted, preferred_element_type=f32
        )

    def mixer_rows_local():
        cum, cum_t, step = local[0]
        read_b[...] = read_f[...].astype(bf16)
        affinity = lax.dot_general(
            read_f[...],
            write_f[...],
            (((1,), (1,)), ((), ())),
            precision=highest,
            preferred_element_type=f32,
        )
        causal = row >= lane
        for pair in range(heads // 2):
            at = slice(pair * 2 * head_dim, (pair + 1) * 2 * head_dim)
            parts = []
            for h in (2 * pair, 2 * pair + 1):
                gap = jnp.where(causal, cum_t[:, h : h + 1] - cum[h : h + 1, :], -jnp.inf)
                parts.append((affinity * jnp.exp(gap) * step[h : h + 1, :]).astype(bf16))
            both = hval[:, at].astype(bf16)
            side = lax.broadcasted_iota(jnp.int32, both.shape, 1) < head_dim
            zero = jnp.zeros_like(both)
            y_v[:, at] = jnp.dot(
                parts[0], jnp.where(side, both, zero), preferred_element_type=f32
            ) + jnp.dot(parts[1], jnp.where(side, zero, both), preferred_element_type=f32)

    side_x, plane, planes = e % 2, e // 2, ep_count // 2
    is_head = side_x == 1 - t % 2
    is_tail = side_x == t % 2
    later_head = is_head & (side_x == 1)
    early_head = is_head & (side_x == 0)
    beside = (e + 1 - 2 * side_x, t)
    above = ((e + 2) % ep_count, t)

    def states_pair():
        @pl.when(is_tail)
        def _():
            out_s[0] = own_s[...].astype(bf16)
            out_d[0] = own_d[...]

        send_if(M_PAIR_S, out_s.at[0], in_s.at[0], beside, is_tail)
        send_if(M_PAIR_D, out_d.at[0], in_d.at[0], beside, is_tail)

    def states_plane():
        prepare(M_PLANE_S, out_s.at[1], in_s.at[1], above)
        prepare(M_PLANE_D, out_d.at[1], in_d.at[1], above)
        guarded.append((M_PLANE_S, is_head & (plane < planes - 1)))
        guarded.append((M_PLANE_D, is_head & (plane < planes - 1)))

        @pl.when(is_head)
        def _():
            arrived(M_PAIR_S)
            arrived(M_PAIR_D)

        @pl.when(later_head)
        def _():
            plane_s[...] = own_s[...] + jnp.exp(own_d[...]) * in_s[0].astype(f32)

        @pl.when(early_head)
        def _():
            plane_s[...] = in_s[0].astype(f32) + jnp.exp(in_d[0]) * own_s[...]

        @pl.when(is_head)
        def _():
            plane_d[...] = own_d[...] + in_d[0]

        @pl.when(is_head & (plane == 0))
        def _():
            in_s[1] = jnp.zeros(in_s.shape[1:], bf16)
            in_d[1] = jnp.zeros(in_d.shape[1:], f32)
            out_s[1] = plane_s[...].astype(bf16)
            out_d[1] = plane_d[...]
            copies[M_PLANE_S].start()
            copies[M_PLANE_D].start()

    def states_up(k):
        @pl.when(is_head & (plane == k))
        def _():
            arrived(M_PLANE_S)
            arrived(M_PLANE_D)
            if k < planes - 1:
                out_s[1] = (plane_s[...] + jnp.exp(plane_d[...]) * in_s[1].astype(f32)).astype(bf16)
                out_d[1] = plane_d[...] + in_d[1]
                copies[M_PLANE_S].start()
                copies[M_PLANE_D].start()

    def states_last():
        @pl.when(later_head)
        def _():
            bef_s[...] = in_s[0].astype(f32) + jnp.exp(in_d[0]) * in_s[1].astype(f32)
            out_s[2] = in_s[1]

        @pl.when(early_head)
        def _():
            bef_s[...] = in_s[1].astype(f32)
            out_s[2] = (own_s[...] + jnp.exp(own_d[...]) * in_s[1].astype(f32)).astype(bf16)

        send_if(M_LAST_S, out_s.at[2], in_s.at[2], beside, is_head)

    def states_in():
        @pl.when(is_tail)
        def _():
            arrived(M_LAST_S)
            bef_s[...] = in_s[2].astype(f32)

    def mixer_finish():
        square = jnp.zeros((tok_m, 1), f32)
        for n in range(0, chans, 256):
            at = slice(n, n + 256)
            carried = jnp.dot(read_b[...], bef_s[:, at].astype(bf16), preferred_element_type=f32)
            value = (y_v[:, at] + carried * grow_v[:, at]) * jax.nn.silu(ogate_v[:, at].astype(f32))
            y_v[:, at] = value
            square = square + jnp.sum(value * value, axis=-1, keepdims=True)
        scale = lax.rsqrt(square / chans + eps_norm)
        normed = (y_v[...] * scale * mgain_ref[...]).astype(bf16)
        block = mix_v.shape[1]
        for n in range(0, width, col):
            part = jnp.dot(normed, proj_v[:, n : n + col], preferred_element_type=f32).astype(bf16)
            for i in range(4):
                mix_v[i, :, n : n + col] = part[i * block : (i + 1) * block]
        send(M_MIX_CORE, mix_v.at[t_core], mix_r.at[0], core)
        send(M_MIX_FAR, mix_v.at[t_far], mix_r.at[1], core)

    def mix_across():
        arrived(M_MIX_CORE)
        arrived(M_MIX_FAR)
        mix_s[...] = (mix_v[t_y].astype(f32) + mix_r[1].astype(f32)).astype(bf16)
        send(M_MIX_Y, mix_s, mix_ry, ydev)

    def rows_in():
        arrived(M_META_Y)
        arrived(M_ROWS_Y)

    pl.semaphore_wait(barrier, len(peers))
    halo_out()
    a0(0)
    rows_out()
    bo(1)
    bo(2)
    bo(3)
    weights_out()
    mixer_early()
    mixer_states()
    states_pair()
    a0(1)
    states_plane()
    mixer_rows_local()
    a0(2)
    a1(0)
    rows_in()
    by(1)
    by(2)
    states_up(1)
    a1(1)
    by(3)
    shared_in()
    shared_rows(0)
    shared_rows(1)
    a0(3)
    expert_in()
    b3(0)
    a3(0)
    states_up(2)
    b3(1)
    b3(2)
    a5(0)
    a3(1)
    a1(2)
    states_up(3)
    states_last()
    a3(2)
    a1(3)
    a5(1)
    b3(3)
    states_in()
    mix_in()
    mixer_finish()
    a5(2)
    a3(3)
    mix_across()
    a5(3)
    dense_out()

    arrived(M_MIX_Y)
    mix_out[...] = (mix_v[t].astype(f32) + mix_r[0].astype(f32) + mix_ry[...].astype(f32)).astype(bf16)
    for d in range(half):
        arrived(block_message(B_FA, d))
    arrived(M_DENSE)
    columns = jnp.transpose(meta_v[0])
    picks = chosen_slots(columns, other)
    for n in range(0, width, col):
        at = slice(n, n + col)
        value = mixed(columns, picks, ret_a[:, at]) + dense[0, :, at] + dense_r[:, at].astype(f32)
        moe_out[:, at] = value.astype(bf16)
    for name, here in guarded:

        @pl.when(here)
        def _(name=name):
            copies[name].wait_send()

    kept_back = [name for name, _ in guarded]
    for name in copies:
        if name not in kept_back:
            copies[name].wait_send()


def settle_kernel(mix_ref, moe_ref, mix_out, moe_out, sem):
    copies = [
        pltpu.make_async_copy(mix_ref, mix_out, sem.at[0]),
        pltpu.make_async_copy(moe_ref, moe_out, sem.at[1]),
    ]
    for copy in copies:
        copy.start()
    for copy in copies:
        copy.wait()


def settle(mix, moe):
    return pl.pallas_call(
        settle_kernel,
        out_shape=tuple(jax.ShapeDtypeStruct(x.shape, x.dtype) for x in (mix, moe)),
        in_specs=[pl.BlockSpec(memory_space=pltpu.VMEM)] * 2,
        out_specs=tuple([pl.BlockSpec(memory_space=pl.ANY)] * 2),
        scratch_shapes=[pltpu.SemaphoreType.DMA((2,))],
        name="settle",
    )(mix, moe)


def exchange(ep_count, capacity, small, large):
    (rows, heads, write, read, ogate, proj, gate, up, down, sgate, sup, sdown) = large
    half = ep_count // 2
    tok, width = rows.shape
    bf16, f32 = jnp.bfloat16, jnp.float32
    cap = capacity
    tok_m, chans = heads.shape
    state = write.shape[1]
    mix_block = tok_m // 4
    count = SINGLE + BLOCK_KINDS * half
    shapes = [(array.shape, bf16) for array in (rows, heads, write, read, ogate, proj)]
    shapes += [((2, *array.shape), bf16) for array in (gate, up, down, sgate, sup, sdown)]
    shapes += [
        ((16, chans), bf16),
        ((16, state), bf16),
        ((16, state), bf16),
        ((tok_m + 8, chans), f32),
        ((tok_m + 8, state), f32),
        ((tok_m + 8, state), f32),
        ((tok_m, chans), f32),
        ((tok_m, state), f32),
        ((tok_m, state), f32),
        ((tok_m, chans), f32),
        ((tok_m, chans), f32),
        ((tok_m, state), bf16),
        ((tok_m, chans), f32),
        ((state, chans), f32),
        ((1, chans), f32),
        ((state, chans), f32),
        ((1, chans), f32),
        ((state, chans), f32),
        ((3, state, chans), bf16),
        ((2, 1, chans), f32),
        ((3, state, chans), bf16),
        ((2, 1, chans), f32),
        ((4, mix_block, width), bf16),
        ((2, mix_block, width), bf16),
        ((mix_block, width), bf16),
        ((mix_block, width), bf16),
        ((2, 8, tok), f32),
        ((2, tok, width), bf16),
        ((half, cap, width), bf16),
        ((half - 1, 2 * cap, width), bf16),
        ((half, 2 * cap, width), bf16),
        ((half, 2 * cap, width), bf16),
        ((half, 2 * cap, width), bf16),
        ((half - 1, 2, cap, width), bf16),
        ((half, cap, width), bf16),
        ((half, cap, width), bf16),
        ((half * cap, width), bf16),
        ((2, half * cap, width), bf16),
        ((2, tok, width), f32),
        ((tok, width), bf16),
        ((tok, width), bf16),
    ]
    any_spec = pl.BlockSpec(memory_space=pl.ANY)
    vmem_spec = pl.BlockSpec(memory_space=pltpu.VMEM)
    return pl.pallas_call(
        functools.partial(exchange_kernel, ep_count, capacity),
        out_shape=(
            jax.ShapeDtypeStruct((mix_block, width), bf16),
            jax.ShapeDtypeStruct((tok, width), bf16),
        ),
        in_specs=[any_spec] * len(large) + [vmem_spec] * len(small),
        out_specs=(vmem_spec, vmem_spec),
        scratch_shapes=[pltpu.VMEM(shape, dtype) for shape, dtype in shapes]
        + [
            pltpu.SemaphoreType.DMA((len(large),)),
            pltpu.SemaphoreType.DMA((count,)),
            pltpu.SemaphoreType.DMA((count,)),
        ],
        compiler_params=pltpu.CompilerParams(
            collective_id=0, has_side_effects=True, vmem_limit_bytes=62 * 1024 * 1024
        ),
        name="mixer_and_experts",
    )(*large, *small)


def direct(
    head_inputs_unfiltered,
    group_write_vectors,
    group_read_vectors,
    output_gate_inputs,
    step_preactivation,
    extra_decay_logs,
    head_decay_logs,
    head_filter_taps,
    write_filter_taps,
    read_filter_taps,
    grouped_norm_gain,
    mixer_output_weight,
    expert_input_rows,
    expert_norm_gain,
    routes,
    router_chosen_scores,
    routed_gate_weight,
    routed_up_weight,
    routed_down_weight,
    shared_gate_weight,
    shared_up_weight,
    shared_down_weight,
):
    ep_count = lax.axis_size("ep")
    capacity = 3 * expert_input_rows.shape[0] * routes.shape[1] // (2 * ep_count)
    small = (
        routes.T,
        router_chosen_scores.T,
        expert_norm_gain.reshape(1, -1),
        step_preactivation,
        extra_decay_logs,
        head_decay_logs.reshape(1, -1),
        head_filter_taps,
        write_filter_taps,
        read_filter_taps,
        grouped_norm_gain.reshape(1, -1),
    )
    large = (
        expert_input_rows,
        head_inputs_unfiltered,
        group_write_vectors,
        group_read_vectors,
        output_gate_inputs,
        mixer_output_weight,
        routed_gate_weight[0],
        routed_up_weight[0],
        routed_down_weight[0],
        shared_gate_weight,
        shared_up_weight,
        shared_down_weight,
    )
    return settle(*exchange(ep_count, capacity, small, large))


def fits_direct(mesh, rows, mix_rows, top_count, experts, groups):
    ep_count, tp_count = mesh.shape["ep"], mesh.shape["tp"]
    tok_local = rows // (ep_count * tp_count)
    capacity = 3 * tok_local * top_count // (2 * experts)
    return (
        tp_count == 4
        and groups == tp_count
        and experts == ep_count
        and ep_count == 8
        and top_count == 2
        and capacity % 16 == 0
        and tok_local == 128
        and mix_rows == tok_local * ep_count
    )


def solution(mesh):
    in_specs = (
        P("ep", "tp"),
        P("ep", "tp"),
        P("ep", "tp"),
        P("ep", "tp"),
        P("tp", "ep"),
        P("tp", "ep"),
        P("tp"),
        P(None, "tp"),
        P(None, "tp"),
        P(None, "tp"),
        P("tp"),
        P("tp", None),
        P(("ep", "tp"), None),
        P(),
        P(("ep", "tp"), None),
        P(("ep", "tp"), None),
        P("ep", None, "tp"),
        P("ep", None, "tp"),
        P("ep", "tp", None),
        P(None, "tp"),
        P(None, "tp"),
        P("tp", None),
    )
    out_specs = (P(("ep", "tp"), None), P(("ep", "tp"), None))
    def step(*args):
        direct_form = fits_direct(
            mesh,
            args[12].shape[0],
            args[0].shape[0],
            args[14].shape[1],
            args[16].shape[0],
            args[1].shape[1] // STATE,
        )
        return jax.shard_map(
            direct if direct_form else local,
            mesh=mesh,
            in_specs=in_specs,
            out_specs=out_specs,
            check_vma=False,
        )(*args)

    return step
```
